256 devices in a mesh: grp: 2 (over y), sp: 32 (over z, core), tp: 4 (over x).
Axes of the slice: x: 4, y: 2, z: 16, core: 2. Of those that a mesh axis runs over, the one named last changes fastest.
The devices are a block of a 4x16x16 slice.
Arguments:
- latent: bfloat16 [16384, 512], P(('grp', 'sp')), parts along dimension 0, may hold values from -6 to 6
- rope_key: bfloat16 [16384, 64], P(('grp', 'sp')), parts along dimension 0, may hold values from -6 to 6
- wide_query: bfloat16 [16384, 1536], P(('grp', 'sp'), 'tp'), parts along dimension 0, may hold values from -1300 to 1300
- narrow_query: bfloat16 [16384, 1024], P(('grp', 'sp'), 'tp'), parts along dimension 0, may hold values from -1300 to 1300
- wide_key_weight: bfloat16 [512, 1024], P(None, 'tp'), may hold values from -0.25 to 0.25
- wide_value_weight: bfloat16 [512, 1024], P(None, 'tp'), may hold values from -0.25 to 0.25
- narrow_key_weight: bfloat16 [512, 512], P(None, 'tp'), may hold values from -0.25 to 0.25
- narrow_value_weight: bfloat16 [512, 512], P(None, 'tp'), may hold values from -0.25 to 0.25
- latent_norm_scale: float32 [512], replicated, may hold values from 0.1 to 1.9
- out_wide: bfloat16 [1024, 4096], P('tp'), may hold values from -0.4375 to 0.4375
- out_narrow: bfloat16 [512, 4096], P('tp'), may hold values from -0.4375 to 0.4375
- residual: bfloat16 [16384, 4096], P(('grp', 'sp', 'tp')), parts along dimension 0, may hold values from -6 to 6
- ffn_gain: float32 [4096], replicated, may hold values from 0.1 to 1.9
- shared_gate: bfloat16 [4096, 512], P(None, 'tp'), may hold values from -0.09375 to 0.09375
- shared_up: bfloat16 [4096, 512], P(None, 'tp'), may hold values from -0.09375 to 0.09375
- shared_down: bfloat16 [512, 4096], P('tp'), may hold values from -0.25 to 0.25
- expert_gate: bfloat16 [128, 4096, 192], P(('sp', 'tp')), may hold values from -0.09375 to 0.09375
- expert_up: bfloat16 [128, 4096, 192], P(('sp', 'tp')), may hold values from -0.09375 to 0.09375
- expert_down: bfloat16 [128, 192, 4096], P(('sp', 'tp')), may hold values from -0.4375 to 0.4375
- routes: int32 [16384, 2], P(('grp', 'sp', 'tp')), parts along dimension 0, may hold values from 0 to 127, all different within a row; in each aligned block of 64 rows (0 to 63, 64 to 127, ...) at most 2 rows name the same one
- route_weights: float32 [16384, 2], P(('grp', 'sp', 'tp')), parts along dimension 0, may hold values from 0.25 to 1.5
Outputs:
- layer_out: bfloat16 [16384, 4096], P(('grp', 'sp', 'tp')), parts along dimension 0
The draws below stay inside these ranges and needn't reach their ends.
There are 2 independent parts, one for each index of `grp`. The reference program is written for one: setup_inputs(seed, part) draws one part's arguments, and reference() takes and returns one part's arrays. A program takes and returns all parts, laid end to end along the dimension named above; an argument that names none is the same for every part. Nothing has to cross between parts.
Inputs may be any that keep to these rules, and one draw needn't show every extreme that they name: `routes`: each row names 2 different experts; in each aligned block of 64 rows no expert is named by more than 2 rows, and some block has an expert named exactly 2 times.
All inputs are finite; a program needn't handle non-finite values.
Results may differ from the reference program's by a relative error of at most 0.023.
Values may be sent and summed in bfloat16 or wider, within the bound.
A program may use at most 128 MiB of HBM per device.

```python
import math
import jax
import jax.numpy as jnp
import numpy as np
from jax import lax

D = 4096
LATENT_WIDTH = 512
ROPE = 64
FIRST_HEADS = 8
WIDE_HEAD_SIZE = 128
SECOND_HEADS = 8
NARROW_HEAD_SIZE = 64
SHARED_FF = 512
EXPERT_FF = 192
TOPK = 2
TOKEN_COUNT = 8192
ROWS = 64
EXPERTS = 128
CAP = 2
N_SP = 32
N_TP = 4


def query_values(key, columns):
    values = jnp.clip(2.5 * jax.random.normal(key, (TOKEN_COUNT, columns), jnp.float32), -15.0, 15.0)
    return values.astype(jnp.bfloat16)


def draw_wide_query(key, part):
    return query_values(jax.random.fold_in(key, 11), FIRST_HEADS * (WIDE_HEAD_SIZE + ROPE))


def draw_narrow_query(key, part):
    return query_values(jax.random.fold_in(key, 23), SECOND_HEADS * (NARROW_HEAD_SIZE + ROPE))


def levels(own_key, shape, cuts, low, largest):
    level = 1.0
    for dim, blocks in cuts:
        heights = jax.random.uniform(jax.random.fold_in(jax.random.fold_in(own_key, 6), dim), (blocks,), jnp.float32, low / len(cuts), largest / len(cuts))
        level = level * jnp.repeat(jnp.exp(heights), shape[dim] // blocks).reshape((-1,) + (1,) * (len(shape) - 1 - dim))
    return level


def deal_out(stream_key, own, number, rows, count, top, limit, skew):
    order = jax.random.permutation(stream_key, count)
    crowded, ordinary = portions_of(count, rows * top, limit, skew, True), portions_of(count, rows * top, limit, skew, False)
    places = jnp.arange(count)

    def named(lengths, turn):
        used = int((lengths > 0).sum())
        fixed = max(1, used // 4)
        passed = fixed + (places - fixed + turn * (used - fixed)) % max(1, count - fixed)
        return jnp.zeros((count,), jnp.int32).at[order[jnp.where(places < fixed, places, passed)]].set(jnp.asarray(lengths, jnp.int32))

    lengths = jnp.where(number % 4 == 0, named(crowded, number // 4), named(ordinary, number - number // 4 - 1))
    mixed = jax.random.permutation(jax.random.fold_in(own, 3), count)
    source_of, receiver = mixed[0:count // 2 * 2:2], mixed[1:count // 2 * 2:2]
    slack = jnp.minimum(lengths[source_of] - 1, limit - lengths[receiver]) // 2
    slack = jnp.where((source_of == order[0]) | (receiver == order[0]) | (lengths[receiver] == 0), 0, jnp.maximum(slack, 0))
    passed = jax.random.randint(jax.random.fold_in(own, 4), (count // 2,), 0, 1 << 20) % (slack + 1)
    lengths = lengths.at[source_of].add(-passed).at[receiver].add(passed)
    items = jnp.searchsorted(jnp.cumsum(lengths), jnp.arange(rows * top), side="right").astype(jnp.int32)
    grid = items.reshape(top, rows).T
    grid = grid[jax.random.permutation(jax.random.fold_in(own, 1), rows)]
    turn = jax.random.randint(jax.random.fold_in(own, 2), (rows, 1), 0, top)
    return jnp.take_along_axis(grid, (jnp.arange(top)[None, :] + turn) % top, axis=1)


def portions_of(number_of, total, reach, slope, full):
    weights = [(1 << 20) // math.isqrt(standing ** slope) + 1 for standing in range(1, number_of + 1)]
    largest = reach if full else min(reach, max(-(-total // number_of), total * weights[0] // sum(weights)))
    least = 1 if total - largest >= number_of - 1 else 0
    counts, surplus = [largest] + [least] * (number_of - 1), total - largest - least * (number_of - 1)
    while surplus > 0:
        free = [i for i in range(1, number_of) if counts[i] < largest] or [i for i in range(1, number_of) if counts[i] < reach]
        whole, budget = sum([weights[i] for i in free]), surplus
        for i in free:
            addition = min(reach - counts[i], max(1, budget * weights[i] // whole), surplus)
            counts[i] = counts[i] + addition
            surplus = surplus - addition
    return np.array(counts)


def centred(stream_key, extent, width, bound, shards=(), kind=jnp.bfloat16):
    level = levels(stream_key, extent, shards, -0.22, 0.18) if shards else 1.0
    drawn = jax.random.normal(stream_key, extent, jnp.float32) * width * level
    return jnp.minimum(jnp.maximum(drawn, -bound), bound).astype(kind)


def setup_inputs(seed: int = 0, part: int = 0) -> dict:
    key_list = jax.random.split(jax.random.key(seed), 22)
    part_splits = jax.random.split(jax.random.fold_in(key_list[21], part), 22)
    latent = centred(part_splits[0], (TOKEN_COUNT, LATENT_WIDTH), 1.0, 6.0, ((0, 32),))
    rope_key = centred(part_splits[1], (TOKEN_COUNT, ROPE), 1.0, 6.0, ((0, 32),))
    wide_query = draw_wide_query(jax.random.fold_in(jax.random.fold_in(key_list[21], part), 71), part)
    narrow_query = draw_narrow_query(jax.random.fold_in(jax.random.fold_in(key_list[21], part), 71), part)
    wide_key_weight = centred(key_list[4], (LATENT_WIDTH, FIRST_HEADS * WIDE_HEAD_SIZE), LATENT_WIDTH ** -0.5, 0.25, ((1, 4),))
    wide_value_weight = centred(key_list[5], (LATENT_WIDTH, FIRST_HEADS * WIDE_HEAD_SIZE), LATENT_WIDTH ** -0.5, 0.25, ((1, 4),))
    narrow_key_weight = centred(key_list[6], (LATENT_WIDTH, SECOND_HEADS * NARROW_HEAD_SIZE), LATENT_WIDTH ** -0.5, 0.25, ((1, 4),))
    narrow_value_weight = centred(key_list[7], (LATENT_WIDTH, SECOND_HEADS * NARROW_HEAD_SIZE), LATENT_WIDTH ** -0.5, 0.25, ((1, 4),))
    latent_norm_scale = jnp.clip(1.0 + 0.18 * jax.random.normal(key_list[8], (LATENT_WIDTH,), jnp.float32), 0.1, 1.9)
    out_wide = centred(key_list[9], (FIRST_HEADS * WIDE_HEAD_SIZE, D), ((FIRST_HEADS * WIDE_HEAD_SIZE + SECOND_HEADS * NARROW_HEAD_SIZE) // 8) ** -0.5, 0.4375, ((0, 4),))
    out_narrow = centred(key_list[10], (SECOND_HEADS * NARROW_HEAD_SIZE, D), ((FIRST_HEADS * WIDE_HEAD_SIZE + SECOND_HEADS * NARROW_HEAD_SIZE) // 8) ** -0.5, 0.4375, ((0, 4),))
    residual = centred(part_splits[11], (TOKEN_COUNT, D), 1.0, 6.0, ((0, 128),))
    ffn_gain = jnp.clip(1.0 + 0.18 * jax.random.normal(key_list[12], (D,), jnp.float32), 0.1, 1.9)
    shared_gate = centred(key_list[13], (D, SHARED_FF), D ** -0.5, 0.09375, ((1, 4),))
    shared_up = centred(key_list[14], (D, SHARED_FF), D ** -0.5, 0.09375, ((1, 4),))
    shared_down = centred(key_list[15], (SHARED_FF, D), SHARED_FF ** -0.5, 0.25, ((0, 4),))
    expert_gate = centred(key_list[16], (EXPERTS, D, EXPERT_FF), D ** -0.5, 0.09375, ((0, 128),))
    expert_up = centred(key_list[17], (EXPERTS, D, EXPERT_FF), D ** -0.5, 0.09375, ((0, 128),))
    expert_down = centred(key_list[18], (EXPERTS, EXPERT_FF, D), EXPERT_FF ** -0.5, 0.4375, ((0, 128),))
    routes_keys = jax.random.split(jax.random.fold_in(part_splits[19], 1), TOKEN_COUNT // ROWS)
    routes_turns = jax.random.permutation(jax.random.fold_in(part_splits[19], 3), TOKEN_COUNT // ROWS)
    routes = jax.vmap(lambda own, number: deal_out(jax.random.fold_in(part_splits[19], 2), own, number, ROWS, EXPERTS, TOPK, CAP, 1))(routes_keys, routes_turns).reshape((TOKEN_COUNT, TOPK))
    route_weights = jnp.clip(0.25 + 1.25 * jax.random.uniform(part_splits[20], (TOKEN_COUNT, TOPK), jnp.float32) ** levels(part_splits[20], (TOKEN_COUNT, TOPK), ((0, 128),), -0.2, 0.2), 0.25, 1.5)
    return {"latent": latent, "rope_key": rope_key, "wide_query": wide_query, "narrow_query": narrow_query, "wide_key_weight": wide_key_weight, "wide_value_weight": wide_value_weight, "narrow_key_weight": narrow_key_weight, "narrow_value_weight": narrow_value_weight, "latent_norm_scale": latent_norm_scale, "out_wide": out_wide, "out_narrow": out_narrow, "residual": residual, "ffn_gain": ffn_gain, "shared_gate": shared_gate, "shared_up": shared_up, "shared_down": shared_down, "expert_gate": expert_gate, "expert_up": expert_up, "expert_down": expert_down, "routes": routes, "route_weights": route_weights}


EPS = 1e-06
ROPE_BASE = 10000.0
NEG_FILL = -1e+30

def rounded(values):
    return lax.optimization_barrier(values.astype(jnp.bfloat16)).astype(jnp.float32)

def rotate(values, positions):
    half_size = values.shape[-1] // 2
    inverse = ROPE_BASE ** (-jnp.arange(half_size, dtype=jnp.float32) * 2.0 / values.shape[-1])
    angles = positions.astype(jnp.float32)[:, None] * inverse[None, :]
    shaped = (angles.shape[0],) + (1,) * (values.ndim - 2) + (half_size,)
    cosine_table = jnp.cos(angles).reshape(shaped)
    sine_table = jnp.sin(angles).reshape(shaped)
    first_half = values[..., :half_size]
    second_half = values[..., half_size:]
    return jnp.concatenate([first_half * cosine_table - second_half * sine_table, second_half * cosine_table + first_half * sine_table], axis=-1)

def rms_scale(values, gain):
    return values * lax.rsqrt(lax.optimization_barrier(jnp.mean(values * values, axis=-1, keepdims=True)) + EPS) * gain

def update(state, query_plain, query_turned, keys, turned_rows, values, visible, factor):
    running_max, running_sum, weighted = state
    scores = jnp.einsum('qhd,khd->hqk', query_plain.astype(jnp.float32), keys.astype(jnp.float32))
    scores = scores + jnp.einsum('qhr,kr->hqk', query_turned.astype(jnp.float32), turned_rows.astype(jnp.float32))
    scores = jnp.where(visible[None], scores * factor, NEG_FILL)
    new_max = jnp.maximum(running_max, lax.optimization_barrier(jnp.max(scores, axis=2)))
    probs = jnp.where(visible[None], jnp.exp(scores - new_max[:, :, None]), 0.0)
    fading = jnp.exp(running_max - new_max)
    running_sum = running_sum * fading + lax.optimization_barrier(jnp.sum(probs, axis=2))
    weighted = weighted * fading[:, :, None] + jnp.einsum('hqk,khd->hqd', rounded(probs), values.astype(jnp.float32))
    return (new_max, running_sum, weighted)

def attend_group(query_plain, query_turned, keys, values, turned_keys, factor):
    tokens_all, heads, value_size = values.shape
    block = math.gcd(tokens_all, 512)
    blocks_all = tokens_all // block

    def per_query(block_index):
        query_start = block_index * block
        plain_rows = lax.dynamic_slice_in_dim(query_plain, query_start, block, 0)
        turned_rows_q = lax.dynamic_slice_in_dim(query_turned, query_start, block, 0)
        query_pos = query_start + jnp.arange(block, dtype=jnp.int32)

        def per_key(key_index, state):
            key_start = key_index * block
            key_pos = key_start + jnp.arange(block, dtype=jnp.int32)
            visible = key_pos[None, :] <= query_pos[:, None]
            return update(state, plain_rows, turned_rows_q, lax.dynamic_slice_in_dim(keys, key_start, block, 0), lax.dynamic_slice_in_dim(turned_keys, key_start, block, 0), lax.dynamic_slice_in_dim(values, key_start, block, 0), visible, factor)
        initial = (jnp.full((heads, block), NEG_FILL, jnp.float32), jnp.zeros((heads, block), jnp.float32), jnp.zeros((heads, block, value_size), jnp.float32))
        final = lax.fori_loop(0, block_index + 1, per_key, initial)
        normal_sampler = final[2] / final[1][:, :, None]
        return normal_sampler.astype(jnp.bfloat16).transpose(1, 0, 2).reshape(block, heads * value_size)
    outputs = lax.map(per_query, jnp.arange(blocks_all, dtype=jnp.int32))
    return outputs.reshape(tokens_all, heads * value_size)

def reference(latent, rope_key, wide_query, narrow_query, wide_key_weight, wide_value_weight, narrow_key_weight, narrow_value_weight, latent_norm_scale, out_wide, out_narrow, residual, ffn_gain, shared_gate, shared_up, shared_down, expert_gate, expert_up, expert_down, routes, route_weights):
    positions = jnp.arange(TOKEN_COUNT, dtype=jnp.int32)
    normed_latent = rms_scale(latent.astype(jnp.float32), latent_norm_scale).astype(jnp.bfloat16)
    turned_key = rotate(rope_key.astype(jnp.float32), positions).astype(jnp.bfloat16)
    wide_heads_q = wide_query.reshape(TOKEN_COUNT, FIRST_HEADS, WIDE_HEAD_SIZE + ROPE)
    wide_plain = wide_heads_q[..., :WIDE_HEAD_SIZE]
    wide_turned = rotate(wide_heads_q[..., WIDE_HEAD_SIZE:].astype(jnp.float32), positions).astype(jnp.bfloat16)
    narrow_heads_q = narrow_query.reshape(TOKEN_COUNT, SECOND_HEADS, NARROW_HEAD_SIZE + ROPE)
    narrow_plain = narrow_heads_q[..., :NARROW_HEAD_SIZE]
    narrow_turned = rotate(narrow_heads_q[..., NARROW_HEAD_SIZE:].astype(jnp.float32), positions).astype(jnp.bfloat16)
    wide_keys = jnp.dot(normed_latent, wide_key_weight, preferred_element_type=jnp.float32).astype(jnp.bfloat16).reshape(TOKEN_COUNT, FIRST_HEADS, WIDE_HEAD_SIZE)
    wide_values = jnp.dot(normed_latent, wide_value_weight, preferred_element_type=jnp.float32).astype(jnp.bfloat16).reshape(TOKEN_COUNT, FIRST_HEADS, WIDE_HEAD_SIZE)
    narrow_keys = jnp.dot(normed_latent, narrow_key_weight, preferred_element_type=jnp.float32).astype(jnp.bfloat16).reshape(TOKEN_COUNT, SECOND_HEADS, NARROW_HEAD_SIZE)
    narrow_values = jnp.dot(normed_latent, narrow_value_weight, preferred_element_type=jnp.float32).astype(jnp.bfloat16).reshape(TOKEN_COUNT, SECOND_HEADS, NARROW_HEAD_SIZE)
    wide_mix = attend_group(wide_plain, wide_turned, wide_keys, wide_values, turned_key, (WIDE_HEAD_SIZE + ROPE) ** (-0.5))
    narrow_mix = attend_group(narrow_plain, narrow_turned, narrow_keys, narrow_values, turned_key, (NARROW_HEAD_SIZE + ROPE) ** (-0.5))
    wide_share = FIRST_HEADS * WIDE_HEAD_SIZE // N_TP
    narrow_share = SECOND_HEADS * NARROW_HEAD_SIZE // N_TP
    projected = jnp.zeros((TOKEN_COUNT, D), jnp.float32)
    for member in range(N_TP):
        partial_value = jnp.dot(wide_mix[:, member * wide_share:(member + 1) * wide_share], out_wide[member * wide_share:(member + 1) * wide_share], preferred_element_type=jnp.float32)
        partial_value = partial_value + jnp.dot(narrow_mix[:, member * narrow_share:(member + 1) * narrow_share], out_narrow[member * narrow_share:(member + 1) * narrow_share], preferred_element_type=jnp.float32)
        projected = projected + rounded(partial_value)
    stream = (residual.astype(jnp.float32) + projected).astype(jnp.bfloat16)
    normed = rms_scale(stream.astype(jnp.float32), ffn_gain).astype(jnp.bfloat16)
    shared_share = SHARED_FF // N_TP
    shared = jnp.zeros((TOKEN_COUNT, D), jnp.float32)
    for member in range(N_TP):
        lower = member * shared_share
        upper = lower + shared_share
        gate_part = jnp.dot(normed, shared_gate[:, lower:upper], preferred_element_type=jnp.float32)
        up_part = jnp.dot(normed, shared_up[:, lower:upper], preferred_element_type=jnp.float32)
        active = (jax.nn.silu(gate_part) * up_part).astype(jnp.bfloat16)
        shared = shared + rounded(jnp.dot(active, shared_down[lower:upper], preferred_element_type=jnp.float32))
    devices_all = N_SP * N_TP
    flat_routes = routes.reshape(devices_all, ROWS * TOPK)
    choose = (flat_routes[:, :, None] == jnp.arange(EXPERTS, dtype=jnp.int32)[None, None, :]).astype(jnp.int32)
    earlier = jnp.cumsum(choose, axis=1) - choose
    slots = lax.optimization_barrier(jnp.sum(earlier * choose, axis=2)).astype(jnp.int32)
    device_ids = jnp.broadcast_to(jnp.arange(devices_all, dtype=jnp.int32)[:, None], flat_routes.shape)
    token_of = (device_ids * ROWS + jnp.arange(ROWS * TOPK, dtype=jnp.int32)[None, :] // TOPK).astype(jnp.int32)
    table = jnp.zeros((EXPERTS, devices_all, CAP), jnp.int32).at[flat_routes, device_ids, slots].set(token_of)

    def run_expert(member):
        rows_in = normed[table[member].reshape(-1)]
        gate_part = jnp.dot(rows_in, expert_gate[member], preferred_element_type=jnp.float32)
        up_part = jnp.dot(rows_in, expert_up[member], preferred_element_type=jnp.float32)
        active = (jax.nn.silu(gate_part) * up_part).astype(jnp.bfloat16)
        return jnp.dot(active, expert_down[member], preferred_element_type=jnp.float32).astype(jnp.bfloat16)
    results = lax.map(run_expert, jnp.arange(EXPERTS, dtype=jnp.int32))
    picked = results[flat_routes, device_ids * CAP + slots]
    routed = lax.optimization_barrier(jnp.sum(picked.reshape(TOKEN_COUNT, TOPK, D).astype(jnp.float32) * route_weights[:, :, None], axis=1))
    return (stream.astype(jnp.float32) + shared + routed).astype(jnp.bfloat16)
```

```python
import functools
import math

import jax
import jax.numpy as jnp
import numpy as np
from jax import lax
from jax.experimental import pallas as pl
from jax.experimental.pallas import tpu as pltpu
from jax.sharding import PartitionSpec as P

ROPE = 64
WIDE_HEAD_SIZE = 128
NARROW_HEAD_SIZE = 64
LANES = 128


EPS = 1e-06
ROPE_BASE = 10000.0
NEG_FILL = -1e30
LOG2E = 1.4426950408889634


def split_up(array, dim, peers):
    before, after = (array.shape[:dim], array.shape[dim + 1 :])
    return jnp.moveaxis(array.reshape(*before, peers, -1, *after), dim, 0)


def summed_on_arrival(array, axis, dim):
    peers = lax.axis_size(axis)
    blocks = lax.all_to_all(split_up(array, dim, peers), axis, 0, 0, tiled=True)
    return jnp.sum(blocks.astype(jnp.float32), axis=0)


def rms_scale(values, gain):
    return values * lax.rsqrt(jnp.mean(values * values, axis=-1, keepdims=True) + EPS) * gain


def angle_tables(positions):
    half = ROPE // 2
    inverse = ROPE_BASE ** (-np.arange(half) * 2.0 / ROPE)
    angles = positions[:, None] * np.concatenate([inverse, inverse])[None, :]
    pad = ((0, 0), (0, LANES - ROPE))
    return (
        np.pad(np.cos(angles), pad).astype(np.float32),
        np.pad(np.sin(angles), pad).astype(np.float32),
    )


def attention_kernel(
    n_sp,
    n_tp,
    latent_ref,
    rope_key_ref,
    wide_query_ref,
    narrow_query_ref,
    wide_key_ref,
    wide_value_ref,
    narrow_key_ref,
    narrow_value_ref,
    gain_ref,
    local_cos_ref,
    local_sin_ref,
    base_cos_ref,
    base_sin_ref,
    out_ref,
    rows_buf,
    queries,
    narrow_weight,
    top,
    mixed,
    z_send,
    z_recv,
    x_send,
    x_recv,
    d_send,
    d_recv,
):
    tokens, width = latent_ref.shape
    quarter = tokens // n_tp
    zn = n_sp // 2
    steps_up = zn // 2
    steps_down = zn - 1 - steps_up
    me = lax.axis_index("sp")
    x = lax.axis_index("tp")
    z = me // 2
    core = lax.rem(me, 2)
    right = lax.rem(x + 1, n_tp)
    left = lax.rem(x + n_tp - 1, n_tp)
    up = lax.rem(z + 1, zn)
    down = lax.rem(z + zn - 1, zn)
    partner = z * 2 + 1 - core

    barrier = pltpu.get_barrier_semaphore()
    for place in ({"sp": up * 2 + core}, {"sp": down * 2 + core}, {"sp": partner}, {"tp": left}, {"tp": right}):
        pl.semaphore_signal(barrier, inc=1, device_id=place, device_id_type=pl.DeviceIdType.MESH)

    lane = lax.broadcasted_iota(jnp.int32, (tokens, LANES), 1)
    low = lane < ROPE
    lc, ls = local_cos_ref[...], local_sin_ref[...]
    bc, bs = base_cos_ref[pl.ds(me, 1), :], base_sin_ref[pl.ds(me, 1), :]
    cosine = lc * bc - ls * bs
    sine = jnp.where(lane < ROPE // 2, -1.0, 1.0) * (ls * bc + lc * bs)

    def turn(v):
        other = jnp.where(
            lane < ROPE // 2, pltpu.roll(v, LANES - ROPE // 2, 1), pltpu.roll(v, ROPE // 2, 1)
        )
        return (v * cosine + other * sine).astype(jnp.bfloat16)

    lat = latent_ref[...].astype(jnp.float32)
    normed = rms_scale(lat, gain_ref[...]).astype(jnp.bfloat16)
    rope = rope_key_ref[...].astype(jnp.float32)
    turned = turn(jnp.concatenate([rope, jnp.zeros_like(rope)], axis=1))
    for q in range(n_tp):
        rows_buf[me, q, :, :width] = normed[q * quarter : (q + 1) * quarter]
        rows_buf[me, q, :, width:] = turned[q * quarter : (q + 1) * quarter]

    t1 = wide_query_ref[:, LANES : 2 * LANES].astype(jnp.float32)
    t2 = wide_query_ref[:, 2 * LANES :].astype(jnp.float32)
    n0 = narrow_query_ref[:, :LANES].astype(jnp.float32)
    n1 = narrow_query_ref[:, LANES:].astype(jnp.float32)
    half = LANES // 2
    queries[0, :, :LANES] = wide_query_ref[:, :LANES]
    queries[0, :, LANES:] = turn(t1)
    queries[1, :, :LANES] = pltpu.roll(jnp.where(low, t2, t1), half, 1).astype(jnp.bfloat16)
    queries[1, :, LANES:] = turn(pltpu.roll(t2, half, 1))
    queries[2, :, :LANES] = jnp.where(low, n0, 0.0).astype(jnp.bfloat16)
    queries[2, :, LANES:] = turn(pltpu.roll(n0, half, 1))
    queries[3, :, :LANES] = pltpu.roll(jnp.where(low, n1, 0.0), half, 1).astype(jnp.bfloat16)
    queries[3, :, LANES:] = turn(pltpu.roll(n1, half, 1))
    narrow_weight[:, :LANES] = narrow_key_ref[...]
    narrow_weight[:, LANES:] = narrow_value_ref[...]
    top[...] = jnp.full(top.shape, NEG_FILL, jnp.float32)
    mixed[...] = jnp.zeros(mixed.shape, jnp.float32)
    pl.semaphore_wait(barrier, 5)

    def along_z(d, k, j):
        block = jnp.where(d == 0, z - k + zn, z + k) % zn
        target = jnp.where(d == 0, up, down)
        q = lax.rem(x + j, n_tp)
        spot = rows_buf.at[block * 2 + core, q]
        return pltpu.make_async_remote_copy(
            src_ref=spot,
            dst_ref=spot,
            send_sem=z_send.at[d, k, j],
            recv_sem=z_recv.at[d, k + 1, j],
            device_id={"sp": target * 2 + core},
            device_id_type=pl.DeviceIdType.MESH,
        )

    def along_x(d, k, j):
        block = jnp.where(d == 0, z - k + zn, z + k) % zn
        q = lax.rem(x + j, n_tp)
        spot = rows_buf.at[block * 2 + core, q]
        return pltpu.make_async_remote_copy(
            src_ref=spot,
            dst_ref=spot,
            send_sem=x_send.at[d, k, j],
            recv_sem=x_recv.at[d, k, j],
            device_id={"tp": right if j == 0 else left},
            device_id_type=pl.DeviceIdType.MESH,
        )

    def to_partner(d, k):
        block = jnp.where(d == 0, z - k + zn, z + k) % zn
        spot = rows_buf.at[block * 2 + core]
        return pltpu.make_async_remote_copy(
            src_ref=spot,
            dst_ref=spot,
            send_sem=d_send.at[d, k],
            recv_sem=d_recv.at[d, k],
            device_id={"sp": partner},
            device_id_type=pl.DeviceIdType.MESH,
        )

    def arrives(d, k):
        going_up = (k <= z) & (k <= steps_up)
        going_down = ((z + k) % zn < steps_down) & (k <= steps_down)
        return jnp.where(d == 0, going_up, going_down)

    def goes_on(d, k):
        going_up = (k <= z) & (k < steps_up) & (z + 1 < zn)
        going_down = ((z + k) % zn < steps_down) & (k < steps_down)
        return jnp.where(d == 0, going_up, going_down)

    def seen(d, k):
        going_up = (k <= z) & (k <= steps_up)
        going_down = (z + k >= zn) & (z + k - zn < steps_down) & (k <= steps_down)
        return (k >= 1) & jnp.where(d == 0, going_up, going_down)

    wide_factor = (WIDE_HEAD_SIZE + ROPE) ** (-0.5) * LOG2E
    narrow_factor = (NARROW_HEAD_SIZE + ROPE) ** (-0.5) * LOG2E

    def attend(plane, own):
        rows = rows_buf[pl.ds(plane * 2, 2)].reshape(2 * tokens, width + LANES)
        latents, turned_rows = rows[:, :width], rows[:, width:]
        keys = 2 * tokens
        ones = jnp.ones((keys, LANES), jnp.bfloat16)

        def up_from(weight):
            return jnp.dot(latents, weight[...], preferred_element_type=jnp.float32).astype(jnp.bfloat16)

        wide_k, wide_v, narrow = up_from(wide_key_ref), up_from(wide_value_ref), up_from(narrow_weight)
        narrow_k = jnp.concatenate([narrow[:, :LANES], turned_rows], axis=1)
        narrow_v = jnp.concatenate([narrow[:, LANES:], ones], axis=1)
        if own:
            gap = lax.broadcasted_iota(jnp.int32, (tokens, keys), 1) - lax.broadcasted_iota(
                jnp.int32, (tokens, keys), 0
            )
            visible = gap <= core * tokens
        for h in range(4):
            if h < 2:
                at = slice(h * LANES, (h + 1) * LANES)
                k_h = jnp.concatenate([wide_k[:, at], turned_rows], axis=1)
                v_h = jnp.concatenate([wide_v[:, at], ones], axis=1)
            else:
                k_h, v_h = narrow_k, narrow_v
            scores = lax.dot_general(
                queries[h], k_h, (((1,), (1,)), ((), ())), preferred_element_type=jnp.float32
            ) * (wide_factor if h < 2 else narrow_factor)
            if own:
                scores = jnp.where(visible, scores, NEG_FILL)
            old = top[h]
            new = jnp.maximum(old, jnp.max(scores, axis=1, keepdims=True))
            top[h] = new
            weights = jnp.exp2(scores - jnp.concatenate([new] * (keys // LANES), axis=1)).astype(jnp.bfloat16)
            fading = jnp.exp2(old - new)
            mixed[h] = mixed[h] * jnp.concatenate([fading, fading], axis=1) + jnp.dot(
                weights, v_h, preferred_element_type=jnp.float32
            )

    to_partner(0, 0).start()
    for d in range(2):

        @pl.when(goes_on(d, 0))
        def _():
            for j in range(2):
                along_z(d, 0, j).start()

    to_partner(0, 0).wait_recv()

    attend(z, True)

    def one_step(k, carry):
        def forward(d, c):
            @pl.when(arrives(d, k))
            def _():
                for j in range(2):
                    along_z(d, k - 1, j).wait_recv()

            @pl.when(goes_on(d, k))
            def _():
                for j in range(2):
                    along_z(d, k, j).start()

            @pl.when(seen(d, k))
            def _():
                for j in range(2):
                    along_x(d, k, j).start()

            @pl.when(seen(d, k - 1))
            def _():
                for j in range(2):
                    along_x(d, k - 1, j).wait_recv()
                to_partner(d, k - 1).start()

            return c

        lax.fori_loop(0, 2, forward, 0)

        def work(d, c):
            @pl.when(seen(d, k - 2))
            def _():
                to_partner(d, k - 2).wait_recv()
                attend(jnp.where(d == 0, z - k + 2, z + k - 2 - zn), False)

            return c

        lax.fori_loop(0, 2, work, 0)
        return carry

    lax.fori_loop(1, steps_up + 3, one_step, 0)

    to_partner(0, 0).wait_send()

    def settle(k, carry):
        def both(d, c):
            @pl.when(goes_on(d, k))
            def _():
                for j in range(2):
                    along_z(d, k, j).wait_send()

            @pl.when(seen(d, k))
            def _():
                for j in range(2):
                    along_x(d, k, j).wait_send()
                to_partner(d, k).wait_send()

            return c

        return lax.fori_loop(0, 2, both, carry)

    lax.fori_loop(0, steps_up + 1, settle, 0)

    for h in range(2):
        out_ref[:, h * LANES : (h + 1) * LANES] = (mixed[h, :, :LANES] / mixed[h, :, LANES:]).astype(
            out_ref.dtype
        )
    out_ref[:, 2 * LANES :] = jnp.where(
        low, mixed[2, :, :LANES] / mixed[2, :, LANES:], mixed[3, :, :LANES] / mixed[3, :, LANES:]
    ).astype(out_ref.dtype)


def attention(
    latent, rope_key, wide_query, narrow_query, wide_key, wide_value, narrow_key, narrow_value, gain
):
    tokens, width = latent.shape
    n_sp, n_tp = lax.axis_size("sp"), lax.axis_size("tp")
    zn = n_sp // 2
    assert n_sp % 4 == 0 and n_tp == 4 and wide_query.shape[1] == 3 * LANES
    assert narrow_query.shape[1] == 2 * LANES and zn >= 4
    local_cos, local_sin = angle_tables(np.arange(tokens, dtype=np.float64))
    base_cos, base_sin = angle_tables(np.arange(n_sp, dtype=np.float64) * tokens)
    hops = zn // 2 + 1
    dma = pltpu.SemaphoreType.DMA
    vmem = pl.BlockSpec(memory_space=pltpu.VMEM)
    return pl.pallas_call(
        functools.partial(attention_kernel, n_sp, n_tp),
        out_shape=jax.ShapeDtypeStruct((tokens, 3 * LANES), jnp.bfloat16),
        in_specs=[vmem] * 13,
        out_specs=vmem,
        scratch_shapes=[
            pltpu.VMEM((n_sp, n_tp, tokens // n_tp, width + LANES), jnp.bfloat16),
            pltpu.VMEM((4, tokens, 2 * LANES), jnp.bfloat16),
            pltpu.VMEM((width, 2 * LANES), jnp.bfloat16),
            pltpu.VMEM((4, tokens, LANES), jnp.float32),
            pltpu.VMEM((4, tokens, 2 * LANES), jnp.float32),
            dma((2, hops, 2)),
            dma((2, hops + 1, 2)),
            dma((2, hops, 2)),
            dma((2, hops, 2)),
            dma((2, hops)),
            dma((2, hops)),
        ],
        compiler_params=pltpu.CompilerParams(
            collective_id=0, has_side_effects=True, vmem_limit_bytes=48 * 1024 * 1024
        ),
    )(
        latent,
        rope_key,
        wide_query,
        narrow_query,
        wide_key,
        wide_value,
        narrow_key,
        narrow_value,
        gain.reshape(1, width),
        local_cos,
        local_sin,
        base_cos,
        base_sin,
    )


def body(
    latent,
    rope_key,
    wide_query,
    narrow_query,
    wide_key_weight,
    wide_value_weight,
    narrow_key_weight,
    narrow_value_weight,
    latent_norm_scale,
    out_wide,
    out_narrow,
    residual,
    ffn_gain,
    shared_gate,
    shared_up,
    shared_down,
    expert_gate,
    expert_up,
    expert_down,
    routes,
    route_weights,
):
    mix = attention(
        latent,
        rope_key,
        wide_query,
        narrow_query,
        wide_key_weight,
        wide_value_weight,
        narrow_key_weight,
        narrow_value_weight,
        latent_norm_scale,
    )
    wide_cols = out_wide.shape[0]
    wide_mix, narrow_mix = mix[:, :wide_cols], mix[:, wide_cols:]
    projected = summed_on_arrival(
        (
            jnp.dot(wide_mix, out_wide, preferred_element_type=jnp.float32)
            + jnp.dot(narrow_mix, out_narrow, preferred_element_type=jnp.float32)
        ).astype(jnp.bfloat16),
        "tp",
        0,
    )
    stream = (residual.astype(jnp.float32) + projected).astype(jnp.bfloat16)
    normed = rms_scale(stream.astype(jnp.float32), ffn_gain).astype(jnp.bfloat16)
    piece = lax.all_gather(normed, "tp", axis=0, tiled=True)
    gate_part = jnp.dot(piece, shared_gate, preferred_element_type=jnp.float32)
    up_part = jnp.dot(piece, shared_up, preferred_element_type=jnp.float32)
    active = (jax.nn.silu(gate_part) * up_part).astype(jnp.bfloat16)
    shared_terms = jnp.dot(active, shared_down, preferred_element_type=jnp.float32)
    shared = lax.psum_scatter(
        shared_terms.astype(jnp.bfloat16), "tp", scatter_dimension=0, tiled=True
    ).astype(jnp.float32)
    rows_here, top_count = routes.shape
    local_experts = expert_gate.shape[0]
    experts_all = local_experts * lax.axis_size(("sp", "tp"))
    capacity = max(2, 2 * top_count * rows_here // experts_all)
    model_width = normed.shape[1]
    flat_routes = routes.reshape(-1)
    assigned = flat_routes.shape[0]
    choose = (flat_routes[:, None] == jnp.arange(experts_all, dtype=jnp.int32)[None, :]).astype(
        jnp.float32
    )
    lower_mask = (jnp.arange(assigned)[:, None] > jnp.arange(assigned)[None, :]).astype(jnp.float32)
    earlier = jnp.dot(lower_mask, choose, precision=lax.Precision.HIGHEST)
    slots = jnp.sum(earlier * choose, axis=1).astype(jnp.int32)
    target = flat_routes * capacity + slots
    send_map = jnp.any(
        target.reshape(rows_here, top_count)[None, :, :]
        == jnp.arange(experts_all * capacity, dtype=jnp.int32)[:, None, None],
        axis=2,
    ).astype(jnp.bfloat16)
    outgoing = jnp.dot(send_map, normed, preferred_element_type=jnp.float32).astype(jnp.bfloat16)
    incoming = lax.all_to_all(outgoing, ("sp", "tp"), split_axis=0, concat_axis=0, tiled=True)
    finished = []
    for x in range(local_experts):
        rows = incoming
        if local_experts > 1:
            rows = incoming.reshape(-1, local_experts, capacity, model_width)[:, x].reshape(-1, model_width)
        gate_part = jnp.dot(rows, expert_gate[x], preferred_element_type=jnp.float32)
        up_part = jnp.dot(rows, expert_up[x], preferred_element_type=jnp.float32)
        active = (jax.nn.silu(gate_part) * up_part).astype(jnp.bfloat16)
        finished.append(
            jnp.dot(active, expert_down[x], preferred_element_type=jnp.float32).astype(jnp.bfloat16)
        )
    if local_experts > 1:
        stacked = jnp.stack([f.reshape(-1, capacity, model_width) for f in finished], axis=1)
        finished = [stacked.reshape(-1, model_width)]
    returned = lax.all_to_all(finished[0], ("sp", "tp"), split_axis=0, concat_axis=0, tiled=True)
    chosen = target.reshape(rows_here, top_count)
    places = jnp.arange(experts_all * capacity, dtype=jnp.int32)[None, :]
    routed = jnp.zeros((rows_here, model_width), jnp.float32)
    for c in range(top_count):
        pick = (chosen[:, c : c + 1] == places).astype(jnp.bfloat16)
        routed = routed + route_weights[:, c : c + 1] * jnp.dot(
            pick, returned, preferred_element_type=jnp.float32
        )
    return (stream.astype(jnp.float32) + shared + routed).astype(jnp.bfloat16)


def solution(mesh):
    placed = (
        P(("grp", "sp"), None),
        P(("grp", "sp"), None),
        P(("grp", "sp"), "tp"),
        P(("grp", "sp"), "tp"),
        P(None, "tp"),
        P(None, "tp"),
        P(None, "tp"),
        P(None, "tp"),
        P(),
        P("tp", None),
        P("tp", None),
        P(("grp", "sp", "tp"), None),
        P(),
        P(None, "tp"),
        P(None, "tp"),
        P("tp", None),
        P(("sp", "tp"), None, None),
        P(("sp", "tp"), None, None),
        P(("sp", "tp"), None, None),
        P(("grp", "sp", "tp"), None),
        P(("grp", "sp", "tp"), None),
    )
    return jax.shard_map(
        body, mesh=mesh, in_specs=placed, out_specs=P(("grp", "sp", "tp"), None), check_vma=False
    )
```

```python
import functools

import jax
import jax.numpy as jnp
import numpy as np
from jax import lax
from jax.experimental import pallas as pl
from jax.experimental.pallas import tpu as pltpu
from jax.sharding import PartitionSpec as P

ROPE = 64
WIDE_HEAD_SIZE = 128
NARROW_HEAD_SIZE = 64
LANES = 128


EPS = 1e-06
ROPE_BASE = 10000.0
NEG_FILL = -1e30
LOG2E = 1.4426950408889634


def rms_scale(values, gain):
    return values * lax.rsqrt(jnp.mean(values * values, axis=-1, keepdims=True) + EPS) * gain


def angle_tables(positions):
    half = ROPE // 2
    inverse = ROPE_BASE ** (-np.arange(half) * 2.0 / ROPE)
    angles = positions[:, None] * np.concatenate([inverse, inverse])[None, :]
    pad = ((0, 0), (0, LANES - ROPE))
    return (
        np.pad(np.cos(angles), pad).astype(np.float32),
        np.pad(np.sin(angles), pad).astype(np.float32),
    )


def attention_kernel(
    n_sp,
    n_tp,
    latent_hbm,
    rope_key_hbm,
    wide_query_hbm,
    narrow_query_hbm,
    wide_key_hbm,
    wide_value_hbm,
    narrow_key_hbm,
    narrow_value_hbm,
    gain_hbm,
    local_cos_hbm,
    local_sin_hbm,
    base_cos_hbm,
    base_sin_hbm,
    out_ref,
    latent_ref,
    rope_key_ref,
    wide_query_ref,
    narrow_query_ref,
    wide_key_ref,
    wide_value_ref,
    gain_ref,
    local_cos_ref,
    local_sin_ref,
    base_cos_ref,
    base_sin_ref,
    rows_buf,
    queries,
    narrow_weight,
    top,
    mixed,
    fetch,
    z_send,
    z_recv,
    x_send,
    x_recv,
    d_send,
    d_recv,
):
    tokens, width = latent_hbm.shape
    quarter = tokens // n_tp
    zn = n_sp // 2
    steps_up = zn // 2
    steps_down = zn - 1 - steps_up
    me = lax.axis_index("sp")
    x = lax.axis_index("tp")
    z = me // 2
    core = lax.rem(me, 2)
    right = lax.rem(x + 1, n_tp)
    left = lax.rem(x + n_tp - 1, n_tp)
    up = lax.rem(z + 1, zn)
    down = lax.rem(z + zn - 1, zn)
    partner = z * 2 + 1 - core

    fetches = [
        pltpu.make_async_copy(source, target, fetch.at[i])
        for i, (source, target) in enumerate(
            (
                (latent_hbm, latent_ref),
                (rope_key_hbm, rope_key_ref),
                (gain_hbm, gain_ref),
                (local_cos_hbm, local_cos_ref),
                (local_sin_hbm, local_sin_ref),
                (base_cos_hbm, base_cos_ref),
                (base_sin_hbm, base_sin_ref),
                (wide_query_hbm, wide_query_ref),
                (narrow_query_hbm, narrow_query_ref),
                (wide_key_hbm, wide_key_ref),
                (wide_value_hbm, wide_value_ref),
                (narrow_key_hbm, narrow_weight.at[:, pl.ds(0, LANES)]),
                (narrow_value_hbm, narrow_weight.at[:, pl.ds(LANES, LANES)]),
            )
        )
    ]
    for copy in fetches:
        copy.start()

    barrier = pltpu.get_barrier_semaphore()
    for place in ({"sp": up * 2 + core}, {"sp": down * 2 + core}, {"sp": partner}, {"tp": left}, {"tp": right}):
        pl.semaphore_signal(barrier, inc=1, device_id=place, device_id_type=pl.DeviceIdType.MESH)

    for copy in fetches:
        copy.wait()
    lane = lax.broadcasted_iota(jnp.int32, (tokens, LANES), 1)
    low = lane < ROPE
    lc, ls = local_cos_ref[...], local_sin_ref[...]
    bc, bs = base_cos_ref[pl.ds(me, 1), :], base_sin_ref[pl.ds(me, 1), :]
    cosine = lc * bc - ls * bs
    sine = jnp.where(lane < ROPE // 2, -1.0, 1.0) * (ls * bc + lc * bs)

    def turn(v):
        other = jnp.where(
            lane < ROPE // 2, pltpu.roll(v, LANES - ROPE // 2, 1), pltpu.roll(v, ROPE // 2, 1)
        )
        return (v * cosine + other * sine).astype(jnp.bfloat16)

    lat = latent_ref[...].astype(jnp.float32)
    normed = rms_scale(lat, gain_ref[...]).astype(jnp.bfloat16)
    rope = rope_key_ref[...].astype(jnp.float32)
    turned = turn(jnp.concatenate([rope, jnp.zeros_like(rope)], axis=1))
    for q in range(n_tp):
        rows_buf[me, q, :, :width] = normed[q * quarter : (q + 1) * quarter]
        rows_buf[me, q, :, width:] = turned[q * quarter : (q + 1) * quarter]

    t1 = wide_query_ref[:, LANES : 2 * LANES].astype(jnp.float32)
    t2 = wide_query_ref[:, 2 * LANES :].astype(jnp.float32)
    n0 = narrow_query_ref[:, :LANES].astype(jnp.float32)
    n1 = narrow_query_ref[:, LANES:].astype(jnp.float32)
    half = LANES // 2
    queries[0, :, :LANES] = wide_query_ref[:, :LANES]
    queries[0, :, LANES:] = turn(t1)
    queries[1, :, :LANES] = pltpu.roll(jnp.where(low, t2, t1), half, 1).astype(jnp.bfloat16)
    queries[1, :, LANES:] = turn(pltpu.roll(t2, half, 1))
    queries[2, :, :LANES] = jnp.where(low, n0, 0.0).astype(jnp.bfloat16)
    queries[2, :, LANES:] = turn(pltpu.roll(n0, half, 1))
    queries[3, :, :LANES] = pltpu.roll(jnp.where(low, n1, 0.0), half, 1).astype(jnp.bfloat16)
    queries[3, :, LANES:] = turn(pltpu.roll(n1, half, 1))
    top[...] = jnp.full(top.shape, NEG_FILL, jnp.float32)
    mixed[...] = jnp.zeros(mixed.shape, jnp.float32)
    pl.semaphore_wait(barrier, 5)

    def along_z(d, k, j):
        block = jnp.where(d == 0, z - k + zn, z + k) % zn
        target = jnp.where(d == 0, up, down)
        q = lax.rem(x + j, n_tp)
        spot = rows_buf.at[block * 2 + core, q]
        return pltpu.make_async_remote_copy(
            src_ref=spot,
            dst_ref=spot,
            send_sem=z_send.at[d, k, j],
            recv_sem=z_recv.at[d, k + 1, j],
            device_id={"sp": target * 2 + core},
            device_id_type=pl.DeviceIdType.MESH,
        )

    def along_x(d, k, j):
        block = jnp.where(d == 0, z - k + zn, z + k) % zn
        q = lax.rem(x + j, n_tp)
        spot = rows_buf.at[block * 2 + core, q]
        return pltpu.make_async_remote_copy(
            src_ref=spot,
            dst_ref=spot,
            send_sem=x_send.at[d, k, j],
            recv_sem=x_recv.at[d, k, j],
            device_id={"tp": right if j == 0 else left},
            device_id_type=pl.DeviceIdType.MESH,
        )

    def to_partner(d, k):
        block = jnp.where(d == 0, z - k + zn, z + k) % zn
        spot = rows_buf.at[block * 2 + core]
        return pltpu.make_async_remote_copy(
            src_ref=spot,
            dst_ref=spot,
            send_sem=d_send.at[d, k],
            recv_sem=d_recv.at[d, k],
            device_id={"sp": partner},
            device_id_type=pl.DeviceIdType.MESH,
        )

    def arrives(d, k):
        going_up = (k <= z) & (k <= steps_up)
        going_down = ((z + k) % zn < steps_down) & (k <= steps_down)
        return jnp.where(d == 0, going_up, going_down)

    def goes_on(d, k):
        going_up = (k <= z) & (k < steps_up) & (z + 1 < zn)
        going_down = ((z + k) % zn < steps_down) & (k < steps_down)
        return jnp.where(d == 0, going_up, going_down)

    def seen(d, k):
        going_up = (k <= z) & (k <= steps_up)
        going_down = (z + k >= zn) & (z + k - zn < steps_down) & (k <= steps_down)
        return (k >= 1) & jnp.where(d == 0, going_up, going_down)

    wide_factor = (WIDE_HEAD_SIZE + ROPE) ** (-0.5) * LOG2E
    narrow_factor = (NARROW_HEAD_SIZE + ROPE) ** (-0.5) * LOG2E

    def attend(plane, own):
        rows = rows_buf[pl.ds(plane * 2, 2)].reshape(2 * tokens, width + LANES)
        latents, turned_rows = rows[:, :width], rows[:, width:]
        keys = 2 * tokens
        ones = jnp.ones((keys, LANES), jnp.bfloat16)

        def up_from(weight):
            return jnp.dot(latents, weight[...], preferred_element_type=jnp.float32).astype(jnp.bfloat16)

        wide_k, wide_v, narrow = up_from(wide_key_ref), up_from(wide_value_ref), up_from(narrow_weight)
        narrow_k = jnp.concatenate([narrow[:, :LANES], turned_rows], axis=1)
        narrow_v = jnp.concatenate([narrow[:, LANES:], ones], axis=1)
        if own:
            gap = lax.broadcasted_iota(jnp.int32, (tokens, keys), 1) - lax.broadcasted_iota(
                jnp.int32, (tokens, keys), 0
            )
            visible = gap <= core * tokens
        for h in range(4):
            if h < 2:
                at = slice(h * LANES, (h + 1) * LANES)
                k_h = jnp.concatenate([wide_k[:, at], turned_rows], axis=1)
                v_h = jnp.concatenate([wide_v[:, at], ones], axis=1)
            else:
                k_h, v_h = narrow_k, narrow_v
            scores = lax.dot_general(
                queries[h], k_h, (((1,), (1,)), ((), ())), preferred_element_type=jnp.float32
            ) * (wide_factor if h < 2 else narrow_factor)
            if own:
                scores = jnp.where(visible, scores, NEG_FILL)
            old = top[h]
            new = jnp.maximum(old, jnp.max(scores, axis=1, keepdims=True))
            top[h] = new
            weights = jnp.exp2(scores - jnp.concatenate([new] * (keys // LANES), axis=1)).astype(jnp.bfloat16)
            fading = jnp.exp2(old - new)
            mixed[h] = mixed[h] * jnp.concatenate([fading, fading], axis=1) + jnp.dot(
                weights, v_h, preferred_element_type=jnp.float32
            )

    to_partner(0, 0).start()
    for d in range(2):

        @pl.when(goes_on(d, 0))
        def _():
            for j in range(2):
                along_z(d, 0, j).start()

    to_partner(0, 0).wait_recv()

    attend(z, True)

    def one_step(k, carry):
        def forward(d, c):
            @pl.when(arrives(d, k))
            def _():
                for j in range(2):
                    along_z(d, k - 1, j).wait_recv()

            @pl.when(goes_on(d, k))
            def _():
                for j in range(2):
                    along_z(d, k, j).start()

            @pl.when(seen(d, k))
            def _():
                for j in range(2):
                    along_x(d, k, j).start()

            @pl.when(seen(d, k - 1))
            def _():
                for j in range(2):
                    along_x(d, k - 1, j).wait_recv()
                to_partner(d, k - 1).start()

            return c

        lax.fori_loop(0, 2, forward, 0)

        def work(d, c):
            @pl.when(seen(d, k - 2))
            def _():
                to_partner(d, k - 2).wait_recv()
                attend(jnp.where(d == 0, z - k + 2, z + k - 2 - zn), False)

            return c

        lax.fori_loop(0, 2, work, 0)
        return carry

    lax.fori_loop(1, steps_up + 3, one_step, 0)

    to_partner(0, 0).wait_send()

    def settle(k, carry):
        def both(d, c):
            @pl.when(goes_on(d, k))
            def _():
                for j in range(2):
                    along_z(d, k, j).wait_send()

            @pl.when(seen(d, k))
            def _():
                for j in range(2):
                    along_x(d, k, j).wait_send()
                to_partner(d, k).wait_send()

            return c

        return lax.fori_loop(0, 2, both, carry)

    lax.fori_loop(0, steps_up + 1, settle, 0)

    for h in range(2):
        out_ref[:, h * LANES : (h + 1) * LANES] = (mixed[h, :, :LANES] / mixed[h, :, LANES:]).astype(
            out_ref.dtype
        )
    out_ref[:, 2 * LANES :] = jnp.where(
        low, mixed[2, :, :LANES] / mixed[2, :, LANES:], mixed[3, :, :LANES] / mixed[3, :, LANES:]
    ).astype(out_ref.dtype)


def attention(
    latent, rope_key, wide_query, narrow_query, wide_key, wide_value, narrow_key, narrow_value, gain
):
    tokens, width = latent.shape
    n_sp, n_tp = lax.axis_size("sp"), lax.axis_size("tp")
    zn = n_sp // 2
    assert n_sp % 4 == 0 and n_tp == 4 and wide_query.shape[1] == 3 * LANES
    assert narrow_query.shape[1] == 2 * LANES and zn >= 4
    local_cos, local_sin = angle_tables(np.arange(tokens, dtype=np.float64))
    base_cos, base_sin = angle_tables(np.arange(n_sp, dtype=np.float64) * tokens)
    hops = zn // 2 + 1
    dma = pltpu.SemaphoreType.DMA
    vmem = pl.BlockSpec(memory_space=pltpu.VMEM)
    return pl.pallas_call(
        functools.partial(attention_kernel, n_sp, n_tp),
        out_shape=jax.ShapeDtypeStruct((tokens, 3 * LANES), jnp.bfloat16),
        in_specs=[pl.BlockSpec(memory_space=pltpu.HBM)] * 13,
        out_specs=vmem,
        scratch_shapes=[
            pltpu.VMEM(latent.shape, jnp.bfloat16),
            pltpu.VMEM(rope_key.shape, jnp.bfloat16),
            pltpu.VMEM(wide_query.shape, jnp.bfloat16),
            pltpu.VMEM(narrow_query.shape, jnp.bfloat16),
            pltpu.VMEM(wide_key.shape, jnp.bfloat16),
            pltpu.VMEM(wide_value.shape, jnp.bfloat16),
            pltpu.VMEM((1, width), jnp.float32),
            pltpu.VMEM(local_cos.shape, jnp.float32),
            pltpu.VMEM(local_sin.shape, jnp.float32),
            pltpu.VMEM(base_cos.shape, jnp.float32),
            pltpu.VMEM(base_sin.shape, jnp.float32),
            pltpu.VMEM((n_sp, n_tp, tokens // n_tp, width + LANES), jnp.bfloat16),
            pltpu.VMEM((4, tokens, 2 * LANES), jnp.bfloat16),
            pltpu.VMEM((width, 2 * LANES), jnp.bfloat16),
            pltpu.VMEM((4, tokens, LANES), jnp.float32),
            pltpu.VMEM((4, tokens, 2 * LANES), jnp.float32),
            dma((13,)),
            dma((2, hops, 2)),
            dma((2, hops + 1, 2)),
            dma((2, hops, 2)),
            dma((2, hops, 2)),
            dma((2, hops)),
            dma((2, hops)),
        ],
        compiler_params=pltpu.CompilerParams(
            collective_id=0, has_side_effects=True, vmem_limit_bytes=48 * 1024 * 1024
        ),
    )(
        latent,
        rope_key,
        wide_query,
        narrow_query,
        wide_key,
        wide_value,
        narrow_key,
        narrow_value,
        gain.reshape(1, width),
        local_cos,
        local_sin,
        base_cos,
        base_sin,
    )


DELTAS = ((0, 1, -1, 4, -4, 5, -5, 8), (2, -2, 3, -3, 6, -6, 7, -7))
COLUMNS = 1024


def silu(v):
    return v / (1.0 + jnp.exp(-v))


def experts_kernel(
    n_sp,
    n_tp,
    mix_ref,
    send_map_ref,
    pick_ref,
    weight_ref,
    out_wide_hbm,
    out_narrow_hbm,
    residual_hbm,
    gain_hbm,
    shared_gate_hbm,
    shared_up_hbm,
    shared_down_hbm,
    expert_gate_hbm,
    expert_up_hbm,
    expert_down_hbm,
    out_ref,
    out_weight,
    residual_ref,
    gain_ref,
    shared_in,
    shared_down,
    expert_gate,
    expert_up,
    expert_down,
    part,
    opposite,
    summed,
    landed,
    stream,
    gathered,
    outgoing,
    first_recv,
    first_relay,
    second_send,
    second_recv,
    finished,
    back_recv,
    back_send,
    back_relay,
    returned,
    shared_send,
    shared_recv,
    fetch,
    send_sems,
    recv_sems,
):
    rows, depth = residual_hbm.shape
    half = depth // 2
    zn = n_sp // 2
    lanes = 2 * n_tp
    piece = outgoing.shape[1]
    wide_rows = out_wide_hbm.shape[0]
    ff = shared_gate_hbm.shape[1]
    me = lax.axis_index("sp")
    x = lax.axis_index("tp")
    z = me // 2
    core = lax.rem(me, 2)
    lane = core * n_tp + x

    def at_plane(delta):
        return lax.rem(z + (delta + zn), zn)

    def on_plane(delta):
        return {"sp": at_plane(delta) * 2 + core}

    def along_x(dx):
        return {"tp": lax.rem(x + (dx + n_tp), n_tp)}

    def in_plane(dc, dx):
        other = 1 - core if dc else core
        return {"sp": z * 2 + other, "tp": lax.rem(x + (dx + n_tp), n_tp)}

    relative = [(dc, dx) for dc in range(2) for dx in range(n_tp)]

    taken = [0]

    def remote(source, target, place):
        i = taken[0]
        taken[0] += 1
        return pltpu.make_async_remote_copy(
            src_ref=source,
            dst_ref=target,
            send_sem=send_sems.at[i],
            recv_sem=recv_sems.at[i],
            device_id=place,
            device_id_type=pl.DeviceIdType.MESH,
        )

    barrier = pltpu.get_barrier_semaphore()
    greeted = [on_plane(d) for d in range(1, zn)] + [in_plane(dc, dx) for dc, dx in relative[1:]]
    for place in greeted:
        pl.semaphore_signal(barrier, inc=1, device_id=place, device_id_type=pl.DeviceIdType.MESH)

    fetches = [
        pltpu.make_async_copy(source, target, fetch.at[i])
        for i, (source, target) in enumerate(
            (
                (out_wide_hbm, out_weight.at[pl.ds(0, wide_rows)]),
                (out_narrow_hbm, out_weight.at[pl.ds(wide_rows, out_narrow_hbm.shape[0])]),
                (residual_hbm, residual_ref),
                (gain_hbm, gain_ref),
                (shared_gate_hbm, shared_in.at[:, pl.ds(0, ff)]),
                (shared_up_hbm, shared_in.at[:, pl.ds(ff, ff)]),
                (shared_down_hbm, shared_down),
                (expert_gate_hbm.at[0], expert_gate),
                (expert_up_hbm.at[0], expert_up),
                (expert_down_hbm.at[0], expert_down),
            )
        )
    ]
    for copy in fetches:
        copy.start()

    def chunks():
        return [pl.ds(n, COLUMNS) for n in range(0, depth, COLUMNS)]

    def project(dx):
        q = pl.multiple_of(lax.rem(x + dx, n_tp) * rows, rows)
        mine = mix_ref[pl.ds(q, rows), :]
        for cols in chunks():
            part[dx, :, cols] = jnp.dot(
                mine, out_weight[:, cols], preferred_element_type=jnp.float32
            ).astype(jnp.bfloat16)

    lower, upper = pl.ds(0, half), pl.ds(half, half)
    fetches[0].wait()
    fetches[1].wait()
    project(2)
    pl.semaphore_wait(barrier, len(greeted))
    over_right = remote(part.at[2, :, lower], opposite.at[0], along_x(1))
    over_left = remote(part.at[2, :, upper], opposite.at[1], along_x(-1))
    over_right.start()
    over_left.start()
    project(1)
    straight_right = remote(part.at[1, :, upper], landed.at[0, 1], along_x(1))
    straight_right.start()
    project(3)
    straight_left = remote(part.at[3, :, lower], landed.at[1, 0], along_x(-1))
    straight_left.start()
    project(0)
    over_right.wait_recv()
    summed[0] = (part[1, :, lower].astype(jnp.float32) + opposite[0].astype(jnp.float32)).astype(jnp.bfloat16)
    joined_right = remote(summed.at[0], landed.at[0, 0], along_x(1))
    joined_right.start()
    over_left.wait_recv()
    summed[1] = (part[3, :, upper].astype(jnp.float32) + opposite[1].astype(jnp.float32)).astype(jnp.bfloat16)
    joined_left = remote(summed.at[1], landed.at[1, 1], along_x(-1))
    joined_left.start()
    fetches[2].wait()
    fetches[3].wait()
    for copy in (straight_right, straight_left, joined_right, joined_left):
        copy.wait_recv()
    for h, cols in enumerate((lower, upper)):
        stream[:, cols] = (
            residual_ref[:, cols].astype(jnp.float32)
            + part[0, :, cols].astype(jnp.float32)
            + landed[0, h].astype(jnp.float32)
            + landed[1, h].astype(jnp.float32)
        ).astype(jnp.bfloat16)
    gathered[0] = rms_scale(stream[...].astype(jnp.float32), gain_ref[...]).astype(jnp.bfloat16)

    for cols in chunks():
        outgoing[:, :, cols] = (
            jnp.dot(send_map_ref[...], gathered[0, :, cols], preferred_element_type=jnp.float32)
            .astype(jnp.bfloat16)
            .reshape(zn, piece, COLUMNS)
        )
    sent = [over_right, over_left, straight_right, straight_left, joined_right, joined_left]
    far = at_plane(8)
    relay_up = remote(outgoing.at[far, :, lower], first_relay.at[0], on_plane(4))
    relay_down = remote(outgoing.at[far, :, upper], first_relay.at[1], on_plane(-4))
    relay_up.start()
    relay_down.start()
    first = [{}, {}]
    for ch in range(2):
        for j, delta in enumerate(DELTAS[ch]):
            if delta in (0, 8):
                continue
            first[ch][j] = remote(outgoing.at[at_plane(delta)], first_recv.at[ch, j], on_plane(delta))
            first[ch][j].start()
        if ch == 0:
            spread = [remote(gathered.at[0], gathered.at[dx], along_x(dx)) for dx in (1, 3, 2)]
            for copy in spread:
                copy.start()
    first_recv[0, 0] = outgoing[z]
    far_slot = DELTAS[0].index(8)
    onward_up = remote(first_relay.at[0], first_recv.at[0, far_slot, :, lower], on_plane(4))
    onward_down = remote(first_relay.at[1], first_recv.at[0, far_slot, :, upper], on_plane(-4))
    relay_up.wait_recv()
    onward_up.start()
    relay_down.wait_recv()
    onward_down.start()
    sent += [relay_up, relay_down, onward_up, onward_down] + spread
    sent += list(first[0].values()) + list(first[1].values())

    for copy in fetches[4:]:
        copy.wait()
    for copy in spread:
        copy.wait_recv()
    every = gathered[...].reshape(n_tp * rows, depth)
    both = jnp.dot(every, shared_in[...], preferred_element_type=jnp.float32)
    act = (silu(both[:, :ff]) * both[:, ff:]).astype(jnp.bfloat16)
    for cols in chunks():
        shared_send[:, :, cols] = (
            jnp.dot(act, shared_down[:, cols], preferred_element_type=jnp.float32)
            .astype(jnp.bfloat16)
            .reshape(n_tp, rows, COLUMNS)
        )
    shared_back = [remote(shared_send.at[dx], shared_recv.at[dx - 1], along_x(-dx)) for dx in range(1, n_tp)]
    for copy in shared_back:
        copy.start()
    sent += shared_back

    count = lanes * piece
    o = lax.broadcasted_iota(jnp.int32, (count, count), 0)
    i = lax.broadcasted_iota(jnp.int32, (count, count), 1)
    swap = jnp.where(
        (o // piece == (i % piece) // 2) & ((o % piece) // 2 == i // piece) & (o % 2 == i % 2), 1.0, 0.0
    ).astype(jnp.bfloat16)

    def swapped(source, target, ch):
        for cols in chunks():
            target[ch, :, :, cols] = (
                jnp.dot(
                    swap, source[ch, :, :, cols].reshape(count, COLUMNS), preferred_element_type=jnp.float32
                )
                .astype(jnp.bfloat16)
                .reshape(lanes, piece, COLUMNS)
            )

    def to_lanes(ch):
        swapped(first_recv, second_send, ch)
        copies = []
        for r, (dc, dx) in enumerate(relative):
            if r == 0:
                continue
            other = (1 - core if dc else core) * n_tp + lax.rem(x + dx, n_tp)
            copies.append(remote(second_send.at[ch, other], second_recv.at[ch, r], in_plane(dc, dx)))
            copies[-1].start()
        second_recv[ch, 0] = second_send[ch, lane]
        return copies

    def run_expert(ch):
        taken_in = second_recv[ch].reshape(count, depth)
        gate = jnp.dot(taken_in, expert_gate[...], preferred_element_type=jnp.float32)
        lifted = jnp.dot(taken_in, expert_up[...], preferred_element_type=jnp.float32)
        active = (silu(gate) * lifted).astype(jnp.bfloat16)
        for cols in chunks():
            finished[ch, :, :, cols] = (
                jnp.dot(active, expert_down[:, cols], preferred_element_type=jnp.float32)
                .astype(jnp.bfloat16)
                .reshape(lanes, piece, COLUMNS)
            )
        copies = []
        for r, (dc, dx) in enumerate(relative):
            if r == 0:
                continue
            copies.append(remote(finished.at[ch, r], back_recv.at[ch, lane], in_plane(dc, -dx)))
            copies[-1].start()
        back_recv[ch, lane] = finished[ch, 0]
        return copies

    def home(ch):
        swapped(back_recv, back_send, ch)
        copies = []
        relays = []
        for j, delta in enumerate(DELTAS[ch]):
            if delta == 8:
                relays = [
                    remote(back_send.at[ch, j, :, lower], back_relay.at[0], on_plane(4)),
                    remote(back_send.at[ch, j, :, upper], back_relay.at[1], on_plane(-4)),
                ]
                for copy in relays:
                    copy.start()
        for j, delta in enumerate(DELTAS[ch]):
            if delta == 0:
                returned[z] = back_send[ch, j]
            elif delta != 8:
                copies.append(remote(back_send.at[ch, j], returned.at[z], on_plane(-delta)))
                copies[-1].start()
        return copies, relays

    for copy in list(first[0].values()) + [onward_up, onward_down]:
        copy.wait_recv()
    lane_copies = to_lanes(0)
    for copy in lane_copies:
        copy.wait_recv()
    back_copies = run_expert(0)
    for copy in back_copies:
        copy.wait_recv()
    home_copies, relays = home(0)
    sent += lane_copies + back_copies + home_copies + relays

    for copy in first[1].values():
        copy.wait_recv()
    lane_copies = to_lanes(1)
    relays[0].wait_recv()
    last_up = remote(back_relay.at[0], returned.at[at_plane(-4), :, lower], on_plane(4))
    last_up.start()
    relays[1].wait_recv()
    last_down = remote(back_relay.at[1], returned.at[at_plane(4), :, upper], on_plane(-4))
    last_down.start()
    for copy in lane_copies:
        copy.wait_recv()
    back_copies = run_expert(1)
    for copy in back_copies:
        copy.wait_recv()
    more_home, _ = home(1)
    sent += lane_copies + back_copies + more_home + [last_up, last_down]

    for copy in shared_back:
        copy.wait_recv()
    for copy in home_copies + more_home + [last_up, last_down]:
        copy.wait_recv()
    for cols in chunks():
        total = stream[:, cols].astype(jnp.float32) + shared_send[0, :, cols].astype(jnp.float32)
        for dx in range(n_tp - 1):
            total = total + shared_recv[dx, :, cols].astype(jnp.float32)
        results = returned[:, :, cols].reshape(zn * piece, COLUMNS)
        for c in range(pick_ref.shape[0]):
            total = total + weight_ref[:, c : c + 1] * jnp.dot(
                pick_ref[c], results, preferred_element_type=jnp.float32
            )
        out_ref[:, cols] = total.astype(out_ref.dtype)
    for copy in sent:
        copy.wait_send()


def projected_experts(
    mix,
    send_map,
    pick,
    route_weights,
    out_wide,
    out_narrow,
    residual,
    gain,
    shared_gate,
    shared_up,
    shared_down,
    expert_gate,
    expert_up,
    expert_down,
):
    rows, depth = residual.shape
    n_sp, n_tp = lax.axis_size("sp"), lax.axis_size("tp")
    zn, lanes = n_sp // 2, 2 * n_tp
    piece = send_map.shape[0] // zn
    ff = shared_gate.shape[1]
    assert zn == 16 and n_tp == 4 and piece == 2 * lanes and expert_gate.shape[0] == 1
    vmem, hbm = pl.BlockSpec(memory_space=pltpu.VMEM), pl.BlockSpec(memory_space=pltpu.HBM)
    bf16 = jnp.bfloat16
    chunk = (2, lanes, piece, depth)
    dma = pltpu.SemaphoreType.DMA
    return pl.pallas_call(
        functools.partial(experts_kernel, n_sp, n_tp),
        out_shape=jax.ShapeDtypeStruct((rows, depth), bf16),
        in_specs=[vmem] * 4 + [hbm] * 10,
        out_specs=vmem,
        scratch_shapes=[
            pltpu.VMEM((out_wide.shape[0] + out_narrow.shape[0], depth), bf16),
            pltpu.VMEM((rows, depth), bf16),
            pltpu.VMEM((1, depth), jnp.float32),
            pltpu.VMEM((depth, 2 * ff), bf16),
            pltpu.VMEM(shared_down.shape, bf16),
            pltpu.VMEM(expert_gate.shape[1:], bf16),
            pltpu.VMEM(expert_up.shape[1:], bf16),
            pltpu.VMEM(expert_down.shape[1:], bf16),
            pltpu.VMEM((n_tp, rows, depth), bf16),
            pltpu.VMEM((2, rows, depth // 2), bf16),
            pltpu.VMEM((2, rows, depth // 2), bf16),
            pltpu.VMEM((2, 2, rows, depth // 2), bf16),
            pltpu.VMEM((rows, depth), bf16),
            pltpu.VMEM((n_tp, rows, depth), bf16),
            pltpu.VMEM((zn, piece, depth), bf16),
            pltpu.VMEM(chunk, bf16),
            pltpu.VMEM((2, piece, depth // 2), bf16),
            pltpu.VMEM(chunk, bf16),
            pltpu.VMEM(chunk, bf16),
            pltpu.VMEM(chunk, bf16),
            pltpu.VMEM(chunk, bf16),
            pltpu.VMEM(chunk, bf16),
            pltpu.VMEM((2, piece, depth // 2), bf16),
            pltpu.VMEM((zn, piece, depth), bf16),
            pltpu.VMEM((n_tp, rows, depth), bf16),
            pltpu.VMEM((n_tp - 1, rows, depth), bf16),
            dma((10,)),
            dma((80,)),
            dma((80,)),
        ],
        compiler_params=pltpu.CompilerParams(
            collective_id=1, has_side_effects=True, vmem_limit_bytes=56 * 1024 * 1024
        ),
    )(
        mix,
        send_map,
        pick,
        route_weights,
        out_wide,
        out_narrow,
        residual,
        gain.reshape(1, depth),
        shared_gate,
        shared_up,
        shared_down,
        expert_gate,
        expert_up,
        expert_down,
    )


def body(
    latent,
    rope_key,
    wide_query,
    narrow_query,
    wide_key_weight,
    wide_value_weight,
    narrow_key_weight,
    narrow_value_weight,
    latent_norm_scale,
    out_wide,
    out_narrow,
    residual,
    ffn_gain,
    shared_gate,
    shared_up,
    shared_down,
    expert_gate,
    expert_up,
    expert_down,
    routes,
    route_weights,
):
    mix = attention(
        latent,
        rope_key,
        wide_query,
        narrow_query,
        wide_key_weight,
        wide_value_weight,
        narrow_key_weight,
        narrow_value_weight,
        latent_norm_scale,
    )
    rows_here, top_count = routes.shape
    local_experts = expert_gate.shape[0]
    experts_all = local_experts * lax.axis_size(("sp", "tp"))
    capacity = max(2, 2 * top_count * rows_here // experts_all)
    flat_routes = routes.reshape(-1)
    assigned = flat_routes.shape[0]
    choose = (flat_routes[:, None] == jnp.arange(experts_all, dtype=jnp.int32)[None, :]).astype(
        jnp.float32
    )
    lower_mask = (jnp.arange(assigned)[:, None] > jnp.arange(assigned)[None, :]).astype(jnp.float32)
    earlier = jnp.dot(lower_mask, choose, precision=lax.Precision.HIGHEST)
    slots = jnp.sum(earlier * choose, axis=1).astype(jnp.int32)
    target = flat_routes * capacity + slots
    send_map = jnp.any(
        target.reshape(rows_here, top_count)[None, :, :]
        == jnp.arange(experts_all * capacity, dtype=jnp.int32)[:, None, None],
        axis=2,
    ).astype(jnp.bfloat16)
    chosen = target.reshape(rows_here, top_count)
    places = jnp.arange(experts_all * capacity, dtype=jnp.int32)
    pick = (chosen.T[:, :, None] == places[None, None, :]).astype(jnp.bfloat16)
    return projected_experts(
        mix,
        send_map,
        pick,
        route_weights,
        out_wide,
        out_narrow,
        residual,
        ffn_gain,
        shared_gate,
        shared_up,
        shared_down,
        expert_gate,
        expert_up,
        expert_down,
    )


def solution(mesh):
    placed = (
        P(("grp", "sp"), None),
        P(("grp", "sp"), None),
        P(("grp", "sp"), "tp"),
        P(("grp", "sp"), "tp"),
        P(None, "tp"),
        P(None, "tp"),
        P(None, "tp"),
        P(None, "tp"),
        P(),
        P("tp", None),
        P("tp", None),
        P(("grp", "sp", "tp"), None),
        P(),
        P(None, "tp"),
        P(None, "tp"),
        P("tp", None),
        P(("sp", "tp"), None, None),
        P(("sp", "tp"), None, None),
        P(("sp", "tp"), None, None),
        P(("grp", "sp", "tp"), None),
        P(("grp", "sp", "tp"), None),
    )
    return jax.shard_map(
        body, mesh=mesh, in_specs=placed, out_specs=P(("grp", "sp", "tp"), None), check_vma=False
    )
```

```python
import functools

import jax
import jax.numpy as jnp
import numpy as np
from jax import lax
from jax.experimental import pallas as pl
from jax.experimental.pallas import tpu as pltpu
from jax.sharding import PartitionSpec as P

ROPE = 64
WIDE_HEAD_SIZE = 128
NARROW_HEAD_SIZE = 64
LANES = 128
VMEM_BYTES = 67_043_328


EPS = 1e-06
ROPE_BASE = 10000.0
NEG_FILL = -1e30
LOG2E = 1.4426950408889634


def rms_scale(values, gain):
    return values * lax.rsqrt(jnp.mean(values * values, axis=-1, keepdims=True) + EPS) * gain


def angle_tables(positions):
    half = ROPE // 2
    inverse = ROPE_BASE ** (-np.arange(half) * 2.0 / ROPE)
    angles = positions[:, None] * np.concatenate([inverse, inverse])[None, :]
    pad = ((0, 0), (0, LANES - ROPE))
    return (
        np.pad(np.cos(angles), pad).astype(np.float32),
        np.pad(np.sin(angles), pad).astype(np.float32),
    )


def attention_kernel(
    n_sp,
    n_tp,
    latent_hbm,
    rope_key_hbm,
    wide_query_hbm,
    narrow_query_hbm,
    wide_key_hbm,
    wide_value_hbm,
    narrow_key_hbm,
    narrow_value_hbm,
    gain_hbm,
    local_cos_hbm,
    local_sin_hbm,
    base_cos_hbm,
    base_sin_hbm,
    out_ref,
    latent_ref,
    rope_key_ref,
    wide_query_ref,
    narrow_query_ref,
    wide_key_ref,
    wide_value_ref,
    gain_ref,
    local_cos_ref,
    local_sin_ref,
    base_cos_ref,
    base_sin_ref,
    rows_buf,
    queries,
    narrow_weight,
    top,
    mixed,
    fetch,
    z_send,
    z_recv,
    x_send,
    x_recv,
    d_send,
    d_recv,
):
    tokens, width = latent_hbm.shape
    quarter = tokens // n_tp
    zn = n_sp // 2
    steps_up = zn // 2
    steps_down = zn - 1 - steps_up
    me = lax.axis_index("sp")
    x = lax.axis_index("tp")
    z = me // 2
    core = lax.rem(me, 2)
    right = lax.rem(x + 1, n_tp)
    left = lax.rem(x + n_tp - 1, n_tp)
    up = lax.rem(z + 1, zn)
    down = lax.rem(z + zn - 1, zn)
    partner = z * 2 + 1 - core

    fetches = [
        pltpu.make_async_copy(source, target, fetch.at[i])
        for i, (source, target) in enumerate(
            (
                (latent_hbm, latent_ref),
                (rope_key_hbm, rope_key_ref),
                (gain_hbm, gain_ref),
                (local_cos_hbm, local_cos_ref),
                (local_sin_hbm, local_sin_ref),
                (base_cos_hbm, base_cos_ref),
                (base_sin_hbm, base_sin_ref),
                (wide_query_hbm, wide_query_ref),
                (narrow_query_hbm, narrow_query_ref),
                (wide_key_hbm, wide_key_ref),
                (wide_value_hbm, wide_value_ref),
                (narrow_key_hbm, narrow_weight.at[:, pl.ds(0, LANES)]),
                (narrow_value_hbm, narrow_weight.at[:, pl.ds(LANES, LANES)]),
            )
        )
    ]
    for copy in fetches:
        copy.start()

    barrier = pltpu.get_barrier_semaphore()
    for place in ({"sp": up * 2 + core}, {"sp": down * 2 + core}, {"sp": partner}, {"tp": left}, {"tp": right}):
        pl.semaphore_signal(barrier, inc=1, device_id=place, device_id_type=pl.DeviceIdType.MESH)

    for copy in fetches:
        copy.wait()
    lane = lax.broadcasted_iota(jnp.int32, (tokens, LANES), 1)
    low = lane < ROPE
    lc, ls = local_cos_ref[...], local_sin_ref[...]
    bc, bs = base_cos_ref[pl.ds(me, 1), :], base_sin_ref[pl.ds(me, 1), :]
    cosine = lc * bc - ls * bs
    sine = jnp.where(lane < ROPE // 2, -1.0, 1.0) * (ls * bc + lc * bs)

    def turn(v):
        other = jnp.where(
            lane < ROPE // 2, pltpu.roll(v, LANES - ROPE // 2, 1), pltpu.roll(v, ROPE // 2, 1)
        )
        return (v * cosine + other * sine).astype(jnp.bfloat16)

    lat = latent_ref[...].astype(jnp.float32)
    normed = rms_scale(lat, gain_ref[...]).astype(jnp.bfloat16)
    rope = rope_key_ref[...].astype(jnp.float32).T
    turned = turn(jnp.concatenate([rope, jnp.zeros_like(rope)], axis=1))
    for q in range(n_tp):
        rows_buf[me, q, :, :width] = normed[q * quarter : (q + 1) * quarter]
        rows_buf[me, q, :, width:] = turned[q * quarter : (q + 1) * quarter]

    t1 = wide_query_ref[:, LANES : 2 * LANES].astype(jnp.float32)
    t2 = wide_query_ref[:, 2 * LANES :].astype(jnp.float32)
    n0 = narrow_query_ref[:, :LANES].astype(jnp.float32)
    n1 = narrow_query_ref[:, LANES:].astype(jnp.float32)
    half = LANES // 2
    queries[0, :, :LANES] = wide_query_ref[:, :LANES]
    queries[0, :, LANES:] = turn(t1)
    queries[1, :, :LANES] = pltpu.roll(jnp.where(low, t2, t1), half, 1).astype(jnp.bfloat16)
    queries[1, :, LANES:] = turn(pltpu.roll(t2, half, 1))
    queries[2, :, :LANES] = jnp.where(low, n0, 0.0).astype(jnp.bfloat16)
    queries[2, :, LANES:] = turn(pltpu.roll(n0, half, 1))
    queries[3, :, :LANES] = pltpu.roll(jnp.where(low, n1, 0.0), half, 1).astype(jnp.bfloat16)
    queries[3, :, LANES:] = turn(pltpu.roll(n1, half, 1))
    top[...] = jnp.full(top.shape, NEG_FILL, jnp.float32)
    mixed[...] = jnp.zeros(mixed.shape, jnp.float32)
    pl.semaphore_wait(barrier, 5)

    def along_z(d, k, j):
        block = jnp.where(d == 0, z - k + zn, z + k) % zn
        target = jnp.where(d == 0, up, down)
        q = lax.rem(x + j, n_tp)
        spot = rows_buf.at[block * 2 + core, q]
        return pltpu.make_async_remote_copy(
            src_ref=spot,
            dst_ref=spot,
            send_sem=z_send.at[d, k, j],
            recv_sem=z_recv.at[d, k + 1, j],
            device_id={"sp": target * 2 + core},
            device_id_type=pl.DeviceIdType.MESH,
        )

    def along_x(d, k, j):
        block = jnp.where(d == 0, z - k + zn, z + k) % zn
        q = lax.rem(x + j, n_tp)
        spot = rows_buf.at[block * 2 + core, q]
        return pltpu.make_async_remote_copy(
            src_ref=spot,
            dst_ref=spot,
            send_sem=x_send.at[d, k, j],
            recv_sem=x_recv.at[d, k, j],
            device_id={"tp": right if j == 0 else left},
            device_id_type=pl.DeviceIdType.MESH,
        )

    def to_partner(d, k):
        block = jnp.where(d == 0, z - k + zn, z + k) % zn
        spot = rows_buf.at[block * 2 + core]
        return pltpu.make_async_remote_copy(
            src_ref=spot,
            dst_ref=spot,
            send_sem=d_send.at[d, k],
            recv_sem=d_recv.at[d, k],
            device_id={"sp": partner},
            device_id_type=pl.DeviceIdType.MESH,
        )

    def arrives(d, k):
        going_up = (k <= z) & (k <= steps_up)
        going_down = ((z + k) % zn < steps_down) & (k <= steps_down)
        return jnp.where(d == 0, going_up, going_down)

    def goes_on(d, k):
        going_up = (k <= z) & (k < steps_up) & (z + 1 < zn)
        going_down = ((z + k) % zn < steps_down) & (k < steps_down)
        return jnp.where(d == 0, going_up, going_down)

    def seen(d, k):
        going_up = (k <= z) & (k <= steps_up)
        going_down = (z + k >= zn) & (z + k - zn < steps_down) & (k <= steps_down)
        return (k >= 1) & jnp.where(d == 0, going_up, going_down)

    wide_factor = (WIDE_HEAD_SIZE + ROPE) ** (-0.5) * LOG2E
    narrow_factor = (NARROW_HEAD_SIZE + ROPE) ** (-0.5) * LOG2E

    def attend(plane, own):
        rows = rows_buf[pl.ds(plane * 2, 2)].reshape(2 * tokens, width + LANES)
        latents, turned_rows = rows[:, :width], rows[:, width:]
        keys = 2 * tokens
        ones = jnp.ones((keys, LANES), jnp.bfloat16)

        def up_from(weight):
            return jnp.dot(latents, weight[...], preferred_element_type=jnp.float32).astype(jnp.bfloat16)

        wide_k, wide_v, narrow = up_from(wide_key_ref), up_from(wide_value_ref), up_from(narrow_weight)
        narrow_k = jnp.concatenate([narrow[:, :LANES], turned_rows], axis=1)
        narrow_v = jnp.concatenate([narrow[:, LANES:], ones], axis=1)
        if own:
            gap = lax.broadcasted_iota(jnp.int32, (tokens, keys), 1) - lax.broadcasted_iota(
                jnp.int32, (tokens, keys), 0
            )
            visible = gap <= core * tokens
        for h in range(4):
            if h < 2:
                at = slice(h * LANES, (h + 1) * LANES)
                k_h = jnp.concatenate([wide_k[:, at], turned_rows], axis=1)
                v_h = jnp.concatenate([wide_v[:, at], ones], axis=1)
            else:
                k_h, v_h = narrow_k, narrow_v
            scores = lax.dot_general(
                queries[h], k_h, (((1,), (1,)), ((), ())), preferred_element_type=jnp.float32
            ) * (wide_factor if h < 2 else narrow_factor)
            if own:
                scores = jnp.where(visible, scores, NEG_FILL)
            old = top[h]
            new = jnp.maximum(old, jnp.max(scores, axis=1, keepdims=True))
            top[h] = new
            weights = jnp.exp2(scores - jnp.concatenate([new] * (keys // LANES), axis=1)).astype(jnp.bfloat16)
            fading = jnp.exp2(old - new)
            mixed[h] = mixed[h] * jnp.concatenate([fading, fading], axis=1) + jnp.dot(
                weights, v_h, preferred_element_type=jnp.float32
            )

    to_partner(0, 0).start()
    for d in range(2):

        @pl.when(goes_on(d, 0))
        def _():
            for j in range(2):
                along_z(d, 0, j).start()

    to_partner(0, 0).wait_recv()

    attend(z, True)

    def one_step(k, carry):
        def forward(d, c):
            @pl.when(arrives(d, k))
            def _():
                for j in range(2):
                    along_z(d, k - 1, j).wait_recv()

            @pl.when(goes_on(d, k))
            def _():
                for j in range(2):
                    along_z(d, k, j).start()

            @pl.when(seen(d, k))
            def _():
                for j in range(2):
                    along_x(d, k, j).start()

            @pl.when(seen(d, k - 1))
            def _():
                for j in range(2):
                    along_x(d, k - 1, j).wait_recv()
                to_partner(d, k - 1).start()

            return c

        lax.fori_loop(0, 2, forward, 0)

        def work(d, c):
            @pl.when(seen(d, k - 2))
            def _():
                to_partner(d, k - 2).wait_recv()
                attend(jnp.where(d == 0, z - k + 2, z + k - 2 - zn), False)

            return c

        lax.fori_loop(0, 2, work, 0)
        return carry

    lax.fori_loop(1, steps_up + 3, one_step, 0)

    to_partner(0, 0).wait_send()

    def settle(k, carry):
        def both(d, c):
            @pl.when(goes_on(d, k))
            def _():
                for j in range(2):
                    along_z(d, k, j).wait_send()

            @pl.when(seen(d, k))
            def _():
                for j in range(2):
                    along_x(d, k, j).wait_send()
                to_partner(d, k).wait_send()

            return c

        return lax.fori_loop(0, 2, both, carry)

    lax.fori_loop(0, steps_up + 1, settle, 0)

    for h in range(2):
        out_ref[:, h * LANES : (h + 1) * LANES] = (mixed[h, :, :LANES] / mixed[h, :, LANES:]).astype(
            out_ref.dtype
        )
    out_ref[:, 2 * LANES :] = jnp.where(
        low, mixed[2, :, :LANES] / mixed[2, :, LANES:], mixed[3, :, :LANES] / mixed[3, :, LANES:]
    ).astype(out_ref.dtype)


def attention(
    latent, rope_key, wide_query, narrow_query, wide_key, wide_value, narrow_key, narrow_value, gain
):
    tokens, width = latent.shape
    n_sp, n_tp = lax.axis_size("sp"), lax.axis_size("tp")
    zn = n_sp // 2
    assert n_sp % 4 == 0 and n_tp == 4 and wide_query.shape[1] == 3 * LANES
    assert narrow_query.shape[1] == 2 * LANES and zn >= 4
    local_cos, local_sin = angle_tables(np.arange(tokens, dtype=np.float64))
    base_cos, base_sin = angle_tables(np.arange(n_sp, dtype=np.float64) * tokens)
    hops = zn // 2 + 1
    dma = pltpu.SemaphoreType.DMA
    vmem = pl.BlockSpec(memory_space=pltpu.VMEM)
    return pl.pallas_call(
        functools.partial(attention_kernel, n_sp, n_tp),
        out_shape=jax.ShapeDtypeStruct((tokens, 3 * LANES), jnp.bfloat16),
        in_specs=[pl.BlockSpec(memory_space=pltpu.HBM)] * 13,
        out_specs=vmem,
        scratch_shapes=[
            pltpu.VMEM(latent.shape, jnp.bfloat16),
            pltpu.VMEM(rope_key.shape[::-1], jnp.bfloat16),
            pltpu.VMEM(wide_query.shape, jnp.bfloat16),
            pltpu.VMEM(narrow_query.shape, jnp.bfloat16),
            pltpu.VMEM(wide_key.shape, jnp.bfloat16),
            pltpu.VMEM(wide_value.shape, jnp.bfloat16),
            pltpu.VMEM((1, width), jnp.float32),
            pltpu.VMEM(local_cos.shape, jnp.float32),
            pltpu.VMEM(local_sin.shape, jnp.float32),
            pltpu.VMEM(base_cos.shape, jnp.float32),
            pltpu.VMEM(base_sin.shape, jnp.float32),
            pltpu.VMEM((n_sp, n_tp, tokens // n_tp, width + LANES), jnp.bfloat16),
            pltpu.VMEM((4, tokens, 2 * LANES), jnp.bfloat16),
            pltpu.VMEM((width, 2 * LANES), jnp.bfloat16),
            pltpu.VMEM((4, tokens, LANES), jnp.float32),
            pltpu.VMEM((4, tokens, 2 * LANES), jnp.float32),
            dma((13,)),
            dma((2, hops, 2)),
            dma((2, hops + 1, 2)),
            dma((2, hops, 2)),
            dma((2, hops, 2)),
            dma((2, hops)),
            dma((2, hops)),
        ],
        compiler_params=pltpu.CompilerParams(
            collective_id=0, has_side_effects=True, vmem_limit_bytes=VMEM_BYTES
        ),
    )(
        latent,
        rope_key.T,
        wide_query,
        narrow_query,
        wide_key,
        wide_value,
        narrow_key,
        narrow_value,
        gain.reshape(1, width),
        local_cos,
        local_sin,
        base_cos,
        base_sin,
    )


DELTAS = ((0, 1, -1, 4, -4, 5, -5, 8), (2, -2, 3, -3, 6, -6, 7, -7))
COLUMNS = 1024
CAPACITY = 2


def silu(v):
    return v / (1.0 + jnp.exp(-v))


def experts_kernel(
    n_sp,
    n_tp,
    mix_ref,
    routes_hbm,
    weight_hbm,
    out_wide_hbm,
    out_narrow_hbm,
    residual_hbm,
    gain_hbm,
    shared_gate_hbm,
    shared_up_hbm,
    shared_down_hbm,
    expert_gate_hbm,
    expert_up_hbm,
    expert_down_hbm,
    out_ref,
    routes_ref,
    weight_ref,
    places,
    out_weight,
    residual_ref,
    gain_ref,
    shared_in,
    shared_down,
    expert_in,
    expert_down,
    part,
    opposite,
    summed,
    landed,
    stream,
    gathered,
    outgoing,
    first_recv,
    first_relay,
    second_send,
    second_recv,
    finished,
    back_recv,
    back_send,
    back_relay,
    returned,
    shared_send,
    shared_recv,
    fetch,
    send_sems,
    recv_sems,
):
    rows, depth = residual_hbm.shape
    half = depth // 2
    zn = n_sp // 2
    lanes = 2 * n_tp
    piece = outgoing.shape[1]
    wide_rows = out_wide_hbm.shape[0]
    ff = shared_gate_hbm.shape[1]
    hidden = expert_gate_hbm.shape[1]
    top_count = routes_hbm.shape[0]
    me = lax.axis_index("sp")
    x = lax.axis_index("tp")
    z = me // 2
    core = lax.rem(me, 2)
    lane = core * n_tp + x

    def at_plane(delta):
        return lax.rem(z + (delta + zn), zn)

    def on_plane(delta):
        return {"sp": at_plane(delta) * 2 + core}

    def along_x(dx):
        return {"tp": lax.rem(x + (dx + n_tp), n_tp)}

    def in_plane(dc, dx):
        other = 1 - core if dc else core
        return {"sp": z * 2 + other, "tp": lax.rem(x + (dx + n_tp), n_tp)}

    relative = [(dc, dx) for dc in range(2) for dx in range(n_tp)]

    taken = [0]

    def remote(source, target, place):
        i = taken[0]
        taken[0] += 1
        return pltpu.make_async_remote_copy(
            src_ref=source,
            dst_ref=target,
            send_sem=send_sems.at[i],
            recv_sem=recv_sems.at[i],
            device_id=place,
            device_id_type=pl.DeviceIdType.MESH,
        )

    barrier = pltpu.get_barrier_semaphore()
    greeted = [on_plane(d) for d in range(1, zn)] + [in_plane(dc, dx) for dc, dx in relative[1:]]
    for place in greeted:
        pl.semaphore_signal(barrier, inc=1, device_id=place, device_id_type=pl.DeviceIdType.MESH)

    fetches = [
        pltpu.make_async_copy(source, target, fetch.at[i])
        for i, (source, target) in enumerate(
            (
                (routes_hbm, routes_ref),
                (weight_hbm, weight_ref),
                (out_wide_hbm, out_weight.at[pl.ds(0, wide_rows)]),
                (out_narrow_hbm, out_weight.at[pl.ds(wide_rows, out_narrow_hbm.shape[0])]),
                (residual_hbm, residual_ref),
                (gain_hbm, gain_ref),
                (shared_gate_hbm, shared_in.at[:, pl.ds(0, ff)]),
                (shared_up_hbm, shared_in.at[:, pl.ds(ff, ff)]),
                (shared_down_hbm, shared_down),
                (expert_gate_hbm.at[0], expert_in.at[pl.ds(0, hidden)]),
                (expert_up_hbm.at[0], expert_in.at[pl.ds(hidden, hidden)]),
                (expert_down_hbm.at[0], expert_down),
            )
        )
    ]
    for copy in fetches:
        copy.start()

    def chunks():
        return [pl.ds(n, COLUMNS) for n in range(0, depth, COLUMNS)]

    def project(dx):
        q = pl.multiple_of(lax.rem(x + dx, n_tp) * rows, rows)
        mine = mix_ref[pl.ds(q, rows), :]
        for cols in chunks():
            part[dx, :, cols] = jnp.dot(
                mine, out_weight[:, cols], preferred_element_type=jnp.float32
            ).astype(jnp.bfloat16)

    lower, upper = pl.ds(0, half), pl.ds(half, half)
    for copy in fetches[:4]:
        copy.wait()
    project(2)
    pl.semaphore_wait(barrier, len(greeted))
    over_right = remote(part.at[2, :, lower], opposite.at[0], along_x(1))
    over_left = remote(part.at[2, :, upper], opposite.at[1], along_x(-1))
    over_right.start()
    over_left.start()
    project(1)
    straight_right = remote(part.at[1, :, upper], landed.at[0, 1], along_x(1))
    straight_right.start()
    project(3)
    straight_left = remote(part.at[3, :, lower], landed.at[1, 0], along_x(-1))
    straight_left.start()
    project(0)

    r0 = lax.broadcasted_iota(jnp.int32, (rows, rows), 0)
    r1 = lax.broadcasted_iota(jnp.int32, (rows, rows), 1)

    def upright(row):
        return jnp.sum(jnp.where(r0 == r1, row, 0.0), axis=1, keepdims=True)

    named = [routes_ref[c : c + 1, :].astype(jnp.float32) for c in range(top_count)]
    shares = [upright(weight_ref[c : c + 1, :]) for c in range(top_count)]
    slot = lax.broadcasted_iota(jnp.int32, (zn * piece, rows), 0).astype(jnp.float32)
    maps = []
    for c in range(top_count):
        earlier = jnp.zeros((1, rows), jnp.float32)
        for other in range(top_count):
            same = (upright(named[other]) == named[c]) & (r0 < r1)
            earlier = earlier + jnp.sum(jnp.where(same, 1.0, 0.0), axis=0, keepdims=True)
        maps.append(jnp.where(slot == named[c] * CAPACITY + earlier, 1.0, 0.0))
        places[c] = maps[c].T.astype(jnp.bfloat16)
    send_map = sum(maps[1:], maps[0]).astype(jnp.bfloat16)

    over_right.wait_recv()
    summed[0] = (part[1, :, lower].astype(jnp.float32) + opposite[0].astype(jnp.float32)).astype(jnp.bfloat16)
    joined_right = remote(summed.at[0], landed.at[0, 0], along_x(1))
    joined_right.start()
    over_left.wait_recv()
    summed[1] = (part[3, :, upper].astype(jnp.float32) + opposite[1].astype(jnp.float32)).astype(jnp.bfloat16)
    joined_left = remote(summed.at[1], landed.at[1, 1], along_x(-1))
    joined_left.start()
    fetches[4].wait()
    fetches[5].wait()
    for copy in (straight_right, straight_left, joined_right, joined_left):
        copy.wait_recv()
    for h, cols in enumerate((lower, upper)):
        stream[:, cols] = (
            residual_ref[:, cols].astype(jnp.float32)
            + part[0, :, cols].astype(jnp.float32)
            + landed[0, h].astype(jnp.float32)
            + landed[1, h].astype(jnp.float32)
        ).astype(jnp.bfloat16)
    gathered[0] = rms_scale(stream[...].astype(jnp.float32), gain_ref[...]).astype(jnp.bfloat16)

    for cols in chunks():
        outgoing[:, :, cols] = (
            jnp.dot(send_map, gathered[0, :, cols], preferred_element_type=jnp.float32)
            .astype(jnp.bfloat16)
            .reshape(zn, piece, COLUMNS)
        )
    sent = [over_right, over_left, straight_right, straight_left, joined_right, joined_left]
    far = at_plane(8)
    relay_up = remote(outgoing.at[far, :, lower], first_relay.at[0], on_plane(4))
    relay_down = remote(outgoing.at[far, :, upper], first_relay.at[1], on_plane(-4))
    relay_up.start()
    relay_down.start()
    first = [{}, {}]
    for ch in range(2):
        for j, delta in enumerate(DELTAS[ch]):
            if delta in (0, 8):
                continue
            first[ch][j] = remote(outgoing.at[at_plane(delta)], first_recv.at[ch, j], on_plane(delta))
            first[ch][j].start()
        if ch == 0:
            spread = [remote(gathered.at[0], gathered.at[dx], along_x(dx)) for dx in (1, 3, 2)]
            for copy in spread:
                copy.start()
    first_recv[0, 0] = outgoing[z]
    far_slot = DELTAS[0].index(8)
    onward_up = remote(first_relay.at[0], first_recv.at[0, far_slot, :, lower], on_plane(4))
    onward_down = remote(first_relay.at[1], first_recv.at[0, far_slot, :, upper], on_plane(-4))
    relay_up.wait_recv()
    onward_up.start()
    relay_down.wait_recv()
    onward_down.start()
    sent += [relay_up, relay_down, onward_up, onward_down] + spread
    sent += list(first[0].values()) + list(first[1].values())

    for copy in fetches[6:]:
        copy.wait()
    for copy in spread:
        copy.wait_recv()
    every = gathered[...].reshape(n_tp * rows, depth)
    both = jnp.dot(every, shared_in[...], preferred_element_type=jnp.float32)
    act = (silu(both[:, :ff]) * both[:, ff:]).astype(jnp.bfloat16)
    for cols in chunks():
        shared_send[:, :, cols] = (
            jnp.dot(act, shared_down[:, cols], preferred_element_type=jnp.float32)
            .astype(jnp.bfloat16)
            .reshape(n_tp, rows, COLUMNS)
        )
    shared_back = [remote(shared_send.at[dx], shared_recv.at[dx - 1], along_x(-dx)) for dx in range(1, n_tp)]
    for copy in shared_back:
        copy.start()
    sent += shared_back

    count = lanes * piece
    o = lax.broadcasted_iota(jnp.int32, (count, count), 0)
    i = lax.broadcasted_iota(jnp.int32, (count, count), 1)
    swap = jnp.where(
        (o // piece == (i % piece) // 2) & ((o % piece) // 2 == i // piece) & (o % 2 == i % 2), 1.0, 0.0
    ).astype(jnp.bfloat16)

    def swapped(source, target, ch):
        for cols in chunks():
            target[ch, :, :, cols] = (
                jnp.dot(
                    swap, source[ch, :, :, cols].reshape(count, COLUMNS), preferred_element_type=jnp.float32
                )
                .astype(jnp.bfloat16)
                .reshape(lanes, piece, COLUMNS)
            )

    def to_lanes(ch):
        swapped(first_recv, second_send, ch)
        copies = []
        for r, (dc, dx) in enumerate(relative):
            if r == 0:
                continue
            other = (1 - core if dc else core) * n_tp + lax.rem(x + dx, n_tp)
            copies.append(remote(second_send.at[ch, other], second_recv.at[ch, r], in_plane(dc, dx)))
            copies[-1].start()
        second_recv[ch, 0] = second_send[ch, lane]
        return copies

    def run_expert(ch):
        taken_in = second_recv[ch].reshape(count, depth)
        gate, lifted = (
            lax.dot_general(
                taken_in,
                expert_in[pl.ds(at, hidden), :],
                (((1,), (1,)), ((), ())),
                preferred_element_type=jnp.float32,
            )
            for at in (0, hidden)
        )
        active = (silu(gate) * lifted).astype(jnp.bfloat16)
        for cols in chunks():
            finished[ch, :, :, cols] = (
                jnp.dot(active, expert_down[:, cols], preferred_element_type=jnp.float32)
                .astype(jnp.bfloat16)
                .reshape(lanes, piece, COLUMNS)
            )
        copies = []
        for r, (dc, dx) in enumerate(relative):
            if r == 0:
                continue
            copies.append(remote(finished.at[ch, r], back_recv.at[ch, lane], in_plane(dc, -dx)))
            copies[-1].start()
        back_recv[ch, lane] = finished[ch, 0]
        return copies

    def home(ch):
        swapped(back_recv, back_send, ch)
        copies = []
        relays = []
        for j, delta in enumerate(DELTAS[ch]):
            if delta == 8:
                relays = [
                    remote(back_send.at[ch, j, :, lower], back_relay.at[0], on_plane(4)),
                    remote(back_send.at[ch, j, :, upper], back_relay.at[1], on_plane(-4)),
                ]
                for copy in relays:
                    copy.start()
        for j, delta in enumerate(DELTAS[ch]):
            if delta == 0:
                returned[z] = back_send[ch, j]
            elif delta != 8:
                copies.append(remote(back_send.at[ch, j], returned.at[z], on_plane(-delta)))
                copies[-1].start()
        return copies, relays

    for copy in list(first[0].values()) + [onward_up, onward_down]:
        copy.wait_recv()
    lane_copies = to_lanes(0)
    for copy in lane_copies:
        copy.wait_recv()
    back_copies = run_expert(0)
    for copy in back_copies:
        copy.wait_recv()
    home_copies, relays = home(0)
    sent += lane_copies + back_copies + home_copies + relays

    for copy in first[1].values():
        copy.wait_recv()
    lane_copies = to_lanes(1)
    relays[0].wait_recv()
    last_up = remote(back_relay.at[0], returned.at[at_plane(-4), :, lower], on_plane(4))
    last_up.start()
    relays[1].wait_recv()
    last_down = remote(back_relay.at[1], returned.at[at_plane(4), :, upper], on_plane(-4))
    last_down.start()
    for copy in lane_copies:
        copy.wait_recv()
    back_copies = run_expert(1)
    for copy in back_copies:
        copy.wait_recv()
    more_home, _ = home(1)
    sent += lane_copies + back_copies + more_home + [last_up, last_down]

    for copy in shared_back:
        copy.wait_recv()
    for copy in home_copies + more_home + [last_up, last_down]:
        copy.wait_recv()
    for cols in chunks():
        total = stream[:, cols].astype(jnp.float32) + shared_send[0, :, cols].astype(jnp.float32)
        for dx in range(n_tp - 1):
            total = total + shared_recv[dx, :, cols].astype(jnp.float32)
        results = returned[:, :, cols].reshape(zn * piece, COLUMNS)
        for c in range(top_count):
            total = total + shares[c] * jnp.dot(places[c], results, preferred_element_type=jnp.float32)
        out_ref[:, cols] = total.astype(out_ref.dtype)
    for copy in sent:
        copy.wait_send()


def projected_experts(
    mix,
    routes,
    route_weights,
    out_wide,
    out_narrow,
    residual,
    gain,
    shared_gate,
    shared_up,
    shared_down,
    expert_gate,
    expert_up,
    expert_down,
):
    rows, depth = residual.shape
    n_sp, n_tp = lax.axis_size("sp"), lax.axis_size("tp")
    zn, lanes = n_sp // 2, 2 * n_tp
    piece = CAPACITY * lanes
    ff = shared_gate.shape[1]
    hidden = expert_gate.shape[2]
    assert zn == 16 and n_tp == 4 and expert_gate.shape[0] == 1
    vmem, hbm = pl.BlockSpec(memory_space=pltpu.VMEM), pl.BlockSpec(memory_space=pltpu.HBM)
    bf16 = jnp.bfloat16
    chunk = (2, lanes, piece, depth)
    dma = pltpu.SemaphoreType.DMA
    return pl.pallas_call(
        functools.partial(experts_kernel, n_sp, n_tp),
        out_shape=jax.ShapeDtypeStruct((rows, depth), bf16),
        in_specs=[vmem] + [hbm] * 12,
        out_specs=vmem,
        scratch_shapes=[
            pltpu.VMEM(routes.shape[::-1], jnp.int32),
            pltpu.VMEM(route_weights.shape[::-1], jnp.float32),
            pltpu.VMEM((routes.shape[1], rows, zn * piece), bf16),
            pltpu.VMEM((out_wide.shape[0] + out_narrow.shape[0], depth), bf16),
            pltpu.VMEM((rows, depth), bf16),
            pltpu.VMEM((1, depth), jnp.float32),
            pltpu.VMEM((depth, 2 * ff), bf16),
            pltpu.VMEM(shared_down.shape, bf16),
            pltpu.VMEM((2 * hidden, depth), bf16),
            pltpu.VMEM(expert_down.shape[1:], bf16),
            pltpu.VMEM((n_tp, rows, depth), bf16),
            pltpu.VMEM((2, rows, depth // 2), bf16),
            pltpu.VMEM((2, rows, depth // 2), bf16),
            pltpu.VMEM((2, 2, rows, depth // 2), bf16),
            pltpu.VMEM((rows, depth), bf16),
            pltpu.VMEM((n_tp, rows, depth), bf16),
            pltpu.VMEM((zn, piece, depth), bf16),
            pltpu.VMEM(chunk, bf16),
            pltpu.VMEM((2, piece, depth // 2), bf16),
            pltpu.VMEM(chunk, bf16),
            pltpu.VMEM(chunk, bf16),
            pltpu.VMEM(chunk, bf16),
            pltpu.VMEM(chunk, bf16),
            pltpu.VMEM(chunk, bf16),
            pltpu.VMEM((2, piece, depth // 2), bf16),
            pltpu.VMEM((zn, piece, depth), bf16),
            pltpu.VMEM((n_tp, rows, depth), bf16),
            pltpu.VMEM((n_tp - 1, rows, depth), bf16),
            dma((12,)),
            dma((80,)),
            dma((80,)),
        ],
        compiler_params=pltpu.CompilerParams(
            collective_id=1, has_side_effects=True, vmem_limit_bytes=VMEM_BYTES
        ),
    )(
        mix,
        routes.T,
        route_weights.T,
        out_wide,
        out_narrow,
        residual,
        gain.reshape(1, depth),
        shared_gate,
        shared_up,
        shared_down,
        jnp.swapaxes(expert_gate, 1, 2),
        jnp.swapaxes(expert_up, 1, 2),
        expert_down,
    )


def body(
    latent,
    rope_key,
    wide_query,
    narrow_query,
    wide_key_weight,
    wide_value_weight,
    narrow_key_weight,
    narrow_value_weight,
    latent_norm_scale,
    out_wide,
    out_narrow,
    residual,
    ffn_gain,
    shared_gate,
    shared_up,
    shared_down,
    expert_gate,
    expert_up,
    expert_down,
    routes,
    route_weights,
):
    mix = attention(
        latent,
        rope_key,
        wide_query,
        narrow_query,
        wide_key_weight,
        wide_value_weight,
        narrow_key_weight,
        narrow_value_weight,
        latent_norm_scale,
    )
    return projected_experts(
        mix,
        routes,
        route_weights,
        out_wide,
        out_narrow,
        residual,
        ffn_gain,
        shared_gate,
        shared_up,
        shared_down,
        expert_gate,
        expert_up,
        expert_down,
    )


def solution(mesh):
    placed = (
        P(("grp", "sp"), None),
        P(("grp", "sp"), None),
        P(("grp", "sp"), "tp"),
        P(("grp", "sp"), "tp"),
        P(None, "tp"),
        P(None, "tp"),
        P(None, "tp"),
        P(None, "tp"),
        P(),
        P("tp", None),
        P("tp", None),
        P(("grp", "sp", "tp"), None),
        P(),
        P(None, "tp"),
        P(None, "tp"),
        P("tp", None),
        P(("sp", "tp"), None, None),
        P(("sp", "tp"), None, None),
        P(("sp", "tp"), None, None),
        P(("grp", "sp", "tp"), None),
        P(("grp", "sp", "tp"), None),
    )
    return jax.shard_map(
        body, mesh=mesh, in_specs=placed, out_specs=P(("grp", "sp", "tp"), None), check_vma=False
    )
```

```python
import functools

import jax
import jax.numpy as jnp
import numpy as np
from jax import lax
from jax.experimental import pallas as pl
from jax.experimental.pallas import tpu as pltpu
from jax.sharding import PartitionSpec as P

ROPE = 64
WIDE_HEAD_SIZE = 128
NARROW_HEAD_SIZE = 64
LANES = 128
VMEM_BYTES = 67_043_328


EPS = 1e-06
ROPE_BASE = 10000.0
NEG_FILL = -1e30
LOG2E = 1.4426950408889634


def rms_scale(values, gain):
    return values * lax.rsqrt(jnp.mean(values * values, axis=-1, keepdims=True) + EPS) * gain


def angle_tables(positions):
    half = ROPE // 2
    inverse = ROPE_BASE ** (-np.arange(half) * 2.0 / ROPE)
    angles = positions[:, None] * np.concatenate([inverse, inverse])[None, :]
    pad = ((0, 0), (0, LANES - ROPE))
    return (
        np.pad(np.cos(angles), pad).astype(np.float32),
        np.pad(np.sin(angles), pad).astype(np.float32),
    )


def attention_kernel(
    n_sp,
    n_tp,
    latent_hbm,
    rope_key_hbm,
    wide_query_hbm,
    narrow_query_hbm,
    wide_key_hbm,
    wide_value_hbm,
    narrow_key_hbm,
    narrow_value_hbm,
    gain_hbm,
    local_cos_hbm,
    local_sin_hbm,
    base_cos_hbm,
    base_sin_hbm,
    out_ref,
    latent_ref,
    rope_key_ref,
    wide_query_ref,
    narrow_query_ref,
    wide_key_ref,
    wide_value_ref,
    gain_ref,
    local_cos_ref,
    local_sin_ref,
    base_cos_ref,
    base_sin_ref,
    rows_buf,
    queries,
    narrow_weight,
    top,
    mixed,
    fetch,
    z_send,
    z_recv,
    x_send,
    x_recv,
    d_send,
    d_recv,
):
    tokens, width = latent_hbm.shape
    quarter = tokens // n_tp
    zn = n_sp // 2
    steps_up = zn // 2
    steps_down = zn - 1 - steps_up
    me = lax.axis_index("sp")
    x = lax.axis_index("tp")
    z = me // 2
    core = lax.rem(me, 2)
    right = lax.rem(x + 1, n_tp)
    left = lax.rem(x + n_tp - 1, n_tp)
    up = lax.rem(z + 1, zn)
    down = lax.rem(z + zn - 1, zn)
    partner = z * 2 + 1 - core

    fetches = [
        pltpu.make_async_copy(source, target, fetch.at[i])
        for i, (source, target) in enumerate(
            (
                (latent_hbm, latent_ref),
                (rope_key_hbm, rope_key_ref),
                (gain_hbm, gain_ref),
                (local_cos_hbm, local_cos_ref),
                (local_sin_hbm, local_sin_ref),
                (base_cos_hbm, base_cos_ref),
                (base_sin_hbm, base_sin_ref),
                (wide_query_hbm, wide_query_ref),
                (narrow_query_hbm, narrow_query_ref),
                (wide_key_hbm, wide_key_ref),
                (wide_value_hbm, wide_value_ref),
                (narrow_key_hbm, narrow_weight.at[:, pl.ds(0, LANES)]),
                (narrow_value_hbm, narrow_weight.at[:, pl.ds(LANES, LANES)]),
            )
        )
    ]
    for copy in fetches:
        copy.start()

    barrier = pltpu.get_barrier_semaphore()
    for place in ({"sp": up * 2 + core}, {"sp": down * 2 + core}, {"sp": partner}, {"tp": left}, {"tp": right}):
        pl.semaphore_signal(barrier, inc=1, device_id=place, device_id_type=pl.DeviceIdType.MESH)

    for copy in fetches:
        copy.wait()
    lane = lax.broadcasted_iota(jnp.int32, (tokens, LANES), 1)
    low = lane < ROPE
    lc, ls = local_cos_ref[...], local_sin_ref[...]
    bc, bs = base_cos_ref[pl.ds(me, 1), :], base_sin_ref[pl.ds(me, 1), :]
    cosine = lc * bc - ls * bs
    sine = jnp.where(lane < ROPE // 2, -1.0, 1.0) * (ls * bc + lc * bs)

    def turn(v):
        other = jnp.where(
            lane < ROPE // 2, pltpu.roll(v, LANES - ROPE // 2, 1), pltpu.roll(v, ROPE // 2, 1)
        )
        return (v * cosine + other * sine).astype(jnp.bfloat16)

    lat = latent_ref[...].astype(jnp.float32)
    normed = rms_scale(lat, gain_ref[...]).astype(jnp.bfloat16)
    rope = rope_key_ref[...].astype(jnp.float32).T
    turned = turn(jnp.concatenate([rope, jnp.zeros_like(rope)], axis=1))
    for q in range(n_tp):
        rows_buf[me, q, :, :width] = normed[q * quarter : (q + 1) * quarter]
        rows_buf[me, q, :, width:] = turned[q * quarter : (q + 1) * quarter]

    t1 = wide_query_ref[:, LANES : 2 * LANES].astype(jnp.float32)
    t2 = wide_query_ref[:, 2 * LANES :].astype(jnp.float32)
    n0 = narrow_query_ref[:, :LANES].astype(jnp.float32)
    n1 = narrow_query_ref[:, LANES:].astype(jnp.float32)
    half = LANES // 2
    queries[0, :, :LANES] = wide_query_ref[:, :LANES]
    queries[0, :, LANES:] = turn(t1)
    queries[1, :, :LANES] = pltpu.roll(jnp.where(low, t2, t1), half, 1).astype(jnp.bfloat16)
    queries[1, :, LANES:] = turn(pltpu.roll(t2, half, 1))
    queries[2, :, :LANES] = jnp.where(low, n0, 0.0).astype(jnp.bfloat16)
    queries[2, :, LANES:] = turn(pltpu.roll(n0, half, 1))
    queries[3, :, :LANES] = pltpu.roll(jnp.where(low, n1, 0.0), half, 1).astype(jnp.bfloat16)
    queries[3, :, LANES:] = turn(pltpu.roll(n1, half, 1))
    top[...] = jnp.full(top.shape, NEG_FILL, jnp.float32)
    mixed[...] = jnp.zeros(mixed.shape, jnp.float32)
    pl.semaphore_wait(barrier, 5)

    def along_z(d, k, j):
        block = jnp.where(d == 0, z - k + zn, z + k) % zn
        target = jnp.where(d == 0, up, down)
        q = lax.rem(x + j, n_tp)
        spot = rows_buf.at[block * 2 + core, q]
        return pltpu.make_async_remote_copy(
            src_ref=spot,
            dst_ref=spot,
            send_sem=z_send.at[d, k, j],
            recv_sem=z_recv.at[d, k + 1, j],
            device_id={"sp": target * 2 + core},
            device_id_type=pl.DeviceIdType.MESH,
        )

    def along_x(d, k, j):
        block = jnp.where(d == 0, z - k + zn, z + k) % zn
        q = lax.rem(x + j, n_tp)
        spot = rows_buf.at[block * 2 + core, q]
        return pltpu.make_async_remote_copy(
            src_ref=spot,
            dst_ref=spot,
            send_sem=x_send.at[d, k, j],
            recv_sem=x_recv.at[d, k, j],
            device_id={"tp": jnp.where(j == 0, right, left)},
            device_id_type=pl.DeviceIdType.MESH,
        )

    def to_partner(d, k):
        block = jnp.where(d == 0, z - k + zn, z + k) % zn
        spot = rows_buf.at[block * 2 + core]
        return pltpu.make_async_remote_copy(
            src_ref=spot,
            dst_ref=spot,
            send_sem=d_send.at[d, k],
            recv_sem=d_recv.at[d, k],
            device_id={"sp": partner},
            device_id_type=pl.DeviceIdType.MESH,
        )

    def arrives(d, k):
        going_up = (k <= z) & (k <= steps_up)
        going_down = ((z + k) % zn < steps_down) & (k <= steps_down)
        return jnp.where(d == 0, going_up, going_down)

    def goes_on(d, k):
        going_up = (k <= z) & (k < steps_up) & (z + 1 < zn)
        going_down = ((z + k) % zn < steps_down) & (k < steps_down)
        return jnp.where(d == 0, going_up, going_down)

    def seen(d, k):
        going_up = (k <= z) & (k <= steps_up)
        going_down = (z + k >= zn) & (z + k - zn < steps_down) & (k <= steps_down)
        return (k >= 1) & jnp.where(d == 0, going_up, going_down)

    wide_factor = (WIDE_HEAD_SIZE + ROPE) ** (-0.5) * LOG2E
    narrow_factor = (NARROW_HEAD_SIZE + ROPE) ** (-0.5) * LOG2E

    def attend(plane, own):
        rows = rows_buf[pl.ds(plane * 2, 2)].reshape(2 * tokens, width + LANES)
        latents, turned_rows = rows[:, :width], rows[:, width:]
        keys = 2 * tokens
        ones = jnp.ones((keys, LANES), jnp.bfloat16)

        def up_from(weight):
            return jnp.dot(latents, weight[...], preferred_element_type=jnp.float32).astype(jnp.bfloat16)

        wide_k, wide_v, narrow = up_from(wide_key_ref), up_from(wide_value_ref), up_from(narrow_weight)
        narrow_k = jnp.concatenate([narrow[:, :LANES], turned_rows], axis=1)
        narrow_v = jnp.concatenate([narrow[:, LANES:], ones], axis=1)
        if own:
            gap = lax.broadcasted_iota(jnp.int32, (tokens, keys), 1) - lax.broadcasted_iota(
                jnp.int32, (tokens, keys), 0
            )
            visible = gap <= core * tokens
        for h in range(4):
            if h < 2:
                at = slice(h * LANES, (h + 1) * LANES)
                k_h = jnp.concatenate([wide_k[:, at], turned_rows], axis=1)
                v_h = jnp.concatenate([wide_v[:, at], ones], axis=1)
            else:
                k_h, v_h = narrow_k, narrow_v
            scores = lax.dot_general(
                queries[h], k_h, (((1,), (1,)), ((), ())), preferred_element_type=jnp.float32
            ) * (wide_factor if h < 2 else narrow_factor)
            if own:
                scores = jnp.where(visible, scores, NEG_FILL)
            old = top[h]
            new = jnp.maximum(old, jnp.max(scores, axis=1, keepdims=True))
            top[h] = new
            weights = jnp.exp2(scores - jnp.concatenate([new] * (keys // LANES), axis=1)).astype(jnp.bfloat16)
            fading = jnp.exp2(old - new)
            mixed[h] = mixed[h] * jnp.concatenate([fading, fading], axis=1) + jnp.dot(
                weights, v_h, preferred_element_type=jnp.float32
            )

    to_partner(0, 0).start()
    for d in range(2):

        @pl.when(goes_on(d, 0))
        def _():
            for j in range(2):
                along_z(d, 0, j).start()

    to_partner(0, 0).wait_recv()

    attend(z, True)

    def one_step(k, carry):
        def quarter_step(j, carry):
            def forward(d, c):
                @pl.when(arrives(d, k))
                def _():
                    along_z(d, k - 1, j).wait_recv()

                @pl.when(goes_on(d, k))
                def _():
                    along_z(d, k, j).start()

                @pl.when(seen(d, k))
                def _():
                    along_x(d, k, j).start()

                @pl.when(seen(d, k - 1) & (j == 0))
                def _():
                    for side in range(2):
                        along_x(d, k - 1, side).wait_recv()
                    to_partner(d, k - 1).start()

                return c

            lax.fori_loop(0, 2, forward, 0)

            @pl.when(seen(j, k - 2))
            def _():
                to_partner(j, k - 2).wait_recv()
                attend(jnp.where(j == 0, z - k + 2, z + k - 2 - zn), False)

            return carry

        return lax.fori_loop(0, 2, quarter_step, carry)

    lax.fori_loop(1, steps_up + 3, one_step, 0)

    to_partner(0, 0).wait_send()

    def settle(k, carry):
        def both(d, c):
            @pl.when(goes_on(d, k))
            def _():
                for j in range(2):
                    along_z(d, k, j).wait_send()

            @pl.when(seen(d, k))
            def _():
                for j in range(2):
                    along_x(d, k, j).wait_send()
                to_partner(d, k).wait_send()

            return c

        return lax.fori_loop(0, 2, both, carry)

    lax.fori_loop(0, steps_up + 1, settle, 0)

    for h in range(2):
        out_ref[:, h * LANES : (h + 1) * LANES] = (mixed[h, :, :LANES] / mixed[h, :, LANES:]).astype(
            out_ref.dtype
        )
    out_ref[:, 2 * LANES :] = jnp.where(
        low, mixed[2, :, :LANES] / mixed[2, :, LANES:], mixed[3, :, :LANES] / mixed[3, :, LANES:]
    ).astype(out_ref.dtype)


def attention(
    latent, rope_key, wide_query, narrow_query, wide_key, wide_value, narrow_key, narrow_value, gain
):
    tokens, width = latent.shape
    n_sp, n_tp = lax.axis_size("sp"), lax.axis_size("tp")
    zn = n_sp // 2
    assert n_sp % 4 == 0 and n_tp == 4 and wide_query.shape[1] == 3 * LANES
    assert narrow_query.shape[1] == 2 * LANES and zn >= 4
    local_cos, local_sin = angle_tables(np.arange(tokens, dtype=np.float64))
    base_cos, base_sin = angle_tables(np.arange(n_sp, dtype=np.float64) * tokens)
    hops = zn // 2 + 1
    dma = pltpu.SemaphoreType.DMA
    vmem = pl.BlockSpec(memory_space=pltpu.VMEM)
    return pl.pallas_call(
        functools.partial(attention_kernel, n_sp, n_tp),
        out_shape=jax.ShapeDtypeStruct((tokens, 3 * LANES), jnp.bfloat16),
        in_specs=[pl.BlockSpec(memory_space=pltpu.HBM)] * 13,
        out_specs=vmem,
        scratch_shapes=[
            pltpu.VMEM(latent.shape, jnp.bfloat16),
            pltpu.VMEM(rope_key.shape[::-1], jnp.bfloat16),
            pltpu.VMEM(wide_query.shape, jnp.bfloat16),
            pltpu.VMEM(narrow_query.shape, jnp.bfloat16),
            pltpu.VMEM(wide_key.shape, jnp.bfloat16),
            pltpu.VMEM(wide_value.shape, jnp.bfloat16),
            pltpu.VMEM((1, width), jnp.float32),
            pltpu.VMEM(local_cos.shape, jnp.float32),
            pltpu.VMEM(local_sin.shape, jnp.float32),
            pltpu.VMEM(base_cos.shape, jnp.float32),
            pltpu.VMEM(base_sin.shape, jnp.float32),
            pltpu.VMEM((n_sp, n_tp, tokens // n_tp, width + LANES), jnp.bfloat16),
            pltpu.VMEM((4, tokens, 2 * LANES), jnp.bfloat16),
            pltpu.VMEM((width, 2 * LANES), jnp.bfloat16),
            pltpu.VMEM((4, tokens, LANES), jnp.float32),
            pltpu.VMEM((4, tokens, 2 * LANES), jnp.float32),
            dma((13,)),
            dma((2, hops, 2)),
            dma((2, hops + 1, 2)),
            dma((2, hops, 2)),
            dma((2, hops, 2)),
            dma((2, hops)),
            dma((2, hops)),
        ],
        compiler_params=pltpu.CompilerParams(
            collective_id=0, has_side_effects=True, vmem_limit_bytes=VMEM_BYTES
        ),
    )(
        latent,
        rope_key.T,
        wide_query,
        narrow_query,
        wide_key,
        wide_value,
        narrow_key,
        narrow_value,
        gain.reshape(1, width),
        local_cos,
        local_sin,
        base_cos,
        base_sin,
    )


DELTAS = ((0, 8, 7, -7, 4, -4, 1, -1), (6, -6, 5, -5, 3, -3, 2, -2))
COLUMNS = 1024
CAPACITY = 2


def silu(v):
    return v / (1.0 + jnp.exp(-v))


def experts_kernel(
    n_sp,
    n_tp,
    mix_ref,
    routes_hbm,
    weight_hbm,
    out_wide_hbm,
    out_narrow_hbm,
    residual_hbm,
    gain_hbm,
    shared_gate_hbm,
    shared_up_hbm,
    shared_down_hbm,
    expert_gate_hbm,
    expert_up_hbm,
    expert_down_hbm,
    out_ref,
    routes_ref,
    weight_ref,
    places,
    out_weight,
    residual_ref,
    gain_ref,
    shared_in,
    shared_down,
    expert_in,
    expert_down,
    part,
    opposite,
    summed,
    landed,
    stream,
    gathered,
    outgoing,
    first_recv,
    first_relay,
    second_send,
    second_recv,
    finished,
    back_recv,
    back_send,
    back_relay,
    returned,
    shared_send,
    shared_recv,
    fetch,
    send_sems,
    recv_sems,
):
    rows, depth = residual_hbm.shape
    half = depth // 2
    zn = n_sp // 2
    lanes = 2 * n_tp
    piece = outgoing.shape[1]
    wide_rows = out_wide_hbm.shape[0]
    ff = shared_gate_hbm.shape[1]
    hidden = expert_gate_hbm.shape[1]
    top_count = routes_hbm.shape[0]
    me = lax.axis_index("sp")
    x = lax.axis_index("tp")
    z = me // 2
    core = lax.rem(me, 2)
    lane = core * n_tp + x

    def at_plane(delta):
        return lax.rem(z + (delta + zn), zn)

    def on_plane(delta):
        return {"sp": at_plane(delta) * 2 + core}

    def along_x(dx):
        return {"tp": lax.rem(x + (dx + n_tp), n_tp)}

    def in_plane(dc, dx):
        other = 1 - core if dc else core
        return {"sp": z * 2 + other, "tp": lax.rem(x + (dx + n_tp), n_tp)}

    relative = [(dc, dx) for dc in range(2) for dx in range(n_tp)]

    taken = [0]

    def remote(source, target, place):
        i = taken[0]
        taken[0] += 1
        return pltpu.make_async_remote_copy(
            src_ref=source,
            dst_ref=target,
            send_sem=send_sems.at[i],
            recv_sem=recv_sems.at[i],
            device_id=place,
            device_id_type=pl.DeviceIdType.MESH,
        )

    barrier = pltpu.get_barrier_semaphore()
    greeted = [on_plane(d) for d in range(1, zn)] + [in_plane(dc, dx) for dc, dx in relative[1:]]
    for place in greeted:
        pl.semaphore_signal(barrier, inc=1, device_id=place, device_id_type=pl.DeviceIdType.MESH)

    fetches = [
        pltpu.make_async_copy(source, target, fetch.at[i])
        for i, (source, target) in enumerate(
            (
                (routes_hbm, routes_ref),
                (weight_hbm, weight_ref),
                (out_wide_hbm, out_weight.at[pl.ds(0, wide_rows)]),
                (out_narrow_hbm, out_weight.at[pl.ds(wide_rows, out_narrow_hbm.shape[0])]),
                (residual_hbm, residual_ref),
                (gain_hbm, gain_ref),
                (shared_gate_hbm, shared_in.at[:, pl.ds(0, ff)]),
                (shared_up_hbm, shared_in.at[:, pl.ds(ff, ff)]),
                (shared_down_hbm, shared_down),
                (expert_gate_hbm.at[0], expert_in.at[pl.ds(0, hidden)]),
                (expert_up_hbm.at[0], expert_in.at[pl.ds(hidden, hidden)]),
                (expert_down_hbm.at[0], expert_down),
            )
        )
    ]
    for copy in fetches:
        copy.start()

    def chunks():
        return [pl.ds(n, COLUMNS) for n in range(0, depth, COLUMNS)]

    def project(dx):
        q = pl.multiple_of(lax.rem(x + dx, n_tp) * rows, rows)
        mine = mix_ref[pl.ds(q, rows), :]
        for cols in chunks():
            part[dx, :, cols] = jnp.dot(
                mine, out_weight[:, cols], preferred_element_type=jnp.float32
            ).astype(jnp.bfloat16)

    lower, upper = pl.ds(0, half), pl.ds(half, half)
    for copy in fetches[:4]:
        copy.wait()
    project(2)
    pl.semaphore_wait(barrier, len(greeted))
    over_right = remote(part.at[2, :, lower], opposite.at[0], along_x(1))
    over_left = remote(part.at[2, :, upper], opposite.at[1], along_x(-1))
    over_right.start()
    over_left.start()
    project(1)
    straight_right = remote(part.at[1, :, upper], landed.at[0, 1], along_x(1))
    straight_right.start()
    project(3)
    straight_left = remote(part.at[3, :, lower], landed.at[1, 0], along_x(-1))
    straight_left.start()
    project(0)

    r0 = lax.broadcasted_iota(jnp.int32, (rows, rows), 0)
    r1 = lax.broadcasted_iota(jnp.int32, (rows, rows), 1)

    def upright(row):
        return jnp.sum(jnp.where(r0 == r1, row, 0.0), axis=1, keepdims=True)

    named = [routes_ref[c : c + 1, :].astype(jnp.float32) for c in range(top_count)]
    shares = [upright(weight_ref[c : c + 1, :]) for c in range(top_count)]
    slot = lax.broadcasted_iota(jnp.int32, (zn * piece, rows), 0).astype(jnp.float32)
    maps = []
    for c in range(top_count):
        earlier = jnp.zeros((1, rows), jnp.float32)
        for other in range(top_count):
            same = (upright(named[other]) == named[c]) & (r0 < r1)
            earlier = earlier + jnp.sum(jnp.where(same, 1.0, 0.0), axis=0, keepdims=True)
        maps.append(jnp.where(slot == named[c] * CAPACITY + earlier, 1.0, 0.0))
        places[c] = maps[c].T.astype(jnp.bfloat16)
    send_map = sum(maps[1:], maps[0]).astype(jnp.bfloat16)

    over_right.wait_recv()
    summed[0] = (part[1, :, lower].astype(jnp.float32) + opposite[0].astype(jnp.float32)).astype(jnp.bfloat16)
    joined_right = remote(summed.at[0], landed.at[0, 0], along_x(1))
    joined_right.start()
    over_left.wait_recv()
    summed[1] = (part[3, :, upper].astype(jnp.float32) + opposite[1].astype(jnp.float32)).astype(jnp.bfloat16)
    joined_left = remote(summed.at[1], landed.at[1, 1], along_x(-1))
    joined_left.start()
    fetches[4].wait()
    fetches[5].wait()
    for copy in (straight_right, straight_left, joined_right, joined_left):
        copy.wait_recv()
    for h, cols in enumerate((lower, upper)):
        stream[:, cols] = (
            residual_ref[:, cols].astype(jnp.float32)
            + part[0, :, cols].astype(jnp.float32)
            + landed[0, h].astype(jnp.float32)
            + landed[1, h].astype(jnp.float32)
        ).astype(jnp.bfloat16)
    gathered[0] = rms_scale(stream[...].astype(jnp.float32), gain_ref[...]).astype(jnp.bfloat16)

    for cols in chunks():
        outgoing[:, :, cols] = (
            jnp.dot(send_map, gathered[0, :, cols], preferred_element_type=jnp.float32)
            .astype(jnp.bfloat16)
            .reshape(zn, piece, COLUMNS)
        )
    sent = [over_right, over_left, straight_right, straight_left, joined_right, joined_left]
    far = at_plane(8)
    relay_up = remote(outgoing.at[far, :, lower], first_relay.at[0], on_plane(4))
    relay_down = remote(outgoing.at[far, :, upper], first_relay.at[1], on_plane(-4))
    relay_up.start()
    relay_down.start()
    first = [{}, {}]
    for ch in range(2):
        for j, delta in enumerate(DELTAS[ch]):
            if delta in (0, 8):
                continue
            first[ch][j] = remote(outgoing.at[at_plane(delta)], first_recv.at[ch, j], on_plane(delta))
            first[ch][j].start()
        if ch == 0:
            spread = [remote(gathered.at[0], gathered.at[dx], along_x(dx)) for dx in (1, 3, 2)]
            for copy in spread:
                copy.start()
    first_recv[0, 0] = outgoing[z]
    far_slot = DELTAS[0].index(8)
    onward_up = remote(first_relay.at[0], first_recv.at[0, far_slot, :, lower], on_plane(4))
    onward_down = remote(first_relay.at[1], first_recv.at[0, far_slot, :, upper], on_plane(-4))
    relay_up.wait_recv()
    onward_up.start()
    relay_down.wait_recv()
    onward_down.start()
    sent += [relay_up, relay_down, onward_up, onward_down] + spread
    sent += list(first[0].values()) + list(first[1].values())

    count = lanes * piece
    o = lax.broadcasted_iota(jnp.int32, (count, count), 0)
    i = lax.broadcasted_iota(jnp.int32, (count, count), 1)
    swap = jnp.where(
        (o // piece == (i % piece) // 2) & ((o % piece) // 2 == i // piece) & (o % 2 == i % 2), 1.0, 0.0
    ).astype(jnp.bfloat16)

    def swapped(source, target, ch):
        for cols in chunks():
            target[ch, :, :, cols] = (
                jnp.dot(
                    swap, source[ch, :, :, cols].reshape(count, COLUMNS), preferred_element_type=jnp.float32
                )
                .astype(jnp.bfloat16)
                .reshape(lanes, piece, COLUMNS)
            )

    def to_lanes(ch):
        swapped(first_recv, second_send, ch)
        copies = []
        for r, (dc, dx) in enumerate(relative):
            if r == 0:
                continue
            other = (1 - core if dc else core) * n_tp + lax.rem(x + dx, n_tp)
            copies.append(remote(second_send.at[ch, other], second_recv.at[ch, r], in_plane(dc, dx)))
            copies[-1].start()
        second_recv[ch, 0] = second_send[ch, lane]
        return copies

    def run_expert(ch):
        taken_in = second_recv[ch].reshape(count, depth)
        gate, lifted = (
            lax.dot_general(
                taken_in,
                expert_in[pl.ds(at, hidden), :],
                (((1,), (1,)), ((), ())),
                preferred_element_type=jnp.float32,
            )
            for at in (0, hidden)
        )
        active = (silu(gate) * lifted).astype(jnp.bfloat16)
        for cols in chunks():
            finished[ch, :, :, cols] = (
                jnp.dot(active, expert_down[:, cols], preferred_element_type=jnp.float32)
                .astype(jnp.bfloat16)
                .reshape(lanes, piece, COLUMNS)
            )
        copies = []
        for r, (dc, dx) in enumerate(relative):
            if r == 0:
                continue
            copies.append(remote(finished.at[ch, r], back_recv.at[ch, lane], in_plane(dc, -dx)))
            copies[-1].start()
        back_recv[ch, lane] = finished[ch, 0]
        return copies

    def home(ch):
        swapped(back_recv, back_send, ch)
        copies = []
        relays = []
        for j, delta in enumerate(DELTAS[ch]):
            if delta == 8:
                relays = [
                    remote(back_send.at[ch, j, :, lower], back_relay.at[0], on_plane(4)),
                    remote(back_send.at[ch, j, :, upper], back_relay.at[1], on_plane(-4)),
                ]
                for copy in relays:
                    copy.start()
        for j, delta in enumerate(DELTAS[ch]):
            if delta == 0:
                returned[z] = back_send[ch, j]
            elif delta != 8:
                copies.append(remote(back_send.at[ch, j], returned.at[z], on_plane(-delta)))
                copies[-1].start()
        return copies, relays

    for copy in list(first[0].values()) + [onward_up, onward_down]:
        copy.wait_recv()
    lane_copies = to_lanes(0)

    for copy in fetches[6:]:
        copy.wait()
    for copy in spread:
        copy.wait_recv()
    every = gathered[...].reshape(n_tp * rows, depth)
    both = jnp.dot(every, shared_in[...], preferred_element_type=jnp.float32)
    act = (silu(both[:, :ff]) * both[:, ff:]).astype(jnp.bfloat16)
    for cols in chunks():
        shared_send[:, :, cols] = (
            jnp.dot(act, shared_down[:, cols], preferred_element_type=jnp.float32)
            .astype(jnp.bfloat16)
            .reshape(n_tp, rows, COLUMNS)
        )

    for copy in lane_copies:
        copy.wait_recv()
    back_copies = run_expert(0)
    for copy in back_copies:
        copy.wait_recv()
    home_copies, relays = home(0)
    sent += lane_copies + back_copies + home_copies + relays

    for copy in first[1].values():
        copy.wait_recv()
    lane_copies = to_lanes(1)
    relays[0].wait_recv()
    last_up = remote(back_relay.at[0], returned.at[at_plane(-4), :, lower], on_plane(4))
    last_up.start()
    relays[1].wait_recv()
    last_down = remote(back_relay.at[1], returned.at[at_plane(4), :, upper], on_plane(-4))
    last_down.start()
    for copy in lane_copies:
        copy.wait_recv()
    back_copies = run_expert(1)
    shared_back = [remote(shared_send.at[dx], shared_recv.at[dx - 1], along_x(-dx)) for dx in range(1, n_tp)]
    for copy in shared_back:
        copy.start()
    sent += shared_back
    for copy in back_copies:
        copy.wait_recv()
    more_home, _ = home(1)
    sent += lane_copies + back_copies + more_home + [last_up, last_down]

    for copy in shared_back:
        copy.wait_recv()
    for copy in home_copies + more_home + [last_up, last_down]:
        copy.wait_recv()
    for cols in chunks():
        total = stream[:, cols].astype(jnp.float32) + shared_send[0, :, cols].astype(jnp.float32)
        for dx in range(n_tp - 1):
            total = total + shared_recv[dx, :, cols].astype(jnp.float32)
        results = returned[:, :, cols].reshape(zn * piece, COLUMNS)
        for c in range(top_count):
            total = total + shares[c] * jnp.dot(places[c], results, preferred_element_type=jnp.float32)
        out_ref[:, cols] = total.astype(out_ref.dtype)
    for copy in sent:
        copy.wait_send()


def projected_experts(
    mix,
    routes,
    route_weights,
    out_wide,
    out_narrow,
    residual,
    gain,
    shared_gate,
    shared_up,
    shared_down,
    expert_gate,
    expert_up,
    expert_down,
):
    rows, depth = residual.shape
    n_sp, n_tp = lax.axis_size("sp"), lax.axis_size("tp")
    zn, lanes = n_sp // 2, 2 * n_tp
    piece = CAPACITY * lanes
    ff = shared_gate.shape[1]
    hidden = expert_gate.shape[2]
    assert zn == 16 and n_tp == 4 and expert_gate.shape[0] == 1
    vmem, hbm = pl.BlockSpec(memory_space=pltpu.VMEM), pl.BlockSpec(memory_space=pltpu.HBM)
    bf16 = jnp.bfloat16
    chunk = (2, lanes, piece, depth)
    dma = pltpu.SemaphoreType.DMA
    return pl.pallas_call(
        functools.partial(experts_kernel, n_sp, n_tp),
        out_shape=jax.ShapeDtypeStruct((rows, depth), bf16),
        in_specs=[vmem] + [hbm] * 12,
        out_specs=vmem,
        scratch_shapes=[
            pltpu.VMEM(routes.shape[::-1], jnp.int32),
            pltpu.VMEM(route_weights.shape[::-1], jnp.float32),
            pltpu.VMEM((routes.shape[1], rows, zn * piece), bf16),
            pltpu.VMEM((out_wide.shape[0] + out_narrow.shape[0], depth), bf16),
            pltpu.VMEM((rows, depth), bf16),
            pltpu.VMEM((1, depth), jnp.float32),
            pltpu.VMEM((depth, 2 * ff), bf16),
            pltpu.VMEM(shared_down.shape, bf16),
            pltpu.VMEM((2 * hidden, depth), bf16),
            pltpu.VMEM(expert_down.shape[1:], bf16),
            pltpu.VMEM((n_tp, rows, depth), bf16),
            pltpu.VMEM((2, rows, depth // 2), bf16),
            pltpu.VMEM((2, rows, depth // 2), bf16),
            pltpu.VMEM((2, 2, rows, depth // 2), bf16),
            pltpu.VMEM((rows, depth), bf16),
            pltpu.VMEM((n_tp, rows, depth), bf16),
            pltpu.VMEM((zn, piece, depth), bf16),
            pltpu.VMEM(chunk, bf16),
            pltpu.VMEM((2, piece, depth // 2), bf16),
            pltpu.VMEM(chunk, bf16),
            pltpu.VMEM(chunk, bf16),
            pltpu.VMEM(chunk, bf16),
            pltpu.VMEM(chunk, bf16),
            pltpu.VMEM(chunk, bf16),
            pltpu.VMEM((2, piece, depth // 2), bf16),
            pltpu.VMEM((zn, piece, depth), bf16),
            pltpu.VMEM((n_tp, rows, depth), bf16),
            pltpu.VMEM((n_tp - 1, rows, depth), bf16),
            dma((12,)),
            dma((80,)),
            dma((80,)),
        ],
        compiler_params=pltpu.CompilerParams(
            collective_id=1, has_side_effects=True, vmem_limit_bytes=VMEM_BYTES
        ),
    )(
        mix,
        routes.T,
        route_weights.T,
        out_wide,
        out_narrow,
        residual,
        gain.reshape(1, depth),
        shared_gate,
        shared_up,
        shared_down,
        jnp.swapaxes(expert_gate, 1, 2),
        jnp.swapaxes(expert_up, 1, 2),
        expert_down,
    )


def body(
    latent,
    rope_key,
    wide_query,
    narrow_query,
    wide_key_weight,
    wide_value_weight,
    narrow_key_weight,
    narrow_value_weight,
    latent_norm_scale,
    out_wide,
    out_narrow,
    residual,
    ffn_gain,
    shared_gate,
    shared_up,
    shared_down,
    expert_gate,
    expert_up,
    expert_down,
    routes,
    route_weights,
):
    mix = attention(
        latent,
        rope_key,
        wide_query,
        narrow_query,
        wide_key_weight,
        wide_value_weight,
        narrow_key_weight,
        narrow_value_weight,
        latent_norm_scale,
    )
    return projected_experts(
        mix,
        routes,
        route_weights,
        out_wide,
        out_narrow,
        residual,
        ffn_gain,
        shared_gate,
        shared_up,
        shared_down,
        expert_gate,
        expert_up,
        expert_down,
    )


def solution(mesh):
    placed = (
        P(("grp", "sp"), None),
        P(("grp", "sp"), None),
        P(("grp", "sp"), "tp"),
        P(("grp", "sp"), "tp"),
        P(None, "tp"),
        P(None, "tp"),
        P(None, "tp"),
        P(None, "tp"),
        P(),
        P("tp", None),
        P("tp", None),
        P(("grp", "sp", "tp"), None),
        P(),
        P(None, "tp"),
        P(None, "tp"),
        P("tp", None),
        P(("sp", "tp"), None, None),
        P(("sp", "tp"), None, None),
        P(("sp", "tp"), None, None),
        P(("grp", "sp", "tp"), None),
        P(("grp", "sp", "tp"), None),
    )
    return jax.shard_map(
        body, mesh=mesh, in_specs=placed, out_specs=P(("grp", "sp", "tp"), None), check_vma=False
    )
```

```python
import functools

import jax
import jax.numpy as jnp
import numpy as np
from jax import lax
from jax.experimental import pallas as pl
from jax.experimental.pallas import tpu as pltpu
from jax.sharding import PartitionSpec as P

ROPE = 64
WIDE_HEAD_SIZE = 128
NARROW_HEAD_SIZE = 64
LANES = 128
VMEM_BYTES = 67_043_328


EPS = 1e-06
ROPE_BASE = 10000.0
NEG_FILL = -1e30
LOG2E = 1.4426950408889634


def rms_scale(values, gain):
    return values * lax.rsqrt(jnp.mean(values * values, axis=-1, keepdims=True) + EPS) * gain


def angle_tables(positions):
    half = ROPE // 2
    inverse = ROPE_BASE ** (-np.arange(half) * 2.0 / ROPE)
    angles = positions[:, None] * np.concatenate([inverse, inverse])[None, :]
    pad = ((0, 0), (0, LANES - ROPE))
    return (
        np.pad(np.cos(angles), pad).astype(np.float32),
        np.pad(np.sin(angles), pad).astype(np.float32),
    )


def attention_kernel(
    n_sp,
    n_tp,
    latent_hbm,
    rope_key_hbm,
    wide_query_hbm,
    narrow_query_hbm,
    wide_key_hbm,
    wide_value_hbm,
    narrow_key_hbm,
    narrow_value_hbm,
    gain_hbm,
    local_cos_hbm,
    local_sin_hbm,
    base_cos_hbm,
    base_sin_hbm,
    out_ref,
    latent_ref,
    rope_key_ref,
    wide_query_ref,
    narrow_query_ref,
    wide_key_ref,
    wide_value_ref,
    gain_ref,
    local_cos_ref,
    local_sin_ref,
    base_cos_ref,
    base_sin_ref,
    rows_buf,
    queries,
    narrow_weight,
    top,
    mixed,
    fetch,
    z_send,
    z_recv,
    x_send,
    x_recv,
    d_send,
    d_recv,
    wrap_open,
):
    tokens, width = latent_hbm.shape
    quarter = tokens // n_tp
    zn = n_sp // 2
    steps_up = zn // 2
    steps_down = zn - 1 - steps_up
    me = lax.axis_index("sp")
    x = lax.axis_index("tp")
    z = me // 2
    core = lax.rem(me, 2)
    right = lax.rem(x + 1, n_tp)
    left = lax.rem(x + n_tp - 1, n_tp)
    up = lax.rem(z + 1, zn)
    down = lax.rem(z + zn - 1, zn)
    partner = z * 2 + 1 - core

    fetches = [
        pltpu.make_async_copy(source, target, fetch.at[i])
        for i, (source, target) in enumerate(
            (
                (latent_hbm, latent_ref),
                (rope_key_hbm, rope_key_ref),
                (gain_hbm, gain_ref),
                (local_cos_hbm, local_cos_ref),
                (local_sin_hbm, local_sin_ref),
                (base_cos_hbm, base_cos_ref),
                (base_sin_hbm, base_sin_ref),
                (wide_query_hbm, wide_query_ref),
                (narrow_query_hbm, narrow_query_ref),
                (wide_key_hbm, wide_key_ref),
                (wide_value_hbm, wide_value_ref),
                (narrow_key_hbm, narrow_weight.at[:, pl.ds(0, LANES)]),
                (narrow_value_hbm, narrow_weight.at[:, pl.ds(LANES, LANES)]),
            )
        )
    ]
    for copy in fetches:
        copy.start()

    barrier = pltpu.get_barrier_semaphore()
    for place in ({"sp": down * 2 + core}, {"sp": partner}, {"tp": left}, {"tp": right}):
        pl.semaphore_signal(barrier, inc=1, device_id=place, device_id_type=pl.DeviceIdType.MESH)

    above = {"sp": up * 2 + core}

    @pl.when(z < zn - 1)
    def _():
        pl.semaphore_signal(barrier, inc=1, device_id=above, device_id_type=pl.DeviceIdType.MESH)


    for copy in fetches:
        copy.wait()
    lane = lax.broadcasted_iota(jnp.int32, (tokens, LANES), 1)
    low = lane < ROPE
    lc, ls = local_cos_ref[...], local_sin_ref[...]
    bc, bs = base_cos_ref[pl.ds(me, 1), :], base_sin_ref[pl.ds(me, 1), :]
    cosine = lc * bc - ls * bs
    sine = jnp.where(lane < ROPE // 2, -1.0, 1.0) * (ls * bc + lc * bs)

    def turn(v):
        other = jnp.where(
            lane < ROPE // 2, pltpu.roll(v, LANES - ROPE // 2, 1), pltpu.roll(v, ROPE // 2, 1)
        )
        return (v * cosine + other * sine).astype(jnp.bfloat16)

    lat = latent_ref[...].astype(jnp.float32)
    normed = rms_scale(lat, gain_ref[...]).astype(jnp.bfloat16)
    rope = rope_key_ref[...].astype(jnp.float32).T
    turned = turn(jnp.concatenate([rope, jnp.zeros_like(rope)], axis=1))
    for q in range(n_tp):
        rows_buf[me, q, :, :width] = normed[q * quarter : (q + 1) * quarter]
        rows_buf[me, q, :, width:] = turned[q * quarter : (q + 1) * quarter]

    t1 = wide_query_ref[:, LANES : 2 * LANES].astype(jnp.float32)
    t2 = wide_query_ref[:, 2 * LANES :].astype(jnp.float32)
    n0 = narrow_query_ref[:, :LANES].astype(jnp.float32)
    n1 = narrow_query_ref[:, LANES:].astype(jnp.float32)
    half = LANES // 2
    queries[0, :, :LANES] = wide_query_ref[:, :LANES]
    queries[0, :, LANES:] = turn(t1)
    queries[1, :, :LANES] = pltpu.roll(jnp.where(low, t2, t1), half, 1).astype(jnp.bfloat16)
    queries[1, :, LANES:] = turn(pltpu.roll(t2, half, 1))
    queries[2, :, :LANES] = jnp.where(low, n0, 0.0).astype(jnp.bfloat16)
    queries[2, :, LANES:] = turn(pltpu.roll(n0, half, 1))
    queries[3, :, :LANES] = pltpu.roll(jnp.where(low, n1, 0.0), half, 1).astype(jnp.bfloat16)
    queries[3, :, LANES:] = turn(pltpu.roll(n1, half, 1))
    top[...] = jnp.full(top.shape, NEG_FILL, jnp.float32)
    mixed[...] = jnp.zeros(mixed.shape, jnp.float32)

    @pl.when(z > 0)
    def _():
        pl.semaphore_wait(barrier, 5)

    @pl.when(z == 0)
    def _():
        pl.semaphore_wait(barrier, 4)

    @pl.when(z == zn - 1)
    def _():
        pl.semaphore_signal(wrap_open, inc=1, device_id=above, device_id_type=pl.DeviceIdType.MESH)

    def along_z(d, k, j):
        block = jnp.where(d == 0, z - k + zn, z + k) % zn
        target = jnp.where(d == 0, up, down)
        q = lax.rem(x + j, n_tp)
        spot = rows_buf.at[block * 2 + core, q]
        return pltpu.make_async_remote_copy(
            src_ref=spot,
            dst_ref=spot,
            send_sem=z_send.at[d, k, j],
            recv_sem=z_recv.at[d, k + 1, j],
            device_id={"sp": target * 2 + core},
            device_id_type=pl.DeviceIdType.MESH,
        )

    def along_x(d, k, j):
        block = jnp.where(d == 0, z - k + zn, z + k) % zn
        q = lax.rem(x + j, n_tp)
        spot = rows_buf.at[block * 2 + core, q]
        return pltpu.make_async_remote_copy(
            src_ref=spot,
            dst_ref=spot,
            send_sem=x_send.at[d, k, j],
            recv_sem=x_recv.at[d, k, j],
            device_id={"tp": right if j == 0 else left},
            device_id_type=pl.DeviceIdType.MESH,
        )

    def to_partner(d, k):
        block = jnp.where(d == 0, z - k + zn, z + k) % zn
        spot = rows_buf.at[block * 2 + core]
        return pltpu.make_async_remote_copy(
            src_ref=spot,
            dst_ref=spot,
            send_sem=d_send.at[d, k],
            recv_sem=d_recv.at[d, k],
            device_id={"sp": partner},
            device_id_type=pl.DeviceIdType.MESH,
        )

    def arrives(d, k):
        going_up = (k <= z) & (k <= steps_up)
        going_down = ((z + k) % zn < steps_down) & (k <= steps_down)
        return jnp.where(d == 0, going_up, going_down)

    def goes_on(d, k):
        going_up = (k <= z) & (k < steps_up) & (z + 1 < zn)
        going_down = ((z + k) % zn < steps_down) & (k < steps_down)
        return jnp.where(d == 0, going_up, going_down)

    def seen(d, k):
        going_up = (k <= z) & (k <= steps_up)
        going_down = (z + k >= zn) & (z + k - zn < steps_down) & (k <= steps_down)
        return (k >= 1) & jnp.where(d == 0, going_up, going_down)

    wide_factor = (WIDE_HEAD_SIZE + ROPE) ** (-0.5) * LOG2E
    narrow_factor = (NARROW_HEAD_SIZE + ROPE) ** (-0.5) * LOG2E

    def attend(plane, own):
        rows = rows_buf[pl.ds(plane * 2, 2)].reshape(2 * tokens, width + LANES)
        latents, turned_rows = rows[:, :width], rows[:, width:]
        keys = 2 * tokens
        ones = jnp.ones((keys, LANES), jnp.bfloat16)

        def up_from(weight):
            return jnp.dot(latents, weight[...], preferred_element_type=jnp.float32).astype(jnp.bfloat16)

        wide_k, wide_v, narrow = up_from(wide_key_ref), up_from(wide_value_ref), up_from(narrow_weight)
        narrow_k = jnp.concatenate([narrow[:, :LANES], turned_rows], axis=1)
        narrow_v = jnp.concatenate([narrow[:, LANES:], ones], axis=1)
        if own:
            gap = lax.broadcasted_iota(jnp.int32, (tokens, keys), 1) - lax.broadcasted_iota(
                jnp.int32, (tokens, keys), 0
            )
            visible = gap <= core * tokens
        for h in range(4):
            if h < 2:
                at = slice(h * LANES, (h + 1) * LANES)
                k_h = jnp.concatenate([wide_k[:, at], turned_rows], axis=1)
                v_h = jnp.concatenate([wide_v[:, at], ones], axis=1)
            else:
                k_h, v_h = narrow_k, narrow_v
            scores = lax.dot_general(
                queries[h], k_h, (((1,), (1,)), ((), ())), preferred_element_type=jnp.float32
            ) * (wide_factor if h < 2 else narrow_factor)
            if own:
                scores = jnp.where(visible, scores, NEG_FILL)
            old = top[h]
            new = jnp.maximum(old, jnp.max(scores, axis=1, keepdims=True))
            top[h] = new
            weights = jnp.exp2(scores - jnp.concatenate([new] * (keys // LANES), axis=1)).astype(jnp.bfloat16)
            fading = jnp.exp2(old - new)
            mixed[h] = mixed[h] * jnp.concatenate([fading, fading], axis=1) + jnp.dot(
                weights, v_h, preferred_element_type=jnp.float32
            )

    to_partner(0, 0).start()
    for d in range(2):

        @pl.when(goes_on(d, 0) & ((d == 0) | (z > 0)))
        def _():
            for j in range(2):
                along_z(d, 0, j).start()

    to_partner(0, 0).wait_recv()

    attend(z, True)

    @pl.when(z == 0)
    def _():
        pl.semaphore_wait(wrap_open, 1)
        for j in range(2):
            along_z(1, 0, j).start()

    def one_step(k, carry):
        def forward(d, c):
            @pl.when(arrives(d, k))
            def _():
                for j in range(2):
                    along_z(d, k - 1, j).wait_recv()

            @pl.when(goes_on(d, k))
            def _():
                for j in range(2):
                    along_z(d, k, j).start()

            @pl.when(seen(d, k))
            def _():
                for j in range(2):
                    along_x(d, k, j).start()

            @pl.when(seen(d, k - 1))
            def _():
                for j in range(2):
                    along_x(d, k - 1, j).wait_recv()
                to_partner(d, k - 1).start()

            return c

        lax.fori_loop(0, 2, forward, 0)

        def work(d, c):
            @pl.when(seen(d, k - 2))
            def _():
                to_partner(d, k - 2).wait_recv()
                attend(jnp.where(d == 0, z - k + 2, z + k - 2 - zn), False)

            return c

        lax.fori_loop(0, 2, work, 0)
        return carry

    lax.fori_loop(1, steps_up + 3, one_step, 0)

    to_partner(0, 0).wait_send()

    def settle(k, carry):
        def both(d, c):
            @pl.when(goes_on(d, k))
            def _():
                for j in range(2):
                    along_z(d, k, j).wait_send()

            @pl.when(seen(d, k))
            def _():
                for j in range(2):
                    along_x(d, k, j).wait_send()
                to_partner(d, k).wait_send()

            return c

        return lax.fori_loop(0, 2, both, carry)

    lax.fori_loop(0, steps_up + 1, settle, 0)

    for h in range(2):
        out_ref[:, h * LANES : (h + 1) * LANES] = (mixed[h, :, :LANES] / mixed[h, :, LANES:]).astype(
            out_ref.dtype
        )
    out_ref[:, 2 * LANES :] = jnp.where(
        low, mixed[2, :, :LANES] / mixed[2, :, LANES:], mixed[3, :, :LANES] / mixed[3, :, LANES:]
    ).astype(out_ref.dtype)


def attention(
    latent, rope_key, wide_query, narrow_query, wide_key, wide_value, narrow_key, narrow_value, gain
):
    tokens, width = latent.shape
    n_sp, n_tp = lax.axis_size("sp"), lax.axis_size("tp")
    zn = n_sp // 2
    assert n_sp % 4 == 0 and n_tp == 4 and wide_query.shape[1] == 3 * LANES
    assert narrow_query.shape[1] == 2 * LANES and zn >= 4
    local_cos, local_sin = angle_tables(np.arange(tokens, dtype=np.float64))
    base_cos, base_sin = angle_tables(np.arange(n_sp, dtype=np.float64) * tokens)
    hops = zn // 2 + 1
    dma = pltpu.SemaphoreType.DMA
    vmem = pl.BlockSpec(memory_space=pltpu.VMEM)
    return pl.pallas_call(
        functools.partial(attention_kernel, n_sp, n_tp),
        out_shape=jax.ShapeDtypeStruct((tokens, 3 * LANES), jnp.bfloat16),
        in_specs=[pl.BlockSpec(memory_space=pltpu.HBM)] * 13,
        out_specs=vmem,
        scratch_shapes=[
            pltpu.VMEM(latent.shape, jnp.bfloat16),
            pltpu.VMEM(rope_key.shape[::-1], jnp.bfloat16),
            pltpu.VMEM(wide_query.shape, jnp.bfloat16),
            pltpu.VMEM(narrow_query.shape, jnp.bfloat16),
            pltpu.VMEM(wide_key.shape, jnp.bfloat16),
            pltpu.VMEM(wide_value.shape, jnp.bfloat16),
            pltpu.VMEM((1, width), jnp.float32),
            pltpu.VMEM(local_cos.shape, jnp.float32),
            pltpu.VMEM(local_sin.shape, jnp.float32),
            pltpu.VMEM(base_cos.shape, jnp.float32),
            pltpu.VMEM(base_sin.shape, jnp.float32),
            pltpu.VMEM((n_sp, n_tp, tokens // n_tp, width + LANES), jnp.bfloat16),
            pltpu.VMEM((4, tokens, 2 * LANES), jnp.bfloat16),
            pltpu.VMEM((width, 2 * LANES), jnp.bfloat16),
            pltpu.VMEM((4, tokens, LANES), jnp.float32),
            pltpu.VMEM((4, tokens, 2 * LANES), jnp.float32),
            dma((13,)),
            dma((2, hops, 2)),
            dma((2, hops + 1, 2)),
            dma((2, hops, 2)),
            dma((2, hops, 2)),
            dma((2, hops)),
            dma((2, hops)),
            pltpu.SemaphoreType.REGULAR,
        ],
        compiler_params=pltpu.CompilerParams(
            collective_id=0, has_side_effects=True, vmem_limit_bytes=VMEM_BYTES
        ),
    )(
        latent,
        rope_key.T,
        wide_query,
        narrow_query,
        wide_key,
        wide_value,
        narrow_key,
        narrow_value,
        gain.reshape(1, width),
        local_cos,
        local_sin,
        base_cos,
        base_sin,
    )


DELTAS = ((0, 8, 7, -7, 4, -4, 1, -1), (6, -6, 5, -5, 3, -3, 2, -2))
COLUMNS = 1024
CAPACITY = 2


def silu(v):
    return v / (1.0 + jnp.exp(-v))


def experts_kernel(
    n_sp,
    n_tp,
    mix_ref,
    routes_hbm,
    weight_hbm,
    out_wide_hbm,
    out_narrow_hbm,
    residual_hbm,
    gain_hbm,
    shared_gate_hbm,
    shared_up_hbm,
    shared_down_hbm,
    expert_gate_hbm,
    expert_up_hbm,
    expert_down_hbm,
    out_ref,
    routes_ref,
    weight_ref,
    places,
    out_weight,
    residual_ref,
    gain_ref,
    shared_in,
    shared_down,
    expert_in,
    expert_down,
    part,
    opposite,
    summed,
    landed,
    stream,
    gathered,
    outgoing,
    first_recv,
    first_relay,
    second_send,
    second_recv,
    finished,
    back_recv,
    back_send,
    back_relay,
    returned,
    shared_send,
    shared_recv,
    fetch,
    send_sems,
    recv_sems,
):
    rows, depth = residual_hbm.shape
    half = depth // 2
    zn = n_sp // 2
    lanes = 2 * n_tp
    piece = outgoing.shape[1]
    wide_rows = out_wide_hbm.shape[0]
    ff = shared_gate_hbm.shape[1]
    hidden = expert_gate_hbm.shape[1]
    top_count = routes_hbm.shape[0]
    me = lax.axis_index("sp")
    x = lax.axis_index("tp")
    z = me // 2
    core = lax.rem(me, 2)
    lane = core * n_tp + x

    def at_plane(delta):
        return lax.rem(z + (delta + zn), zn)

    def on_plane(delta):
        return {"sp": at_plane(delta) * 2 + core}

    def along_x(dx):
        return {"tp": lax.rem(x + (dx + n_tp), n_tp)}

    def in_plane(dc, dx):
        other = 1 - core if dc else core
        return {"sp": z * 2 + other, "tp": lax.rem(x + (dx + n_tp), n_tp)}

    relative = [(dc, dx) for dc in range(2) for dx in range(n_tp)]

    taken = [0]

    def remote(source, target, place):
        i = taken[0]
        taken[0] += 1
        return pltpu.make_async_remote_copy(
            src_ref=source,
            dst_ref=target,
            send_sem=send_sems.at[i],
            recv_sem=recv_sems.at[i],
            device_id=place,
            device_id_type=pl.DeviceIdType.MESH,
        )

    barrier = pltpu.get_barrier_semaphore()
    greeted = [on_plane(d) for d in range(1, zn)] + [in_plane(dc, dx) for dc, dx in relative[1:]]
    for place in greeted:
        pl.semaphore_signal(barrier, inc=1, device_id=place, device_id_type=pl.DeviceIdType.MESH)

    fetches = [
        pltpu.make_async_copy(source, target, fetch.at[i])
        for i, (source, target) in enumerate(
            (
                (routes_hbm, routes_ref),
                (weight_hbm, weight_ref),
                (out_wide_hbm, out_weight.at[pl.ds(0, wide_rows)]),
                (out_narrow_hbm, out_weight.at[pl.ds(wide_rows, out_narrow_hbm.shape[0])]),
                (residual_hbm, residual_ref),
                (gain_hbm, gain_ref),
                (shared_gate_hbm, shared_in.at[:, pl.ds(0, ff)]),
                (shared_up_hbm, shared_in.at[:, pl.ds(ff, ff)]),
                (shared_down_hbm, shared_down),
                (expert_gate_hbm.at[0], expert_in.at[pl.ds(0, hidden)]),
                (expert_up_hbm.at[0], expert_in.at[pl.ds(hidden, hidden)]),
                (expert_down_hbm.at[0], expert_down),
            )
        )
    ]
    for copy in fetches:
        copy.start()

    def normed(values):
        return rms_scale(values.astype(jnp.float32), gain_ref[...]).astype(jnp.bfloat16)

    def chunks():
        return [pl.ds(n, COLUMNS) for n in range(0, depth, COLUMNS)]

    half_cols = (pl.ds(0, half), pl.ds(half, half))
    lower, upper = half_cols
    split = half // 2

    def sides(g):
        return pl.ds(g * half, split), pl.ds(g * half + split, split)

    def project(dx, g):
        q = pl.multiple_of(lax.rem(x + dx, n_tp) * rows, rows)
        mine = mix_ref[pl.ds(q, rows), :]
        for cols in sides(g):
            part[dx, :, cols] = jnp.dot(
                mine, out_weight[:, cols], preferred_element_type=jnp.float32
            ).astype(jnp.bfloat16)

    sent = []

    def begin(source, target, place):
        copy = remote(source, target, place)
        copy.start()
        sent.append(copy)
        return copy

    def to_opposite(g):
        left_side, right_side = sides(g)
        return (
            begin(part.at[2, :, left_side], opposite.at[g, 0], along_x(1)),
            begin(part.at[2, :, right_side], opposite.at[g, 1], along_x(-1)),
        )

    def straight(g):
        left_side, right_side = sides(g)
        return (
            begin(part.at[1, :, right_side], landed.at[g, 0, 1], along_x(1)),
            begin(part.at[3, :, left_side], landed.at[g, 1, 0], along_x(-1)),
        )

    def joined(g, waiting):
        copies = []
        for side, (dx, cols) in enumerate(zip((1, 3), sides(g))):
            waiting[side].wait_recv()
            summed[g, side] = (
                part[dx, :, cols].astype(jnp.float32) + opposite[g, side].astype(jnp.float32)
            ).astype(jnp.bfloat16)
            copies.append(
                begin(summed.at[g, side], landed.at[g, side, side], along_x(1 if side == 0 else -1))
            )
        return tuple(copies)

    def add_up(g, waiting):
        for copy in waiting:
            copy.wait_recv()
        for side, cols in enumerate(sides(g)):
            stream[:, cols] = (
                residual_ref[:, cols].astype(jnp.float32)
                + part[0, :, cols].astype(jnp.float32)
                + landed[g, 0, side].astype(jnp.float32)
                + landed[g, 1, side].astype(jnp.float32)
            ).astype(jnp.bfloat16)
        gathered[0, :, half_cols[g]] = stream[:, half_cols[g]]
        for cols in sides(g):
            outgoing[:, :, cols] = (
                jnp.dot(send_map, gathered[0, :, cols], preferred_element_type=jnp.float32)
                .astype(jnp.bfloat16)
                .reshape(zn, piece, split)
            )

    for copy in fetches[:4]:
        copy.wait()
    project(2, 0)
    pl.semaphore_wait(barrier, len(greeted))
    opposite_copies = [to_opposite(0)]
    project(1, 0)
    project(3, 0)
    straight_copies = [straight(0)]
    project(0, 0)

    r0 = lax.broadcasted_iota(jnp.int32, (rows, rows), 0)
    r1 = lax.broadcasted_iota(jnp.int32, (rows, rows), 1)

    def upright(row):
        return jnp.sum(jnp.where(r0 == r1, row, 0.0), axis=1, keepdims=True)

    named = [routes_ref[c : c + 1, :].astype(jnp.float32) for c in range(top_count)]
    shares = [upright(weight_ref[c : c + 1, :]) for c in range(top_count)]
    slot = lax.broadcasted_iota(jnp.int32, (zn * piece, rows), 0).astype(jnp.float32)
    maps = []
    for c in range(top_count):
        earlier = jnp.zeros((1, rows), jnp.float32)
        for other in range(top_count):
            same = (upright(named[other]) == named[c]) & (r0 < r1)
            earlier = earlier + jnp.sum(jnp.where(same, 1.0, 0.0), axis=0, keepdims=True)
        maps.append(jnp.where(slot == named[c] * CAPACITY + earlier, 1.0, 0.0))
        places[c] = maps[c].T.astype(jnp.bfloat16)
    send_map = sum(maps[1:], maps[0]).astype(jnp.bfloat16)

    project(2, 1)
    joined_copies = [joined(0, opposite_copies[0])]
    opposite_copies.append(to_opposite(1))
    project(1, 1)
    project(3, 1)
    straight_copies.append(straight(1))
    project(0, 1)
    for copy in fetches[4:6]:
        copy.wait()

    far = at_plane(8)
    first = [[], []]
    relays_in = []
    for g, cols in enumerate(half_cols):
        add_up(g, straight_copies[g] + joined_copies[g])
        relays_in.append(begin(outgoing.at[far, :, cols], first_relay.at[g], on_plane(4 if g == 0 else -4)))
        for j, delta in enumerate(DELTAS[0]):
            if delta not in (0, 8):
                first[0].append(
                    begin(outgoing.at[at_plane(delta), :, cols], first_recv.at[0, j, :, cols], on_plane(delta))
                )
        if g == 0:
            joined_copies.append(joined(1, opposite_copies[1]))
    for j, delta in enumerate(DELTAS[1]):
        first[1].append(begin(outgoing.at[at_plane(delta)], first_recv.at[1, j], on_plane(delta)))
    spread = [begin(gathered.at[0], gathered.at[dx], along_x(dx)) for dx in (1, 3, 2)]
    first_recv[0, 0] = outgoing[z]
    far_slot = DELTAS[0].index(8)
    for g, cols in enumerate(half_cols):
        relays_in[g].wait_recv()
        first[0].append(
            begin(first_relay.at[g], first_recv.at[0, far_slot, :, cols], on_plane(4 if g == 0 else -4))
        )

    count = lanes * piece
    o = lax.broadcasted_iota(jnp.int32, (count, count), 0)
    i = lax.broadcasted_iota(jnp.int32, (count, count), 1)
    swap = jnp.where(
        (o // piece == (i % piece) // 2) & ((o % piece) // 2 == i // piece) & (o % 2 == i % 2), 1.0, 0.0
    ).astype(jnp.bfloat16)

    def swapped(source, target, ch):
        for cols in chunks():
            target[ch, :, :, cols] = (
                jnp.dot(
                    swap, source[ch, :, :, cols].reshape(count, COLUMNS), preferred_element_type=jnp.float32
                )
                .astype(jnp.bfloat16)
                .reshape(lanes, piece, COLUMNS)
            )

    def to_lanes(ch):
        swapped(first_recv, second_send, ch)
        copies = []
        for r, (dc, dx) in enumerate(relative):
            if r == 0:
                continue
            other = (1 - core if dc else core) * n_tp + lax.rem(x + dx, n_tp)
            copies.append(remote(second_send.at[ch, other], second_recv.at[ch, r], in_plane(dc, dx)))
            copies[-1].start()
        second_recv[ch, 0] = second_send[ch, lane]
        return copies

    def run_expert(ch):
        taken_in = normed(second_recv[ch].reshape(count, depth))
        gate, lifted = (
            lax.dot_general(
                taken_in,
                expert_in[pl.ds(at, hidden), :],
                (((1,), (1,)), ((), ())),
                preferred_element_type=jnp.float32,
            )
            for at in (0, hidden)
        )
        active = (silu(gate) * lifted).astype(jnp.bfloat16)
        for cols in chunks():
            finished[ch, :, :, cols] = (
                jnp.dot(active, expert_down[:, cols], preferred_element_type=jnp.float32)
                .astype(jnp.bfloat16)
                .reshape(lanes, piece, COLUMNS)
            )
        copies = []
        for r, (dc, dx) in enumerate(relative):
            if r == 0:
                continue
            copies.append(remote(finished.at[ch, r], back_recv.at[ch, lane], in_plane(dc, -dx)))
            copies[-1].start()
        back_recv[ch, lane] = finished[ch, 0]
        return copies

    def home(ch):
        swapped(back_recv, back_send, ch)
        copies = []
        relays = []
        for j, delta in enumerate(DELTAS[ch]):
            if delta == 8:
                relays = [
                    remote(back_send.at[ch, j, :, lower], back_relay.at[0], on_plane(4)),
                    remote(back_send.at[ch, j, :, upper], back_relay.at[1], on_plane(-4)),
                ]
                for copy in relays:
                    copy.start()
        for j, delta in enumerate(DELTAS[ch]):
            if delta == 0:
                returned[z] = back_send[ch, j]
            elif delta != 8:
                copies.append(remote(back_send.at[ch, j], returned.at[z], on_plane(-delta)))
                copies[-1].start()
        return copies, relays

    for copy in first[0]:
        copy.wait_recv()
    lane_copies = to_lanes(0)

    for copy in fetches[6:]:
        copy.wait()
    for copy in spread:
        copy.wait_recv()
    every = normed(gathered[...].reshape(n_tp * rows, depth))
    both = jnp.dot(every, shared_in[...], preferred_element_type=jnp.float32)
    act = (silu(both[:, :ff]) * both[:, ff:]).astype(jnp.bfloat16)
    for cols in chunks():
        shared_send[:, :, cols] = (
            jnp.dot(act, shared_down[:, cols], preferred_element_type=jnp.float32)
            .astype(jnp.bfloat16)
            .reshape(n_tp, rows, COLUMNS)
        )

    for copy in lane_copies:
        copy.wait_recv()
    back_copies = run_expert(0)
    for copy in back_copies:
        copy.wait_recv()
    home_copies, relays = home(0)
    sent += lane_copies + back_copies + home_copies + relays

    for copy in first[1]:
        copy.wait_recv()
    lane_copies = to_lanes(1)
    relays[0].wait_recv()
    last_up = remote(back_relay.at[0], returned.at[at_plane(-4), :, lower], on_plane(4))
    last_up.start()
    relays[1].wait_recv()
    last_down = remote(back_relay.at[1], returned.at[at_plane(4), :, upper], on_plane(-4))
    last_down.start()
    for copy in lane_copies:
        copy.wait_recv()
    back_copies = run_expert(1)
    shared_back = [remote(shared_send.at[dx], shared_recv.at[dx - 1], along_x(-dx)) for dx in range(1, n_tp)]
    for copy in shared_back:
        copy.start()
    sent += shared_back
    for copy in back_copies:
        copy.wait_recv()
    more_home, _ = home(1)
    sent += lane_copies + back_copies + more_home + [last_up, last_down]

    for copy in shared_back:
        copy.wait_recv()
    for copy in home_copies + more_home + [last_up, last_down]:
        copy.wait_recv()
    for cols in chunks():
        total = stream[:, cols].astype(jnp.float32) + shared_send[0, :, cols].astype(jnp.float32)
        for dx in range(n_tp - 1):
            total = total + shared_recv[dx, :, cols].astype(jnp.float32)
        results = returned[:, :, cols].reshape(zn * piece, COLUMNS)
        for c in range(top_count):
            total = total + shares[c] * jnp.dot(places[c], results, preferred_element_type=jnp.float32)
        out_ref[:, cols] = total.astype(out_ref.dtype)
    for copy in sent:
        copy.wait_send()


def projected_experts(
    mix,
    routes,
    route_weights,
    out_wide,
    out_narrow,
    residual,
    gain,
    shared_gate,
    shared_up,
    shared_down,
    expert_gate,
    expert_up,
    expert_down,
):
    rows, depth = residual.shape
    n_sp, n_tp = lax.axis_size("sp"), lax.axis_size("tp")
    zn, lanes = n_sp // 2, 2 * n_tp
    piece = CAPACITY * lanes
    ff = shared_gate.shape[1]
    hidden = expert_gate.shape[2]
    assert zn == 16 and n_tp == 4 and expert_gate.shape[0] == 1
    vmem, hbm = pl.BlockSpec(memory_space=pltpu.VMEM), pl.BlockSpec(memory_space=pltpu.HBM)
    bf16 = jnp.bfloat16
    chunk = (2, lanes, piece, depth)
    dma = pltpu.SemaphoreType.DMA
    return pl.pallas_call(
        functools.partial(experts_kernel, n_sp, n_tp),
        out_shape=jax.ShapeDtypeStruct((rows, depth), bf16),
        in_specs=[vmem] + [hbm] * 12,
        out_specs=vmem,
        scratch_shapes=[
            pltpu.VMEM(routes.shape[::-1], jnp.int32),
            pltpu.VMEM(route_weights.shape[::-1], jnp.float32),
            pltpu.VMEM((routes.shape[1], rows, zn * piece), bf16),
            pltpu.VMEM((out_wide.shape[0] + out_narrow.shape[0], depth), bf16),
            pltpu.VMEM((rows, depth), bf16),
            pltpu.VMEM((1, depth), jnp.float32),
            pltpu.VMEM((depth, 2 * ff), bf16),
            pltpu.VMEM(shared_down.shape, bf16),
            pltpu.VMEM((2 * hidden, depth), bf16),
            pltpu.VMEM(expert_down.shape[1:], bf16),
            pltpu.VMEM((n_tp, rows, depth), bf16),
            pltpu.VMEM((2, 2, rows, depth // 4), bf16),
            pltpu.VMEM((2, 2, rows, depth // 4), bf16),
            pltpu.VMEM((2, 2, 2, rows, depth // 4), bf16),
            pltpu.VMEM((rows, depth), bf16),
            pltpu.VMEM((n_tp, rows, depth), bf16),
            pltpu.VMEM((zn, piece, depth), bf16),
            pltpu.VMEM(chunk, bf16),
            pltpu.VMEM((2, piece, depth // 2), bf16),
            pltpu.VMEM(chunk, bf16),
            pltpu.VMEM(chunk, bf16),
            pltpu.VMEM(chunk, bf16),
            pltpu.VMEM(chunk, bf16),
            pltpu.VMEM(chunk, bf16),
            pltpu.VMEM((2, piece, depth // 2), bf16),
            pltpu.VMEM((zn, piece, depth), bf16),
            pltpu.VMEM((n_tp, rows, depth), bf16),
            pltpu.VMEM((n_tp - 1, rows, depth), bf16),
            dma((12,)),
            dma((104,)),
            dma((104,)),
        ],
        compiler_params=pltpu.CompilerParams(
            collective_id=1, has_side_effects=True, vmem_limit_bytes=VMEM_BYTES
        ),
    )(
        mix,
        routes.T,
        route_weights.T,
        out_wide,
        out_narrow,
        residual,
        gain.reshape(1, depth),
        shared_gate,
        shared_up,
        shared_down,
        jnp.swapaxes(expert_gate, 1, 2),
        jnp.swapaxes(expert_up, 1, 2),
        expert_down,
    )


def body(
    latent,
    rope_key,
    wide_query,
    narrow_query,
    wide_key_weight,
    wide_value_weight,
    narrow_key_weight,
    narrow_value_weight,
    latent_norm_scale,
    out_wide,
    out_narrow,
    residual,
    ffn_gain,
    shared_gate,
    shared_up,
    shared_down,
    expert_gate,
    expert_up,
    expert_down,
    routes,
    route_weights,
):
    mix = attention(
        latent,
        rope_key,
        wide_query,
        narrow_query,
        wide_key_weight,
        wide_value_weight,
        narrow_key_weight,
        narrow_value_weight,
        latent_norm_scale,
    )
    return projected_experts(
        mix,
        routes,
        route_weights,
        out_wide,
        out_narrow,
        residual,
        ffn_gain,
        shared_gate,
        shared_up,
        shared_down,
        expert_gate,
        expert_up,
        expert_down,
    )


def solution(mesh):
    placed = (
        P(("grp", "sp"), None),
        P(("grp", "sp"), None),
        P(("grp", "sp"), "tp"),
        P(("grp", "sp"), "tp"),
        P(None, "tp"),
        P(None, "tp"),
        P(None, "tp"),
        P(None, "tp"),
        P(),
        P("tp", None),
        P("tp", None),
        P(("grp", "sp", "tp"), None),
        P(),
        P(None, "tp"),
        P(None, "tp"),
        P("tp", None),
        P(("sp", "tp"), None, None),
        P(("sp", "tp"), None, None),
        P(("sp", "tp"), None, None),
        P(("grp", "sp", "tp"), None),
        P(("grp", "sp", "tp"), None),
    )
    return jax.shard_map(
        body, mesh=mesh, in_specs=placed, out_specs=P(("grp", "sp", "tp"), None), check_vma=False
    )
```

```python
import functools

import jax
import jax.numpy as jnp
import numpy as np
from jax import lax
from jax.experimental import pallas as pl
from jax.experimental.pallas import tpu as pltpu
from jax.sharding import PartitionSpec as P

ROPE = 64
WIDE_HEAD_SIZE = 128
NARROW_HEAD_SIZE = 64
LANES = 128
VMEM_BYTES = 67_043_328


EPS = 1e-06
ROPE_BASE = 10000.0
NEG_FILL = -1e30
LOG2E = 1.4426950408889634


def rms_scale(values, gain):
    return values * lax.rsqrt(jnp.mean(values * values, axis=-1, keepdims=True) + EPS) * gain


def angle_tables(positions):
    half = ROPE // 2
    inverse = ROPE_BASE ** (-np.arange(half) * 2.0 / ROPE)
    angles = positions[:, None] * np.concatenate([inverse, inverse])[None, :]
    pad = ((0, 0), (0, LANES - ROPE))
    return (
        np.pad(np.cos(angles), pad).astype(np.float32),
        np.pad(np.sin(angles), pad).astype(np.float32),
    )


def attention_kernel(
    n_sp,
    n_tp,
    latent_hbm,
    rope_key_hbm,
    wide_query_hbm,
    narrow_query_hbm,
    wide_key_hbm,
    wide_value_hbm,
    narrow_key_hbm,
    narrow_value_hbm,
    gain_hbm,
    local_cos_hbm,
    local_sin_hbm,
    base_cos_hbm,
    base_sin_hbm,
    out_ref,
    latent_ref,
    rope_key_ref,
    wide_query_ref,
    narrow_query_ref,
    wide_key_ref,
    wide_value_ref,
    gain_ref,
    local_cos_ref,
    local_sin_ref,
    base_cos_ref,
    base_sin_ref,
    rows_buf,
    queries,
    narrow_weight,
    top,
    mixed,
    fetch,
    z_send,
    z_recv,
    x_send,
    x_recv,
    d_send,
    d_recv,
    wrap_open,
):
    tokens, width = latent_hbm.shape
    quarter = tokens // n_tp
    zn = n_sp // 2
    steps_up = zn // 2
    steps_down = zn - 1 - steps_up
    me = lax.axis_index("sp")
    x = lax.axis_index("tp")
    z = me // 2
    core = lax.rem(me, 2)
    right = lax.rem(x + 1, n_tp)
    left = lax.rem(x + n_tp - 1, n_tp)
    up = lax.rem(z + 1, zn)
    down = lax.rem(z + zn - 1, zn)
    partner = z * 2 + 1 - core

    fetches = [
        pltpu.make_async_copy(source, target, fetch.at[i])
        for i, (source, target) in enumerate(
            (
                (latent_hbm, latent_ref),
                (rope_key_hbm, rope_key_ref),
                (gain_hbm, gain_ref),
                (local_cos_hbm, local_cos_ref),
                (local_sin_hbm, local_sin_ref),
                (base_cos_hbm, base_cos_ref),
                (base_sin_hbm, base_sin_ref),
                (wide_query_hbm, wide_query_ref),
                (narrow_query_hbm, narrow_query_ref),
                (wide_key_hbm, wide_key_ref),
                (wide_value_hbm, wide_value_ref),
                (narrow_key_hbm, narrow_weight.at[:, pl.ds(0, LANES)]),
                (narrow_value_hbm, narrow_weight.at[:, pl.ds(LANES, LANES)]),
            )
        )
    ]
    for copy in fetches:
        copy.start()

    barrier = pltpu.get_barrier_semaphore()
    for place in ({"sp": down * 2 + core}, {"sp": partner}, {"tp": left}, {"tp": right}):
        pl.semaphore_signal(barrier, inc=1, device_id=place, device_id_type=pl.DeviceIdType.MESH)

    above = {"sp": up * 2 + core}

    @pl.when(z < zn - 1)
    def _():
        pl.semaphore_signal(barrier, inc=1, device_id=above, device_id_type=pl.DeviceIdType.MESH)


    for copy in fetches:
        copy.wait()
    lane = lax.broadcasted_iota(jnp.int32, (tokens, LANES), 1)
    low = lane < ROPE
    lc, ls = local_cos_ref[...], local_sin_ref[...]
    bc, bs = base_cos_ref[pl.ds(me, 1), :], base_sin_ref[pl.ds(me, 1), :]
    cosine = lc * bc - ls * bs
    sine = jnp.where(lane < ROPE // 2, -1.0, 1.0) * (ls * bc + lc * bs)

    def turn(v):
        other = jnp.where(
            lane < ROPE // 2, pltpu.roll(v, LANES - ROPE // 2, 1), pltpu.roll(v, ROPE // 2, 1)
        )
        return (v * cosine + other * sine).astype(jnp.bfloat16)

    lat = latent_ref[...].astype(jnp.float32)
    normed = rms_scale(lat, gain_ref[...]).astype(jnp.bfloat16)
    rope = rope_key_ref[...].astype(jnp.float32).T
    turned = turn(jnp.concatenate([rope, jnp.zeros_like(rope)], axis=1))
    for q in range(n_tp):
        rows_buf[me, q, :, :width] = normed[q * quarter : (q + 1) * quarter]
        rows_buf[me, q, :, width:] = turned[q * quarter : (q + 1) * quarter]

    t1 = wide_query_ref[:, LANES : 2 * LANES].astype(jnp.float32)
    t2 = wide_query_ref[:, 2 * LANES :].astype(jnp.float32)
    n0 = narrow_query_ref[:, :LANES].astype(jnp.float32)
    n1 = narrow_query_ref[:, LANES:].astype(jnp.float32)
    half = LANES // 2
    queries[0, :, :LANES] = wide_query_ref[:, :LANES]
    queries[0, :, LANES:] = turn(t1)
    queries[1, :, :LANES] = pltpu.roll(jnp.where(low, t2, t1), half, 1).astype(jnp.bfloat16)
    queries[1, :, LANES:] = turn(pltpu.roll(t2, half, 1))
    queries[2, :, :LANES] = jnp.where(low, n0, 0.0).astype(jnp.bfloat16)
    queries[2, :, LANES:] = turn(pltpu.roll(n0, half, 1))
    queries[3, :, :LANES] = pltpu.roll(jnp.where(low, n1, 0.0), half, 1).astype(jnp.bfloat16)
    queries[3, :, LANES:] = turn(pltpu.roll(n1, half, 1))
    top[...] = jnp.full(top.shape, NEG_FILL, jnp.float32)
    mixed[...] = jnp.zeros(mixed.shape, jnp.float32)

    @pl.when(z > 0)
    def _():
        pl.semaphore_wait(barrier, 5)

    @pl.when(z == 0)
    def _():
        pl.semaphore_wait(barrier, 4)

    @pl.when(z == zn - 1)
    def _():
        pl.semaphore_signal(wrap_open, inc=1, device_id=above, device_id_type=pl.DeviceIdType.MESH)

    def along_z(d, k, j):
        block = jnp.where(d == 0, z - k + zn, z + k) % zn
        target = jnp.where(d == 0, up, down)
        q = lax.rem(x + j, n_tp)
        spot = rows_buf.at[block * 2 + core, q]
        return pltpu.make_async_remote_copy(
            src_ref=spot,
            dst_ref=spot,
            send_sem=z_send.at[d, k, j],
            recv_sem=z_recv.at[d, k + 1, j],
            device_id={"sp": target * 2 + core},
            device_id_type=pl.DeviceIdType.MESH,
        )

    def along_x(d, k, j):
        block = jnp.where(d == 0, z - k + zn, z + k) % zn
        q = lax.rem(x + j, n_tp)
        spot = rows_buf.at[block * 2 + core, q]
        return pltpu.make_async_remote_copy(
            src_ref=spot,
            dst_ref=spot,
            send_sem=x_send.at[d, k, j],
            recv_sem=x_recv.at[d, k, j],
            device_id={"tp": jnp.where(j == 0, right, left)},
            device_id_type=pl.DeviceIdType.MESH,
        )

    def to_partner(d, k):
        block = jnp.where(d == 0, z - k + zn, z + k) % zn
        spot = rows_buf.at[block * 2 + core]
        return pltpu.make_async_remote_copy(
            src_ref=spot,
            dst_ref=spot,
            send_sem=d_send.at[d, k],
            recv_sem=d_recv.at[d, k],
            device_id={"sp": partner},
            device_id_type=pl.DeviceIdType.MESH,
        )

    def arrives(d, k):
        going_up = (k <= z) & (k <= steps_up)
        going_down = ((z + k) % zn < steps_down) & (k <= steps_down)
        return jnp.where(d == 0, going_up, going_down)

    def goes_on(d, k):
        going_up = (k <= z) & (k < steps_up) & (z + 1 < zn)
        going_down = ((z + k) % zn < steps_down) & (k < steps_down)
        return jnp.where(d == 0, going_up, going_down)

    def seen(d, k):
        going_up = (k <= z) & (k <= steps_up)
        going_down = (z + k >= zn) & (z + k - zn < steps_down) & (k <= steps_down)
        return (k >= 1) & jnp.where(d == 0, going_up, going_down)

    wide_factor = (WIDE_HEAD_SIZE + ROPE) ** (-0.5) * LOG2E
    narrow_factor = (NARROW_HEAD_SIZE + ROPE) ** (-0.5) * LOG2E

    def attend(plane, own):
        rows = rows_buf[pl.ds(plane * 2, 2)].reshape(2 * tokens, width + LANES)
        latents, turned_rows = rows[:, :width], rows[:, width:]
        keys = 2 * tokens
        ones = jnp.ones((keys, LANES), jnp.bfloat16)

        def up_from(weight):
            return jnp.dot(latents, weight[...], preferred_element_type=jnp.float32).astype(jnp.bfloat16)

        wide_k, wide_v, narrow = up_from(wide_key_ref), up_from(wide_value_ref), up_from(narrow_weight)
        narrow_k = jnp.concatenate([narrow[:, :LANES], turned_rows], axis=1)
        narrow_v = jnp.concatenate([narrow[:, LANES:], ones], axis=1)
        if own:
            gap = lax.broadcasted_iota(jnp.int32, (tokens, keys), 1) - lax.broadcasted_iota(
                jnp.int32, (tokens, keys), 0
            )
            visible = gap <= core * tokens
        for h in range(4):
            if h < 2:
                at = slice(h * LANES, (h + 1) * LANES)
                k_h = jnp.concatenate([wide_k[:, at], turned_rows], axis=1)
                v_h = jnp.concatenate([wide_v[:, at], ones], axis=1)
            else:
                k_h, v_h = narrow_k, narrow_v
            scores = lax.dot_general(
                queries[h], k_h, (((1,), (1,)), ((), ())), preferred_element_type=jnp.float32
            ) * (wide_factor if h < 2 else narrow_factor)
            if own:
                scores = jnp.where(visible, scores, NEG_FILL)
            old = top[h]
            new = jnp.maximum(old, jnp.max(scores, axis=1, keepdims=True))
            top[h] = new
            weights = jnp.exp2(scores - jnp.concatenate([new] * (keys // LANES), axis=1)).astype(jnp.bfloat16)
            fading = jnp.exp2(old - new)
            mixed[h] = mixed[h] * jnp.concatenate([fading, fading], axis=1) + jnp.dot(
                weights, v_h, preferred_element_type=jnp.float32
            )

    to_partner(0, 0).start()
    for d in range(2):

        @pl.when(goes_on(d, 0) & ((d == 0) | (z > 0)))
        def _():
            for j in range(2):
                along_z(d, 0, j).start()

    to_partner(0, 0).wait_recv()

    attend(z, True)

    @pl.when(z == 0)
    def _():
        pl.semaphore_wait(wrap_open, 1)
        for j in range(2):
            along_z(1, 0, j).start()

    def one_step(k, carry):
        def quarter_step(j, carry):
            def forward(d, c):
                @pl.when(arrives(d, k))
                def _():
                    along_z(d, k - 1, j).wait_recv()

                @pl.when(goes_on(d, k))
                def _():
                    along_z(d, k, j).start()

                @pl.when(seen(d, k))
                def _():
                    along_x(d, k, j).start()

                return c

            def share(d, c):
                @pl.when(seen(d, k - 1) & (j == 1))
                def _():
                    for side in range(2):
                        along_x(d, k - 1, side).wait_recv()
                    to_partner(d, k - 1).start()

                return c

            lax.fori_loop(0, 2, forward, 0)
            lax.fori_loop(0, 2, share, 0)

            @pl.when(seen(j, k - 3))
            def _():
                to_partner(j, k - 3).wait_recv()
                attend(jnp.where(j == 0, z - k + 3, z + k - 3 - zn), False)

            return carry

        return lax.fori_loop(0, 2, quarter_step, carry)

    lax.fori_loop(1, steps_up + 4, one_step, 0)

    to_partner(0, 0).wait_send()

    def settle(k, carry):
        def both(d, c):
            @pl.when(goes_on(d, k))
            def _():
                for j in range(2):
                    along_z(d, k, j).wait_send()

            @pl.when(seen(d, k))
            def _():
                for j in range(2):
                    along_x(d, k, j).wait_send()
                to_partner(d, k).wait_send()

            return c

        return lax.fori_loop(0, 2, both, carry)

    lax.fori_loop(0, steps_up + 1, settle, 0)

    for h in range(2):
        out_ref[:, h * LANES : (h + 1) * LANES] = (mixed[h, :, :LANES] / mixed[h, :, LANES:]).astype(
            out_ref.dtype
        )
    out_ref[:, 2 * LANES :] = jnp.where(
        low, mixed[2, :, :LANES] / mixed[2, :, LANES:], mixed[3, :, :LANES] / mixed[3, :, LANES:]
    ).astype(out_ref.dtype)


def attention(
    latent, rope_key, wide_query, narrow_query, wide_key, wide_value, narrow_key, narrow_value, gain
):
    tokens, width = latent.shape
    n_sp, n_tp = lax.axis_size("sp"), lax.axis_size("tp")
    zn = n_sp // 2
    assert n_sp % 4 == 0 and n_tp == 4 and wide_query.shape[1] == 3 * LANES
    assert narrow_query.shape[1] == 2 * LANES and zn >= 4
    local_cos, local_sin = angle_tables(np.arange(tokens, dtype=np.float64))
    base_cos, base_sin = angle_tables(np.arange(n_sp, dtype=np.float64) * tokens)
    hops = zn // 2 + 1
    dma = pltpu.SemaphoreType.DMA
    vmem = pl.BlockSpec(memory_space=pltpu.VMEM)
    return pl.pallas_call(
        functools.partial(attention_kernel, n_sp, n_tp),
        out_shape=jax.ShapeDtypeStruct((tokens, 3 * LANES), jnp.bfloat16),
        in_specs=[pl.BlockSpec(memory_space=pltpu.HBM)] * 13,
        out_specs=vmem,
        scratch_shapes=[
            pltpu.VMEM(latent.shape, jnp.bfloat16),
            pltpu.VMEM(rope_key.shape[::-1], jnp.bfloat16),
            pltpu.VMEM(wide_query.shape, jnp.bfloat16),
            pltpu.VMEM(narrow_query.shape, jnp.bfloat16),
            pltpu.VMEM(wide_key.shape, jnp.bfloat16),
            pltpu.VMEM(wide_value.shape, jnp.bfloat16),
            pltpu.VMEM((1, width), jnp.float32),
            pltpu.VMEM(local_cos.shape, jnp.float32),
            pltpu.VMEM(local_sin.shape, jnp.float32),
            pltpu.VMEM(base_cos.shape, jnp.float32),
            pltpu.VMEM(base_sin.shape, jnp.float32),
            pltpu.VMEM((n_sp, n_tp, tokens // n_tp, width + LANES), jnp.bfloat16),
            pltpu.VMEM((4, tokens, 2 * LANES), jnp.bfloat16),
            pltpu.VMEM((width, 2 * LANES), jnp.bfloat16),
            pltpu.VMEM((4, tokens, LANES), jnp.float32),
            pltpu.VMEM((4, tokens, 2 * LANES), jnp.float32),
            dma((13,)),
            dma((2, hops, 2)),
            dma((2, hops + 1, 2)),
            dma((2, hops, 2)),
            dma((2, hops, 2)),
            dma((2, hops)),
            dma((2, hops)),
            pltpu.SemaphoreType.REGULAR,
        ],
        compiler_params=pltpu.CompilerParams(
            collective_id=0, has_side_effects=True, vmem_limit_bytes=VMEM_BYTES
        ),
    )(
        latent,
        rope_key.T,
        wide_query,
        narrow_query,
        wide_key,
        wide_value,
        narrow_key,
        narrow_value,
        gain.reshape(1, width),
        local_cos,
        local_sin,
        base_cos,
        base_sin,
    )


DELTAS = ((0, 8, 7, -7, 4, -4, 1, -1), (6, -6, 5, -5, 3, -3, 2, -2))
COLUMNS = 1024
CAPACITY = 2


def silu(v):
    return v / (1.0 + jnp.exp(-v))


def experts_kernel(
    n_sp,
    n_tp,
    mix_ref,
    routes_hbm,
    weight_hbm,
    out_wide_hbm,
    out_narrow_hbm,
    residual_hbm,
    gain_hbm,
    shared_gate_hbm,
    shared_up_hbm,
    shared_down_hbm,
    expert_gate_hbm,
    expert_up_hbm,
    expert_down_hbm,
    out_ref,
    routes_ref,
    weight_ref,
    places,
    out_weight,
    residual_ref,
    gain_ref,
    shared_in,
    shared_down,
    expert_in,
    expert_down,
    part,
    opposite,
    summed,
    landed,
    stream,
    gathered,
    outgoing,
    first_recv,
    first_relay,
    second_send,
    second_recv,
    finished,
    back_recv,
    back_send,
    back_relay,
    returned,
    shared_send,
    shared_recv,
    fetch,
    send_sems,
    recv_sems,
):
    rows, depth = residual_hbm.shape
    half = depth // 2
    zn = n_sp // 2
    lanes = 2 * n_tp
    piece = outgoing.shape[1]
    wide_rows = out_wide_hbm.shape[0]
    ff = shared_gate_hbm.shape[1]
    hidden = expert_gate_hbm.shape[1]
    top_count = routes_hbm.shape[0]
    me = lax.axis_index("sp")
    x = lax.axis_index("tp")
    z = me // 2
    core = lax.rem(me, 2)
    lane = core * n_tp + x

    def at_plane(delta):
        return lax.rem(z + (delta + zn), zn)

    def on_plane(delta):
        return {"sp": at_plane(delta) * 2 + core}

    def along_x(dx):
        return {"tp": lax.rem(x + (dx + n_tp), n_tp)}

    def in_plane(dc, dx):
        other = 1 - core if dc else core
        return {"sp": z * 2 + other, "tp": lax.rem(x + (dx + n_tp), n_tp)}

    relative = [(dc, dx) for dc in range(2) for dx in range(n_tp)]

    taken = [0]

    def remote(source, target, place):
        i = taken[0]
        taken[0] += 1
        return pltpu.make_async_remote_copy(
            src_ref=source,
            dst_ref=target,
            send_sem=send_sems.at[i],
            recv_sem=recv_sems.at[i],
            device_id=place,
            device_id_type=pl.DeviceIdType.MESH,
        )

    barrier = pltpu.get_barrier_semaphore()
    greeted = [on_plane(d) for d in range(1, zn)] + [in_plane(dc, dx) for dc, dx in relative[1:]]
    for place in greeted:
        pl.semaphore_signal(barrier, inc=1, device_id=place, device_id_type=pl.DeviceIdType.MESH)

    fetches = [
        pltpu.make_async_copy(source, target, fetch.at[i])
        for i, (source, target) in enumerate(
            (
                (routes_hbm, routes_ref),
                (weight_hbm, weight_ref),
                (out_wide_hbm, out_weight.at[pl.ds(0, wide_rows)]),
                (out_narrow_hbm, out_weight.at[pl.ds(wide_rows, out_narrow_hbm.shape[0])]),
                (residual_hbm, residual_ref),
                (gain_hbm, gain_ref),
                (shared_gate_hbm, shared_in.at[:, pl.ds(0, ff)]),
                (shared_up_hbm, shared_in.at[:, pl.ds(ff, ff)]),
                (shared_down_hbm, shared_down),
                (expert_gate_hbm.at[0], expert_in.at[pl.ds(0, hidden)]),
                (expert_up_hbm.at[0], expert_in.at[pl.ds(hidden, hidden)]),
                (expert_down_hbm.at[0], expert_down),
            )
        )
    ]
    for copy in fetches:
        copy.start()

    def normed(values):
        return rms_scale(values.astype(jnp.float32), gain_ref[...]).astype(jnp.bfloat16)

    def chunks():
        return [pl.ds(n, COLUMNS) for n in range(0, depth, COLUMNS)]

    half_cols = (pl.ds(0, half), pl.ds(half, half))
    lower, upper = half_cols
    split = half // 2

    def sides(g):
        return pl.ds(g * half, split), pl.ds(g * half + split, split)

    def project(dx, g):
        q = pl.multiple_of(lax.rem(x + dx, n_tp) * rows, rows)
        mine = mix_ref[pl.ds(q, rows), :]
        for cols in sides(g):
            part[dx, :, cols] = jnp.dot(
                mine, out_weight[:, cols], preferred_element_type=jnp.float32
            ).astype(jnp.bfloat16)

    sent = []

    def begin(source, target, place):
        copy = remote(source, target, place)
        copy.start()
        sent.append(copy)
        return copy

    def to_opposite(g):
        left_side, right_side = sides(g)
        return (
            begin(part.at[2, :, left_side], opposite.at[g, 0], along_x(1)),
            begin(part.at[2, :, right_side], opposite.at[g, 1], along_x(-1)),
        )

    def straight(g):
        left_side, right_side = sides(g)
        return (
            begin(part.at[1, :, right_side], landed.at[g, 0, 1], along_x(1)),
            begin(part.at[3, :, left_side], landed.at[g, 1, 0], along_x(-1)),
        )

    def joined(g, waiting):
        copies = []
        for side, (dx, cols) in enumerate(zip((1, 3), sides(g))):
            waiting[side].wait_recv()
            summed[g, side] = (
                part[dx, :, cols].astype(jnp.float32) + opposite[g, side].astype(jnp.float32)
            ).astype(jnp.bfloat16)
            copies.append(
                begin(summed.at[g, side], landed.at[g, side, side], along_x(1 if side == 0 else -1))
            )
        return tuple(copies)

    def add_up(g, waiting):
        for copy in waiting:
            copy.wait_recv()
        for side, cols in enumerate(sides(g)):
            stream[:, cols] = (
                residual_ref[:, cols].astype(jnp.float32)
                + part[0, :, cols].astype(jnp.float32)
                + landed[g, 0, side].astype(jnp.float32)
                + landed[g, 1, side].astype(jnp.float32)
            ).astype(jnp.bfloat16)
        gathered[0, :, half_cols[g]] = stream[:, half_cols[g]]
        for cols in sides(g):
            outgoing[:, :, cols] = (
                jnp.dot(send_map, gathered[0, :, cols], preferred_element_type=jnp.float32)
                .astype(jnp.bfloat16)
                .reshape(zn, piece, split)
            )

    for copy in fetches[:4]:
        copy.wait()
    project(2, 0)
    pl.semaphore_wait(barrier, len(greeted))
    opposite_copies = [to_opposite(0)]
    project(1, 0)
    project(3, 0)
    straight_copies = [straight(0)]
    project(0, 0)

    r0 = lax.broadcasted_iota(jnp.int32, (rows, rows), 0)
    r1 = lax.broadcasted_iota(jnp.int32, (rows, rows), 1)

    def upright(row):
        return jnp.sum(jnp.where(r0 == r1, row, 0.0), axis=1, keepdims=True)

    named = [routes_ref[c : c + 1, :].astype(jnp.float32) for c in range(top_count)]
    shares = [upright(weight_ref[c : c + 1, :]) for c in range(top_count)]
    slot = lax.broadcasted_iota(jnp.int32, (zn * piece, rows), 0).astype(jnp.float32)
    maps = []
    for c in range(top_count):
        earlier = jnp.zeros((1, rows), jnp.float32)
        for other in range(top_count):
            same = (upright(named[other]) == named[c]) & (r0 < r1)
            earlier = earlier + jnp.sum(jnp.where(same, 1.0, 0.0), axis=0, keepdims=True)
        maps.append(jnp.where(slot == named[c] * CAPACITY + earlier, 1.0, 0.0))
        places[c] = maps[c].T.astype(jnp.bfloat16)
    send_map = sum(maps[1:], maps[0]).astype(jnp.bfloat16)

    project(2, 1)
    joined_copies = [joined(0, opposite_copies[0])]
    opposite_copies.append(to_opposite(1))
    project(1, 1)
    project(3, 1)
    straight_copies.append(straight(1))
    project(0, 1)
    for copy in fetches[4:6]:
        copy.wait()

    far = at_plane(8)
    first = [[], []]
    relays_in = []
    for g, cols in enumerate(half_cols):
        add_up(g, straight_copies[g] + joined_copies[g])
        relays_in.append(begin(outgoing.at[far, :, cols], first_relay.at[g], on_plane(4 if g == 0 else -4)))
        for j, delta in enumerate(DELTAS[0]):
            if delta not in (0, 8):
                first[0].append(
                    begin(outgoing.at[at_plane(delta), :, cols], first_recv.at[0, j, :, cols], on_plane(delta))
                )
        if g == 0:
            joined_copies.append(joined(1, opposite_copies[1]))
    for j, delta in enumerate(DELTAS[1]):
        first[1].append(begin(outgoing.at[at_plane(delta)], first_recv.at[1, j], on_plane(delta)))
    spread = [begin(gathered.at[0], gathered.at[dx], along_x(dx)) for dx in (1, 3, 2)]
    first_recv[0, 0] = outgoing[z]
    far_slot = DELTAS[0].index(8)
    for g, cols in enumerate(half_cols):
        relays_in[g].wait_recv()
        first[0].append(
            begin(first_relay.at[g], first_recv.at[0, far_slot, :, cols], on_plane(4 if g == 0 else -4))
        )

    count = lanes * piece
    o = lax.broadcasted_iota(jnp.int32, (count, count), 0)
    i = lax.broadcasted_iota(jnp.int32, (count, count), 1)
    swap = jnp.where(
        (o // piece == (i % piece) // 2) & ((o % piece) // 2 == i // piece) & (o % 2 == i % 2), 1.0, 0.0
    ).astype(jnp.bfloat16)

    def swapped(source, target, ch):
        for cols in chunks():
            target[ch, :, :, cols] = (
                jnp.dot(
                    swap, source[ch, :, :, cols].reshape(count, COLUMNS), preferred_element_type=jnp.float32
                )
                .astype(jnp.bfloat16)
                .reshape(lanes, piece, COLUMNS)
            )

    def to_lanes(ch):
        swapped(first_recv, second_send, ch)
        copies = []
        for r, (dc, dx) in enumerate(relative):
            if r == 0:
                continue
            other = (1 - core if dc else core) * n_tp + lax.rem(x + dx, n_tp)
            copies.append(remote(second_send.at[ch, other], second_recv.at[ch, r], in_plane(dc, dx)))
            copies[-1].start()
        second_recv[ch, 0] = second_send[ch, lane]
        return copies

    def run_expert(ch):
        taken_in = normed(second_recv[ch].reshape(count, depth))
        gate, lifted = (
            lax.dot_general(
                taken_in,
                expert_in[pl.ds(at, hidden), :],
                (((1,), (1,)), ((), ())),
                preferred_element_type=jnp.float32,
            )
            for at in (0, hidden)
        )
        active = (silu(gate) * lifted).astype(jnp.bfloat16)
        for cols in chunks():
            finished[ch, :, :, cols] = (
                jnp.dot(active, expert_down[:, cols], preferred_element_type=jnp.float32)
                .astype(jnp.bfloat16)
                .reshape(lanes, piece, COLUMNS)
            )
        copies = []
        for r, (dc, dx) in enumerate(relative):
            if r == 0:
                continue
            copies.append(remote(finished.at[ch, r], back_recv.at[ch, lane], in_plane(dc, -dx)))
            copies[-1].start()
        back_recv[ch, lane] = finished[ch, 0]
        return copies

    def home(ch):
        swapped(back_recv, back_send, ch)
        copies = []
        relays = []
        for j, delta in enumerate(DELTAS[ch]):
            if delta == 8:
                relays = [
                    remote(back_send.at[ch, j, :, lower], back_relay.at[0], on_plane(4)),
                    remote(back_send.at[ch, j, :, upper], back_relay.at[1], on_plane(-4)),
                ]
                for copy in relays:
                    copy.start()
        for j, delta in enumerate(DELTAS[ch]):
            if delta == 0:
                returned[z] = back_send[ch, j]
            elif delta != 8:
                copies.append(remote(back_send.at[ch, j], returned.at[z], on_plane(-delta)))
                copies[-1].start()
        return copies, relays

    for copy in first[0]:
        copy.wait_recv()
    lane_copies = to_lanes(0)

    for copy in fetches[6:]:
        copy.wait()
    for copy in spread:
        copy.wait_recv()
    every = normed(gathered[...].reshape(n_tp * rows, depth))
    both = jnp.dot(every, shared_in[...], preferred_element_type=jnp.float32)
    act = (silu(both[:, :ff]) * both[:, ff:]).astype(jnp.bfloat16)
    for cols in chunks():
        shared_send[:, :, cols] = (
            jnp.dot(act, shared_down[:, cols], preferred_element_type=jnp.float32)
            .astype(jnp.bfloat16)
            .reshape(n_tp, rows, COLUMNS)
        )

    for copy in lane_copies:
        copy.wait_recv()
    back_copies = run_expert(0)
    for copy in back_copies:
        copy.wait_recv()
    home_copies, relays = home(0)
    sent += lane_copies + back_copies + home_copies + relays

    for copy in first[1]:
        copy.wait_recv()
    lane_copies = to_lanes(1)
    relays[0].wait_recv()
    last_up = remote(back_relay.at[0], returned.at[at_plane(-4), :, lower], on_plane(4))
    last_up.start()
    relays[1].wait_recv()
    last_down = remote(back_relay.at[1], returned.at[at_plane(4), :, upper], on_plane(-4))
    last_down.start()
    for copy in lane_copies:
        copy.wait_recv()
    back_copies = run_expert(1)
    shared_back = [remote(shared_send.at[dx], shared_recv.at[dx - 1], along_x(-dx)) for dx in range(1, n_tp)]
    for copy in shared_back:
        copy.start()
    sent += shared_back
    for copy in back_copies:
        copy.wait_recv()
    more_home, _ = home(1)
    sent += lane_copies + back_copies + more_home + [last_up, last_down]

    for copy in shared_back:
        copy.wait_recv()
    for copy in home_copies + more_home + [last_up, last_down]:
        copy.wait_recv()
    for cols in chunks():
        total = stream[:, cols].astype(jnp.float32) + shared_send[0, :, cols].astype(jnp.float32)
        for dx in range(n_tp - 1):
            total = total + shared_recv[dx, :, cols].astype(jnp.float32)
        results = returned[:, :, cols].reshape(zn * piece, COLUMNS)
        for c in range(top_count):
            total = total + shares[c] * jnp.dot(places[c], results, preferred_element_type=jnp.float32)
        out_ref[:, cols] = total.astype(out_ref.dtype)
    for copy in sent:
        copy.wait_send()


def projected_experts(
    mix,
    routes,
    route_weights,
    out_wide,
    out_narrow,
    residual,
    gain,
    shared_gate,
    shared_up,
    shared_down,
    expert_gate,
    expert_up,
    expert_down,
):
    rows, depth = residual.shape
    n_sp, n_tp = lax.axis_size("sp"), lax.axis_size("tp")
    zn, lanes = n_sp // 2, 2 * n_tp
    piece = CAPACITY * lanes
    ff = shared_gate.shape[1]
    hidden = expert_gate.shape[2]
    assert zn == 16 and n_tp == 4 and expert_gate.shape[0] == 1
    vmem, hbm = pl.BlockSpec(memory_space=pltpu.VMEM), pl.BlockSpec(memory_space=pltpu.HBM)
    bf16 = jnp.bfloat16
    chunk = (2, lanes, piece, depth)
    dma = pltpu.SemaphoreType.DMA
    return pl.pallas_call(
        functools.partial(experts_kernel, n_sp, n_tp),
        out_shape=jax.ShapeDtypeStruct((rows, depth), bf16),
        in_specs=[vmem] + [hbm] * 12,
        out_specs=vmem,
        scratch_shapes=[
            pltpu.VMEM(routes.shape[::-1], jnp.int32),
            pltpu.VMEM(route_weights.shape[::-1], jnp.float32),
            pltpu.VMEM((routes.shape[1], rows, zn * piece), bf16),
            pltpu.VMEM((out_wide.shape[0] + out_narrow.shape[0], depth), bf16),
            pltpu.VMEM((rows, depth), bf16),
            pltpu.VMEM((1, depth), jnp.float32),
            pltpu.VMEM((depth, 2 * ff), bf16),
            pltpu.VMEM(shared_down.shape, bf16),
            pltpu.VMEM((2 * hidden, depth), bf16),
            pltpu.VMEM(expert_down.shape[1:], bf16),
            pltpu.VMEM((n_tp, rows, depth), bf16),
            pltpu.VMEM((2, 2, rows, depth // 4), bf16),
            pltpu.VMEM((2, 2, rows, depth // 4), bf16),
            pltpu.VMEM((2, 2, 2, rows, depth // 4), bf16),
            pltpu.VMEM((rows, depth), bf16),
            pltpu.VMEM((n_tp, rows, depth), bf16),
            pltpu.VMEM((zn, piece, depth), bf16),
            pltpu.VMEM(chunk, bf16),
            pltpu.VMEM((2, piece, depth // 2), bf16),
            pltpu.VMEM(chunk, bf16),
            pltpu.VMEM(chunk, bf16),
            pltpu.VMEM(chunk, bf16),
            pltpu.VMEM(chunk, bf16),
            pltpu.VMEM(chunk, bf16),
            pltpu.VMEM((2, piece, depth // 2), bf16),
            pltpu.VMEM((zn, piece, depth), bf16),
            pltpu.VMEM((n_tp, rows, depth), bf16),
            pltpu.VMEM((n_tp - 1, rows, depth), bf16),
            dma((12,)),
            dma((104,)),
            dma((104,)),
        ],
        compiler_params=pltpu.CompilerParams(
            collective_id=1, has_side_effects=True, vmem_limit_bytes=VMEM_BYTES
        ),
    )(
        mix,
        routes.T,
        route_weights.T,
        out_wide,
        out_narrow,
        residual,
        gain.reshape(1, depth),
        shared_gate,
        shared_up,
        shared_down,
        jnp.swapaxes(expert_gate, 1, 2),
        jnp.swapaxes(expert_up, 1, 2),
        expert_down,
    )


def body(
    latent,
    rope_key,
    wide_query,
    narrow_query,
    wide_key_weight,
    wide_value_weight,
    narrow_key_weight,
    narrow_value_weight,
    latent_norm_scale,
    out_wide,
    out_narrow,
    residual,
    ffn_gain,
    shared_gate,
    shared_up,
    shared_down,
    expert_gate,
    expert_up,
    expert_down,
    routes,
    route_weights,
):
    mix = attention(
        latent,
        rope_key,
        wide_query,
        narrow_query,
        wide_key_weight,
        wide_value_weight,
        narrow_key_weight,
        narrow_value_weight,
        latent_norm_scale,
    )
    return projected_experts(
        mix,
        routes,
        route_weights,
        out_wide,
        out_narrow,
        residual,
        ffn_gain,
        shared_gate,
        shared_up,
        shared_down,
        expert_gate,
        expert_up,
        expert_down,
    )


def solution(mesh):
    placed = (
        P(("grp", "sp"), None),
        P(("grp", "sp"), None),
        P(("grp", "sp"), "tp"),
        P(("grp", "sp"), "tp"),
        P(None, "tp"),
        P(None, "tp"),
        P(None, "tp"),
        P(None, "tp"),
        P(),
        P("tp", None),
        P("tp", None),
        P(("grp", "sp", "tp"), None),
        P(),
        P(None, "tp"),
        P(None, "tp"),
        P("tp", None),
        P(("sp", "tp"), None, None),
        P(("sp", "tp"), None, None),
        P(("sp", "tp"), None, None),
        P(("grp", "sp", "tp"), None),
        P(("grp", "sp", "tp"), None),
    )
    return jax.shard_map(
        body, mesh=mesh, in_specs=placed, out_specs=P(("grp", "sp", "tp"), None), check_vma=False
    )
```

```python
import functools

import jax
import jax.numpy as jnp
import numpy as np
from jax import lax
from jax.experimental import pallas as pl
from jax.experimental.pallas import tpu as pltpu
from jax.sharding import PartitionSpec as P

ROPE = 64
WIDE_HEAD_SIZE = 128
NARROW_HEAD_SIZE = 64
LANES = 128
VMEM_BYTES = 67_043_328


EPS = 1e-06
ROPE_BASE = 10000.0
NEG_FILL = -1e30
LOG2E = 1.4426950408889634


def rms_scale(values, gain):
    return values * lax.rsqrt(jnp.mean(values * values, axis=-1, keepdims=True) + EPS) * gain


def angle_tables(positions):
    half = ROPE // 2
    inverse = ROPE_BASE ** (-np.arange(half) * 2.0 / ROPE)
    angles = positions[:, None] * np.concatenate([inverse, inverse])[None, :]
    pad = ((0, 0), (0, LANES - ROPE))
    return (
        np.pad(np.cos(angles), pad).astype(np.float32),
        np.pad(np.sin(angles), pad).astype(np.float32),
    )


def attention_kernel(
    n_sp,
    n_tp,
    latent_hbm,
    rope_key_hbm,
    wide_query_hbm,
    narrow_query_hbm,
    wide_key_hbm,
    wide_value_hbm,
    narrow_key_hbm,
    narrow_value_hbm,
    gain_hbm,
    local_cos_hbm,
    local_sin_hbm,
    base_cos_hbm,
    base_sin_hbm,
    out_ref,
    latent_ref,
    rope_key_ref,
    wide_query_ref,
    narrow_query_ref,
    wide_key_ref,
    wide_value_ref,
    gain_ref,
    local_cos_ref,
    local_sin_ref,
    base_cos_ref,
    base_sin_ref,
    rows_buf,
    queries,
    narrow_weight,
    top,
    mixed,
    fetch,
    z_send,
    z_recv,
    x_send,
    x_recv,
    d_send,
    d_recv,
    wrap_open,
):
    tokens, width = latent_hbm.shape
    quarter = tokens // n_tp
    zn = n_sp // 2
    steps_up = zn // 2
    steps_down = zn - 1 - steps_up
    me = lax.axis_index("sp")
    x = lax.axis_index("tp")
    z = me // 2
    core = lax.rem(me, 2)
    right = lax.rem(x + 1, n_tp)
    left = lax.rem(x + n_tp - 1, n_tp)
    up = lax.rem(z + 1, zn)
    down = lax.rem(z + zn - 1, zn)
    partner = z * 2 + 1 - core

    fetches = [
        pltpu.make_async_copy(source, target, fetch.at[i])
        for i, (source, target) in enumerate(
            (
                (latent_hbm, latent_ref),
                (rope_key_hbm, rope_key_ref),
                (gain_hbm, gain_ref),
                (local_cos_hbm, local_cos_ref),
                (local_sin_hbm, local_sin_ref),
                (base_cos_hbm, base_cos_ref),
                (base_sin_hbm, base_sin_ref),
                (wide_query_hbm, wide_query_ref),
                (narrow_query_hbm, narrow_query_ref),
                (wide_key_hbm, wide_key_ref),
                (wide_value_hbm, wide_value_ref),
                (narrow_key_hbm, narrow_weight.at[:, pl.ds(0, LANES)]),
                (narrow_value_hbm, narrow_weight.at[:, pl.ds(LANES, LANES)]),
            )
        )
    ]
    for copy in fetches:
        copy.start()

    barrier = pltpu.get_barrier_semaphore()
    for place in ({"sp": down * 2 + core}, {"sp": partner}, {"tp": left}, {"tp": right}):
        pl.semaphore_signal(barrier, inc=1, device_id=place, device_id_type=pl.DeviceIdType.MESH)

    above = {"sp": up * 2 + core}

    @pl.when(z < zn - 1)
    def _():
        pl.semaphore_signal(barrier, inc=1, device_id=above, device_id_type=pl.DeviceIdType.MESH)


    for copy in fetches:
        copy.wait()
    lane = lax.broadcasted_iota(jnp.int32, (tokens, LANES), 1)
    low = lane < ROPE
    lc, ls = local_cos_ref[...], local_sin_ref[...]
    bc, bs = base_cos_ref[pl.ds(me, 1), :], base_sin_ref[pl.ds(me, 1), :]
    cosine = lc * bc - ls * bs
    sine = jnp.where(lane < ROPE // 2, -1.0, 1.0) * (ls * bc + lc * bs)

    def turn(v):
        other = jnp.where(
            lane < ROPE // 2, pltpu.roll(v, LANES - ROPE // 2, 1), pltpu.roll(v, ROPE // 2, 1)
        )
        return (v * cosine + other * sine).astype(jnp.bfloat16)

    lat = latent_ref[...].astype(jnp.float32)
    normed = rms_scale(lat, gain_ref[...]).astype(jnp.bfloat16)
    rope = rope_key_ref[...].astype(jnp.float32).T
    turned = turn(jnp.concatenate([rope, jnp.zeros_like(rope)], axis=1))
    for q in range(n_tp):
        rows_buf[me, q, :, :width] = normed[q * quarter : (q + 1) * quarter]
        rows_buf[me, q, :, width:] = turned[q * quarter : (q + 1) * quarter]

    t1 = wide_query_ref[:, LANES : 2 * LANES].astype(jnp.float32)
    t2 = wide_query_ref[:, 2 * LANES :].astype(jnp.float32)
    n0 = narrow_query_ref[:, :LANES].astype(jnp.float32)
    n1 = narrow_query_ref[:, LANES:].astype(jnp.float32)
    half = LANES // 2
    queries[0, :, :LANES] = wide_query_ref[:, :LANES]
    queries[0, :, LANES:] = turn(t1)
    queries[1, :, :LANES] = pltpu.roll(jnp.where(low, t2, t1), half, 1).astype(jnp.bfloat16)
    queries[1, :, LANES:] = turn(pltpu.roll(t2, half, 1))
    queries[2, :, :LANES] = jnp.where(low, n0, 0.0).astype(jnp.bfloat16)
    queries[2, :, LANES:] = turn(pltpu.roll(n0, half, 1))
    queries[3, :, :LANES] = pltpu.roll(jnp.where(low, n1, 0.0), half, 1).astype(jnp.bfloat16)
    queries[3, :, LANES:] = turn(pltpu.roll(n1, half, 1))
    top[...] = jnp.full(top.shape, NEG_FILL, jnp.float32)
    mixed[...] = jnp.zeros(mixed.shape, jnp.float32)

    @pl.when(z > 0)
    def _():
        pl.semaphore_wait(barrier, 5)

    @pl.when(z == 0)
    def _():
        pl.semaphore_wait(barrier, 4)

    @pl.when(z == zn - 1)
    def _():
        pl.semaphore_signal(wrap_open, inc=1, device_id=above, device_id_type=pl.DeviceIdType.MESH)

    def along_z(d, k, j):
        block = jnp.where(d == 0, z - k + zn, z + k) % zn
        target = jnp.where(d == 0, up, down)
        q = lax.rem(x + j, n_tp)
        spot = rows_buf.at[block * 2 + core, q]
        return pltpu.make_async_remote_copy(
            src_ref=spot,
            dst_ref=spot,
            send_sem=z_send.at[d, k, j],
            recv_sem=z_recv.at[d, k + 1, j],
            device_id={"sp": target * 2 + core},
            device_id_type=pl.DeviceIdType.MESH,
        )

    def along_x(d, k, j):
        block = jnp.where(d == 0, z - k + zn, z + k) % zn
        q = lax.rem(x + j, n_tp)
        spot = rows_buf.at[block * 2 + core, q]
        return pltpu.make_async_remote_copy(
            src_ref=spot,
            dst_ref=spot,
            send_sem=x_send.at[d, k, j],
            recv_sem=x_recv.at[d, k, j],
            device_id={"tp": jnp.where(j == 0, right, left)},
            device_id_type=pl.DeviceIdType.MESH,
        )

    def to_partner(d, k):
        block = jnp.where(d == 0, z - k + zn, z + k) % zn
        spot = rows_buf.at[block * 2 + core]
        return pltpu.make_async_remote_copy(
            src_ref=spot,
            dst_ref=spot,
            send_sem=d_send.at[d, k],
            recv_sem=d_recv.at[d, k],
            device_id={"sp": partner},
            device_id_type=pl.DeviceIdType.MESH,
        )

    def arrives(d, k):
        going_up = (k <= z) & (k <= steps_up)
        going_down = ((z + k) % zn < steps_down) & (k <= steps_down)
        return jnp.where(d == 0, going_up, going_down)

    def goes_on(d, k):
        going_up = (k <= z) & (k < steps_up) & (z + 1 < zn)
        going_down = ((z + k) % zn < steps_down) & (k < steps_down)
        return jnp.where(d == 0, going_up, going_down)

    def seen(d, k):
        going_up = (k <= z) & (k <= steps_up)
        going_down = (z + k >= zn) & (z + k - zn < steps_down) & (k <= steps_down)
        return (k >= 1) & jnp.where(d == 0, going_up, going_down)

    wide_factor = (WIDE_HEAD_SIZE + ROPE) ** (-0.5) * LOG2E
    narrow_factor = (NARROW_HEAD_SIZE + ROPE) ** (-0.5) * LOG2E

    def attend(plane, own):
        rows = rows_buf[pl.ds(plane * 2, 2)].reshape(2 * tokens, width + LANES)
        latents, turned_rows = rows[:, :width], rows[:, width:]
        keys = 2 * tokens
        ones = jnp.ones((keys, LANES), jnp.bfloat16)

        def up_from(weight):
            return jnp.dot(latents, weight[...], preferred_element_type=jnp.float32).astype(jnp.bfloat16)

        wide_k, wide_v, narrow = up_from(wide_key_ref), up_from(wide_value_ref), up_from(narrow_weight)
        narrow_k = jnp.concatenate([narrow[:, :LANES], turned_rows], axis=1)
        narrow_v = jnp.concatenate([narrow[:, LANES:], ones], axis=1)
        if own:
            gap = lax.broadcasted_iota(jnp.int32, (tokens, keys), 1) - lax.broadcasted_iota(
                jnp.int32, (tokens, keys), 0
            )
            visible = gap <= core * tokens
        for h in range(4):
            if h < 2:
                at = slice(h * LANES, (h + 1) * LANES)
                k_h = jnp.concatenate([wide_k[:, at], turned_rows], axis=1)
                v_h = jnp.concatenate([wide_v[:, at], ones], axis=1)
            else:
                k_h, v_h = narrow_k, narrow_v
            scores = lax.dot_general(
                queries[h], k_h, (((1,), (1,)), ((), ())), preferred_element_type=jnp.float32
            ) * (wide_factor if h < 2 else narrow_factor)
            if own:
                scores = jnp.where(visible, scores, NEG_FILL)
            old = top[h]
            new = jnp.maximum(old, jnp.max(scores, axis=1, keepdims=True))
            top[h] = new
            weights = jnp.exp2(scores - jnp.concatenate([new] * (keys // LANES), axis=1)).astype(jnp.bfloat16)
            fading = jnp.exp2(old - new)
            mixed[h] = mixed[h] * jnp.concatenate([fading, fading], axis=1) + jnp.dot(
                weights, v_h, preferred_element_type=jnp.float32
            )

    to_partner(0, 0).start()
    for d in range(2):

        @pl.when(goes_on(d, 0) & ((d == 0) | (z > 0)))
        def _():
            for j in range(2):
                along_z(d, 0, j).start()

    to_partner(0, 0).wait_recv()

    attend(z, True)

    @pl.when(z == 0)
    def _():
        pl.semaphore_wait(wrap_open, 1)
        for j in range(2):
            along_z(1, 0, j).start()

    def one_step(k, carry):
        def quarter_step(j, carry):
            def forward(d, c):
                @pl.when(arrives(d, k))
                def _():
                    along_z(d, k - 1, j).wait_recv()

                @pl.when(goes_on(d, k))
                def _():
                    along_z(d, k, j).start()

                @pl.when(seen(d, k))
                def _():
                    along_x(d, k, j).start()

                return c

            def share(d, c):
                @pl.when(seen(d, k - 1) & (j == 1))
                def _():
                    for side in range(2):
                        along_x(d, k - 1, side).wait_recv()
                    to_partner(d, k - 1).start()

                return c

            lax.fori_loop(0, 2, forward, 0)
            lax.fori_loop(0, 2, share, 0)

            @pl.when(seen(j, k - 3))
            def _():
                to_partner(j, k - 3).wait_recv()
                attend(jnp.where(j == 0, z - k + 3, z + k - 3 - zn), False)

            return carry

        return lax.fori_loop(0, 2, quarter_step, carry)

    lax.fori_loop(1, steps_up + 4, one_step, 0)

    to_partner(0, 0).wait_send()

    def settle(k, carry):
        def both(d, c):
            @pl.when(goes_on(d, k))
            def _():
                for j in range(2):
                    along_z(d, k, j).wait_send()

            @pl.when(seen(d, k))
            def _():
                for j in range(2):
                    along_x(d, k, j).wait_send()
                to_partner(d, k).wait_send()

            return c

        return lax.fori_loop(0, 2, both, carry)

    lax.fori_loop(0, steps_up + 1, settle, 0)

    for h in range(2):
        out_ref[:, h * LANES : (h + 1) * LANES] = (mixed[h, :, :LANES] / mixed[h, :, LANES:]).astype(
            out_ref.dtype
        )
    out_ref[:, 2 * LANES :] = jnp.where(
        low, mixed[2, :, :LANES] / mixed[2, :, LANES:], mixed[3, :, :LANES] / mixed[3, :, LANES:]
    ).astype(out_ref.dtype)


def attention(
    latent, rope_key, wide_query, narrow_query, wide_key, wide_value, narrow_key, narrow_value, gain
):
    tokens, width = latent.shape
    n_sp, n_tp = lax.axis_size("sp"), lax.axis_size("tp")
    zn = n_sp // 2
    assert n_sp % 4 == 0 and n_tp == 4 and wide_query.shape[1] == 3 * LANES
    assert narrow_query.shape[1] == 2 * LANES and zn >= 4
    local_cos, local_sin = angle_tables(np.arange(tokens, dtype=np.float64))
    base_cos, base_sin = angle_tables(np.arange(n_sp, dtype=np.float64) * tokens)
    hops = zn // 2 + 1
    dma = pltpu.SemaphoreType.DMA
    vmem = pl.BlockSpec(memory_space=pltpu.VMEM)
    return pl.pallas_call(
        functools.partial(attention_kernel, n_sp, n_tp),
        out_shape=jax.ShapeDtypeStruct((tokens, 3 * LANES), jnp.bfloat16),
        in_specs=[pl.BlockSpec(memory_space=pltpu.HBM)] * 13,
        out_specs=vmem,
        scratch_shapes=[
            pltpu.VMEM(latent.shape, jnp.bfloat16),
            pltpu.VMEM(rope_key.shape[::-1], jnp.bfloat16),
            pltpu.VMEM(wide_query.shape, jnp.bfloat16),
            pltpu.VMEM(narrow_query.shape, jnp.bfloat16),
            pltpu.VMEM(wide_key.shape, jnp.bfloat16),
            pltpu.VMEM(wide_value.shape, jnp.bfloat16),
            pltpu.VMEM((1, width), jnp.float32),
            pltpu.VMEM(local_cos.shape, jnp.float32),
            pltpu.VMEM(local_sin.shape, jnp.float32),
            pltpu.VMEM(base_cos.shape, jnp.float32),
            pltpu.VMEM(base_sin.shape, jnp.float32),
            pltpu.VMEM((n_sp, n_tp, tokens // n_tp, width + LANES), jnp.bfloat16),
            pltpu.VMEM((4, tokens, 2 * LANES), jnp.bfloat16),
            pltpu.VMEM((width, 2 * LANES), jnp.bfloat16),
            pltpu.VMEM((4, tokens, LANES), jnp.float32),
            pltpu.VMEM((4, tokens, 2 * LANES), jnp.float32),
            dma((13,)),
            dma((2, hops, 2)),
            dma((2, hops + 1, 2)),
            dma((2, hops, 2)),
            dma((2, hops, 2)),
            dma((2, hops)),
            dma((2, hops)),
            pltpu.SemaphoreType.REGULAR,
        ],
        compiler_params=pltpu.CompilerParams(
            collective_id=0, has_side_effects=True, vmem_limit_bytes=VMEM_BYTES
        ),
    )(
        latent,
        rope_key.T,
        wide_query,
        narrow_query,
        wide_key,
        wide_value,
        narrow_key,
        narrow_value,
        gain.reshape(1, width),
        local_cos,
        local_sin,
        base_cos,
        base_sin,
    )


DELTAS = ((0, 6, -6, 5, -5, 2, -2, 1), (8, 7, -7, 4, -4, 3, -3, -1))
COLUMNS = 1024
CAPACITY = 2


def silu(v):
    return v / (1.0 + jnp.exp(-v))


def experts_kernel(
    n_sp,
    n_tp,
    mix_ref,
    routes_hbm,
    weight_hbm,
    out_wide_hbm,
    out_narrow_hbm,
    residual_hbm,
    gain_hbm,
    shared_gate_hbm,
    shared_up_hbm,
    shared_down_hbm,
    expert_gate_hbm,
    expert_up_hbm,
    expert_down_hbm,
    out_ref,
    routes_ref,
    weight_ref,
    places,
    out_weight,
    residual_ref,
    gain_ref,
    shared_in,
    shared_down,
    expert_in,
    expert_down,
    part,
    opposite,
    summed,
    landed,
    stream,
    gathered,
    outgoing,
    first_recv,
    first_relay,
    second_send,
    second_recv,
    finished,
    back_recv,
    back_send,
    back_relay,
    returned,
    shared_send,
    shared_recv,
    fetch,
    send_sems,
    recv_sems,
):
    rows, depth = residual_hbm.shape
    half = depth // 2
    zn = n_sp // 2
    lanes = 2 * n_tp
    piece = outgoing.shape[1]
    wide_rows = out_wide_hbm.shape[0]
    ff = shared_gate_hbm.shape[1]
    hidden = expert_gate_hbm.shape[1]
    top_count = routes_hbm.shape[0]
    me = lax.axis_index("sp")
    x = lax.axis_index("tp")
    z = me // 2
    core = lax.rem(me, 2)
    lane = core * n_tp + x

    def at_plane(delta):
        return lax.rem(z + (delta + zn), zn)

    def on_plane(delta):
        return {"sp": at_plane(delta) * 2 + core}

    def along_x(dx):
        return {"tp": lax.rem(x + (dx + n_tp), n_tp)}

    def in_plane(dc, dx):
        other = 1 - core if dc else core
        return {"sp": z * 2 + other, "tp": lax.rem(x + (dx + n_tp), n_tp)}

    relative = [(dc, dx) for dc in range(2) for dx in range(n_tp)]

    taken = [0]

    def remote(source, target, place):
        i = taken[0]
        taken[0] += 1
        return pltpu.make_async_remote_copy(
            src_ref=source,
            dst_ref=target,
            send_sem=send_sems.at[i],
            recv_sem=recv_sems.at[i],
            device_id=place,
            device_id_type=pl.DeviceIdType.MESH,
        )

    barrier = pltpu.get_barrier_semaphore()
    greeted = [on_plane(d) for d in range(1, zn)] + [in_plane(dc, dx) for dc, dx in relative[1:]]
    for place in greeted:
        pl.semaphore_signal(barrier, inc=1, device_id=place, device_id_type=pl.DeviceIdType.MESH)

    fetches = [
        pltpu.make_async_copy(source, target, fetch.at[i])
        for i, (source, target) in enumerate(
            (
                (routes_hbm, routes_ref),
                (weight_hbm, weight_ref),
                (out_wide_hbm, out_weight.at[pl.ds(0, wide_rows)]),
                (out_narrow_hbm, out_weight.at[pl.ds(wide_rows, out_narrow_hbm.shape[0])]),
                (residual_hbm, residual_ref),
                (gain_hbm, gain_ref),
                (shared_gate_hbm, shared_in.at[:, pl.ds(0, ff)]),
                (shared_up_hbm, shared_in.at[:, pl.ds(ff, ff)]),
                (shared_down_hbm, shared_down),
                (expert_gate_hbm.at[0], expert_in.at[pl.ds(0, hidden)]),
                (expert_up_hbm.at[0], expert_in.at[pl.ds(hidden, hidden)]),
                (expert_down_hbm.at[0], expert_down),
            )
        )
    ]
    for copy in fetches:
        copy.start()

    def normed(values):
        return rms_scale(values.astype(jnp.float32), gain_ref[...]).astype(jnp.bfloat16)

    def chunks():
        return [pl.ds(n, COLUMNS) for n in range(0, depth, COLUMNS)]

    half_cols = (pl.ds(0, half), pl.ds(half, half))
    lower, upper = half_cols
    split = half // 2

    def sides(g):
        return pl.ds(g * half, split), pl.ds(g * half + split, split)

    def project(dx, g):
        q = pl.multiple_of(lax.rem(x + dx, n_tp) * rows, rows)
        mine = mix_ref[pl.ds(q, rows), :]
        for cols in sides(g):
            part[dx, :, cols] = jnp.dot(
                mine, out_weight[:, cols], preferred_element_type=jnp.float32
            ).astype(jnp.bfloat16)

    sent = []

    def begin(source, target, place):
        copy = remote(source, target, place)
        copy.start()
        sent.append(copy)
        return copy

    def to_opposite(g):
        left_side, right_side = sides(g)
        return (
            begin(part.at[2, :, left_side], opposite.at[g, 0], along_x(1)),
            begin(part.at[2, :, right_side], opposite.at[g, 1], along_x(-1)),
        )

    def straight(g):
        left_side, right_side = sides(g)
        return (
            begin(part.at[1, :, right_side], landed.at[g, 0, 1], along_x(1)),
            begin(part.at[3, :, left_side], landed.at[g, 1, 0], along_x(-1)),
        )

    def joined(g, waiting):
        copies = []
        for side, (dx, cols) in enumerate(zip((1, 3), sides(g))):
            waiting[side].wait_recv()
            summed[g, side] = (
                part[dx, :, cols].astype(jnp.float32) + opposite[g, side].astype(jnp.float32)
            ).astype(jnp.bfloat16)
            copies.append(
                begin(summed.at[g, side], landed.at[g, side, side], along_x(1 if side == 0 else -1))
            )
        return tuple(copies)

    def add_up(g, waiting):
        for copy in waiting:
            copy.wait_recv()
        for side, cols in enumerate(sides(g)):
            stream[:, cols] = (
                residual_ref[:, cols].astype(jnp.float32)
                + part[0, :, cols].astype(jnp.float32)
                + landed[g, 0, side].astype(jnp.float32)
                + landed[g, 1, side].astype(jnp.float32)
            ).astype(jnp.bfloat16)
        gathered[0, :, half_cols[g]] = stream[:, half_cols[g]]
        for cols in sides(g):
            outgoing[:, :, cols] = (
                jnp.dot(send_map, gathered[0, :, cols], preferred_element_type=jnp.float32)
                .astype(jnp.bfloat16)
                .reshape(zn, piece, split)
            )

    for copy in fetches[:4]:
        copy.wait()
    project(2, 0)
    pl.semaphore_wait(barrier, len(greeted))
    opposite_copies = [to_opposite(0)]
    project(1, 0)
    project(3, 0)
    straight_copies = [straight(0)]
    project(0, 0)

    r0 = lax.broadcasted_iota(jnp.int32, (rows, rows), 0)
    r1 = lax.broadcasted_iota(jnp.int32, (rows, rows), 1)

    def upright(row):
        return jnp.sum(jnp.where(r0 == r1, row, 0.0), axis=1, keepdims=True)

    named = [routes_ref[c : c + 1, :].astype(jnp.float32) for c in range(top_count)]
    shares = [upright(weight_ref[c : c + 1, :]) for c in range(top_count)]
    slot = lax.broadcasted_iota(jnp.int32, (zn * piece, rows), 0).astype(jnp.float32)
    maps = []
    for c in range(top_count):
        earlier = jnp.zeros((1, rows), jnp.float32)
        for other in range(top_count):
            same = (upright(named[other]) == named[c]) & (r0 < r1)
            earlier = earlier + jnp.sum(jnp.where(same, 1.0, 0.0), axis=0, keepdims=True)
        maps.append(jnp.where(slot == named[c] * CAPACITY + earlier, 1.0, 0.0))
        places[c] = maps[c].T.astype(jnp.bfloat16)
    send_map = sum(maps[1:], maps[0]).astype(jnp.bfloat16)

    project(2, 1)
    joined_copies = [joined(0, opposite_copies[0])]
    opposite_copies.append(to_opposite(1))
    project(1, 1)
    project(3, 1)
    straight_copies.append(straight(1))
    project(0, 1)
    for copy in fetches[4:6]:
        copy.wait()

    far = at_plane(8)
    first = [[], []]
    relays_in = []
    for g, cols in enumerate(half_cols):
        add_up(g, straight_copies[g] + joined_copies[g])
        relays_in.append(begin(outgoing.at[far, :, cols], first_relay.at[g], on_plane(4 if g == 0 else -4)))
        for j, delta in enumerate(DELTAS[0]):
            if delta not in (0, 8):
                first[0].append(
                    begin(outgoing.at[at_plane(delta), :, cols], first_recv.at[0, j, :, cols], on_plane(delta))
                )
        if g == 0:
            joined_copies.append(joined(1, opposite_copies[1]))
    spread = [begin(gathered.at[0], gathered.at[dx], along_x(dx)) for dx in (1, 3, 2)]
    first_recv[0, 0] = outgoing[z]
    far_slot = DELTAS[1].index(8)
    for g, cols in enumerate(half_cols):
        relays_in[g].wait_recv()
        first[1].append(
            begin(first_relay.at[g], first_recv.at[1, far_slot, :, cols], on_plane(4 if g == 0 else -4))
        )
    for j, delta in enumerate(DELTAS[1]):
        if delta != 8:
            first[1].append(begin(outgoing.at[at_plane(delta)], first_recv.at[1, j], on_plane(delta)))

    count = lanes * piece
    o = lax.broadcasted_iota(jnp.int32, (count, count), 0)
    i = lax.broadcasted_iota(jnp.int32, (count, count), 1)
    swap = jnp.where(
        (o // piece == (i % piece) // 2) & ((o % piece) // 2 == i // piece) & (o % 2 == i % 2), 1.0, 0.0
    ).astype(jnp.bfloat16)

    def swapped(source, target, ch):
        for cols in chunks():
            target[ch, :, :, cols] = (
                jnp.dot(
                    swap, source[ch, :, :, cols].reshape(count, COLUMNS), preferred_element_type=jnp.float32
                )
                .astype(jnp.bfloat16)
                .reshape(lanes, piece, COLUMNS)
            )

    def to_lanes(ch):
        swapped(first_recv, second_send, ch)
        copies = []
        for r, (dc, dx) in enumerate(relative):
            if r == 0:
                continue
            other = (1 - core if dc else core) * n_tp + lax.rem(x + dx, n_tp)
            copies.append(remote(second_send.at[ch, other], second_recv.at[ch, r], in_plane(dc, dx)))
            copies[-1].start()
        second_recv[ch, 0] = second_send[ch, lane]
        return copies

    def run_expert(ch):
        taken_in = normed(second_recv[ch].reshape(count, depth))
        gate, lifted = (
            lax.dot_general(
                taken_in,
                expert_in[pl.ds(at, hidden), :],
                (((1,), (1,)), ((), ())),
                preferred_element_type=jnp.float32,
            )
            for at in (0, hidden)
        )
        active = (silu(gate) * lifted).astype(jnp.bfloat16)
        for cols in chunks():
            finished[ch, :, :, cols] = (
                jnp.dot(active, expert_down[:, cols], preferred_element_type=jnp.float32)
                .astype(jnp.bfloat16)
                .reshape(lanes, piece, COLUMNS)
            )
        copies = []
        for r, (dc, dx) in enumerate(relative):
            if r == 0:
                continue
            copies.append(remote(finished.at[ch, r], back_recv.at[ch, lane], in_plane(dc, -dx)))
            copies[-1].start()
        back_recv[ch, lane] = finished[ch, 0]
        return copies

    def home(ch):
        swapped(back_recv, back_send, ch)
        copies = []
        relays = []
        for j, delta in enumerate(DELTAS[ch]):
            if delta == 8:
                relays = [
                    remote(back_send.at[ch, j, :, lower], back_relay.at[0], on_plane(4)),
                    remote(back_send.at[ch, j, :, upper], back_relay.at[1], on_plane(-4)),
                ]
                for copy in relays:
                    copy.start()
        for j, delta in enumerate(DELTAS[ch]):
            if delta == 0:
                returned[z] = back_send[ch, j]
            elif delta != 8:
                copies.append(remote(back_send.at[ch, j], returned.at[z], on_plane(-delta)))
                copies[-1].start()
        return copies, relays

    for copy in first[0]:
        copy.wait_recv()
    lane_copies = to_lanes(0)

    for copy in fetches[6:]:
        copy.wait()
    for copy in spread:
        copy.wait_recv()
    every = normed(gathered[...].reshape(n_tp * rows, depth))
    both = jnp.dot(every, shared_in[...], preferred_element_type=jnp.float32)
    act = (silu(both[:, :ff]) * both[:, ff:]).astype(jnp.bfloat16)
    for cols in chunks():
        shared_send[:, :, cols] = (
            jnp.dot(act, shared_down[:, cols], preferred_element_type=jnp.float32)
            .astype(jnp.bfloat16)
            .reshape(n_tp, rows, COLUMNS)
        )

    for copy in lane_copies:
        copy.wait_recv()
    back_copies = run_expert(0)
    for copy in back_copies:
        copy.wait_recv()
    home_copies, _ = home(0)
    sent += lane_copies + back_copies + home_copies

    for copy in first[1]:
        copy.wait_recv()
    lane_copies = to_lanes(1)
    for copy in lane_copies:
        copy.wait_recv()
    back_copies = run_expert(1)
    shared_back = [remote(shared_send.at[dx], shared_recv.at[dx - 1], along_x(-dx)) for dx in range(1, n_tp)]
    for copy in shared_back:
        copy.start()
    sent += shared_back
    for copy in back_copies:
        copy.wait_recv()
    more_home, relays = home(1)
    relays[0].wait_recv()
    last_up = remote(back_relay.at[0], returned.at[at_plane(-4), :, lower], on_plane(4))
    last_up.start()
    relays[1].wait_recv()
    last_down = remote(back_relay.at[1], returned.at[at_plane(4), :, upper], on_plane(-4))
    last_down.start()
    sent += lane_copies + back_copies + more_home + relays + [last_up, last_down]

    for copy in shared_back:
        copy.wait_recv()
    for copy in home_copies + more_home + [last_up, last_down]:
        copy.wait_recv()
    for cols in chunks():
        total = stream[:, cols].astype(jnp.float32) + shared_send[0, :, cols].astype(jnp.float32)
        for dx in range(n_tp - 1):
            total = total + shared_recv[dx, :, cols].astype(jnp.float32)
        results = returned[:, :, cols].reshape(zn * piece, COLUMNS)
        for c in range(top_count):
            total = total + shares[c] * jnp.dot(places[c], results, preferred_element_type=jnp.float32)
        out_ref[:, cols] = total.astype(out_ref.dtype)
    for copy in sent:
        copy.wait_send()


def projected_experts(
    mix,
    routes,
    route_weights,
    out_wide,
    out_narrow,
    residual,
    gain,
    shared_gate,
    shared_up,
    shared_down,
    expert_gate,
    expert_up,
    expert_down,
):
    rows, depth = residual.shape
    n_sp, n_tp = lax.axis_size("sp"), lax.axis_size("tp")
    zn, lanes = n_sp // 2, 2 * n_tp
    piece = CAPACITY * lanes
    ff = shared_gate.shape[1]
    hidden = expert_gate.shape[2]
    assert zn == 16 and n_tp == 4 and expert_gate.shape[0] == 1
    vmem, hbm = pl.BlockSpec(memory_space=pltpu.VMEM), pl.BlockSpec(memory_space=pltpu.HBM)
    bf16 = jnp.bfloat16
    chunk = (2, lanes, piece, depth)
    dma = pltpu.SemaphoreType.DMA
    return pl.pallas_call(
        functools.partial(experts_kernel, n_sp, n_tp),
        out_shape=jax.ShapeDtypeStruct((rows, depth), bf16),
        in_specs=[vmem] + [hbm] * 12,
        out_specs=vmem,
        scratch_shapes=[
            pltpu.VMEM(routes.shape[::-1], jnp.int32),
            pltpu.VMEM(route_weights.shape[::-1], jnp.float32),
            pltpu.VMEM((routes.shape[1], rows, zn * piece), bf16),
            pltpu.VMEM((out_wide.shape[0] + out_narrow.shape[0], depth), bf16),
            pltpu.VMEM((rows, depth), bf16),
            pltpu.VMEM((1, depth), jnp.float32),
            pltpu.VMEM((depth, 2 * ff), bf16),
            pltpu.VMEM(shared_down.shape, bf16),
            pltpu.VMEM((2 * hidden, depth), bf16),
            pltpu.VMEM(expert_down.shape[1:], bf16),
            pltpu.VMEM((n_tp, rows, depth), bf16),
            pltpu.VMEM((2, 2, rows, depth // 4), bf16),
            pltpu.VMEM((2, 2, rows, depth // 4), bf16),
            pltpu.VMEM((2, 2, 2, rows, depth // 4), bf16),
            pltpu.VMEM((rows, depth), bf16),
            pltpu.VMEM((n_tp, rows, depth), bf16),
            pltpu.VMEM((zn, piece, depth), bf16),
            pltpu.VMEM(chunk, bf16),
            pltpu.VMEM((2, piece, depth // 2), bf16),
            pltpu.VMEM(chunk, bf16),
            pltpu.VMEM(chunk, bf16),
            pltpu.VMEM(chunk, bf16),
            pltpu.VMEM(chunk, bf16),
            pltpu.VMEM(chunk, bf16),
            pltpu.VMEM((2, piece, depth // 2), bf16),
            pltpu.VMEM((zn, piece, depth), bf16),
            pltpu.VMEM((n_tp, rows, depth), bf16),
            pltpu.VMEM((n_tp - 1, rows, depth), bf16),
            dma((12,)),
            dma((104,)),
            dma((104,)),
        ],
        compiler_params=pltpu.CompilerParams(
            collective_id=1, has_side_effects=True, vmem_limit_bytes=VMEM_BYTES
        ),
    )(
        mix,
        routes.T,
        route_weights.T,
        out_wide,
        out_narrow,
        residual,
        gain.reshape(1, depth),
        shared_gate,
        shared_up,
        shared_down,
        jnp.swapaxes(expert_gate, 1, 2),
        jnp.swapaxes(expert_up, 1, 2),
        expert_down,
    )


def body(
    latent,
    rope_key,
    wide_query,
    narrow_query,
    wide_key_weight,
    wide_value_weight,
    narrow_key_weight,
    narrow_value_weight,
    latent_norm_scale,
    out_wide,
    out_narrow,
    residual,
    ffn_gain,
    shared_gate,
    shared_up,
    shared_down,
    expert_gate,
    expert_up,
    expert_down,
    routes,
    route_weights,
):
    mix = attention(
        latent,
        rope_key,
        wide_query,
        narrow_query,
        wide_key_weight,
        wide_value_weight,
        narrow_key_weight,
        narrow_value_weight,
        latent_norm_scale,
    )
    return projected_experts(
        mix,
        routes,
        route_weights,
        out_wide,
        out_narrow,
        residual,
        ffn_gain,
        shared_gate,
        shared_up,
        shared_down,
        expert_gate,
        expert_up,
        expert_down,
    )


def solution(mesh):
    placed = (
        P(("grp", "sp"), None),
        P(("grp", "sp"), None),
        P(("grp", "sp"), "tp"),
        P(("grp", "sp"), "tp"),
        P(None, "tp"),
        P(None, "tp"),
        P(None, "tp"),
        P(None, "tp"),
        P(),
        P("tp", None),
        P("tp", None),
        P(("grp", "sp", "tp"), None),
        P(),
        P(None, "tp"),
        P(None, "tp"),
        P("tp", None),
        P(("sp", "tp"), None, None),
        P(("sp", "tp"), None, None),
        P(("sp", "tp"), None, None),
        P(("grp", "sp", "tp"), None),
        P(("grp", "sp", "tp"), None),
    )
    return jax.shard_map(
        body, mesh=mesh, in_specs=placed, out_specs=P(("grp", "sp", "tp"), None), check_vma=False
    )
```

```python
import functools

import jax
import jax.numpy as jnp
import numpy as np
from jax import lax
from jax.experimental import pallas as pl
from jax.experimental.pallas import tpu as pltpu
from jax.sharding import PartitionSpec as P

ROPE = 64
WIDE_HEAD_SIZE = 128
NARROW_HEAD_SIZE = 64
LANES = 128
VMEM_BYTES = 67_043_328


EPS = 1e-06
ROPE_BASE = 10000.0
NEG_FILL = -1e30
LOG2E = 1.4426950408889634


def rms_scale(values, gain):
    return values * lax.rsqrt(jnp.mean(values * values, axis=-1, keepdims=True) + EPS) * gain


def angle_tables(positions):
    half = ROPE // 2
    inverse = ROPE_BASE ** (-np.arange(half) * 2.0 / ROPE)
    angles = positions[:, None] * np.concatenate([inverse, inverse])[None, :]
    pad = ((0, 0), (0, LANES - ROPE))
    return (
        np.pad(np.cos(angles), pad).astype(np.float32),
        np.pad(np.sin(angles), pad).astype(np.float32),
    )


def attention_kernel(
    n_sp,
    n_tp,
    latent_hbm,
    rope_key_hbm,
    wide_query_hbm,
    narrow_query_hbm,
    wide_key_hbm,
    wide_value_hbm,
    narrow_key_hbm,
    narrow_value_hbm,
    gain_hbm,
    local_cos_hbm,
    local_sin_hbm,
    base_cos_hbm,
    base_sin_hbm,
    out_ref,
    latent_ref,
    rope_key_ref,
    wide_query_ref,
    narrow_query_ref,
    wide_key_ref,
    wide_value_ref,
    gain_ref,
    local_cos_ref,
    local_sin_ref,
    base_cos_ref,
    base_sin_ref,
    rows_buf,
    queries,
    narrow_weight,
    top,
    mixed,
    fetch,
    z_send,
    z_recv,
    x_send,
    x_recv,
    d_send,
    d_recv,
    wrap_open,
):
    tokens, width = latent_hbm.shape
    quarter = tokens // n_tp
    zn = n_sp // 2
    steps_up = zn // 2
    steps_down = zn - 1 - steps_up
    me = lax.axis_index("sp")
    x = lax.axis_index("tp")
    z = me // 2
    core = lax.rem(me, 2)
    right = lax.rem(x + 1, n_tp)
    left = lax.rem(x + n_tp - 1, n_tp)
    up = lax.rem(z + 1, zn)
    down = lax.rem(z + zn - 1, zn)
    partner = z * 2 + 1 - core

    fetches = [
        pltpu.make_async_copy(source, target, fetch.at[i])
        for i, (source, target) in enumerate(
            (
                (latent_hbm, latent_ref),
                (rope_key_hbm, rope_key_ref),
                (gain_hbm, gain_ref),
                (local_cos_hbm, local_cos_ref),
                (local_sin_hbm, local_sin_ref),
                (base_cos_hbm, base_cos_ref),
                (base_sin_hbm, base_sin_ref),
                (wide_query_hbm, wide_query_ref),
                (narrow_query_hbm, narrow_query_ref),
                (wide_key_hbm, wide_key_ref),
                (wide_value_hbm, wide_value_ref),
                (narrow_key_hbm, narrow_weight.at[:, pl.ds(0, LANES)]),
                (narrow_value_hbm, narrow_weight.at[:, pl.ds(LANES, LANES)]),
            )
        )
    ]
    for copy in fetches:
        copy.start()

    barrier = pltpu.get_barrier_semaphore()
    for place in ({"sp": down * 2 + core}, {"sp": partner}, {"tp": left}, {"tp": right}):
        pl.semaphore_signal(barrier, inc=1, device_id=place, device_id_type=pl.DeviceIdType.MESH)

    above = {"sp": up * 2 + core}

    @pl.when(z < zn - 1)
    def _():
        pl.semaphore_signal(barrier, inc=1, device_id=above, device_id_type=pl.DeviceIdType.MESH)


    for copy in fetches:
        copy.wait()
    lane = lax.broadcasted_iota(jnp.int32, (tokens, LANES), 1)
    low = lane < ROPE
    lc, ls = local_cos_ref[...], local_sin_ref[...]
    bc, bs = base_cos_ref[pl.ds(me, 1), :], base_sin_ref[pl.ds(me, 1), :]
    cosine = lc * bc - ls * bs
    sine = jnp.where(lane < ROPE // 2, -1.0, 1.0) * (ls * bc + lc * bs)

    def turn(v):
        other = jnp.where(
            lane < ROPE // 2, pltpu.roll(v, LANES - ROPE // 2, 1), pltpu.roll(v, ROPE // 2, 1)
        )
        return (v * cosine + other * sine).astype(jnp.bfloat16)

    lat = latent_ref[...].astype(jnp.float32)
    normed = rms_scale(lat, gain_ref[...]).astype(jnp.bfloat16)
    rope = rope_key_ref[...].astype(jnp.float32).T
    turned = turn(jnp.concatenate([rope, jnp.zeros_like(rope)], axis=1))
    for q in range(n_tp):
        rows_buf[me, q, :, :width] = normed[q * quarter : (q + 1) * quarter]
        rows_buf[me, q, :, width:] = turned[q * quarter : (q + 1) * quarter]

    t1 = wide_query_ref[:, LANES : 2 * LANES].astype(jnp.float32)
    t2 = wide_query_ref[:, 2 * LANES :].astype(jnp.float32)
    n0 = narrow_query_ref[:, :LANES].astype(jnp.float32)
    n1 = narrow_query_ref[:, LANES:].astype(jnp.float32)
    half = LANES // 2
    queries[0, :, :LANES] = wide_query_ref[:, :LANES]
    queries[0, :, LANES:] = turn(t1)
    queries[1, :, :LANES] = pltpu.roll(jnp.where(low, t2, t1), half, 1).astype(jnp.bfloat16)
    queries[1, :, LANES:] = turn(pltpu.roll(t2, half, 1))
    queries[2, :, :LANES] = jnp.where(low, n0, 0.0).astype(jnp.bfloat16)
    queries[2, :, LANES:] = turn(pltpu.roll(n0, half, 1))
    queries[3, :, :LANES] = pltpu.roll(jnp.where(low, n1, 0.0), half, 1).astype(jnp.bfloat16)
    queries[3, :, LANES:] = turn(pltpu.roll(n1, half, 1))
    top[...] = jnp.full(top.shape, NEG_FILL, jnp.float32)
    mixed[...] = jnp.zeros(mixed.shape, jnp.float32)

    @pl.when(z > 0)
    def _():
        pl.semaphore_wait(barrier, 5)

    @pl.when(z == 0)
    def _():
        pl.semaphore_wait(barrier, 4)

    @pl.when(z == zn - 1)
    def _():
        pl.semaphore_signal(wrap_open, inc=1, device_id=above, device_id_type=pl.DeviceIdType.MESH)

    def along_z(d, k, j):
        block = jnp.where(d == 0, z - k + zn, z + k) % zn
        target = jnp.where(d == 0, up, down)
        q = lax.rem(x + j, n_tp)
        spot = rows_buf.at[block * 2 + core, q]
        return pltpu.make_async_remote_copy(
            src_ref=spot,
            dst_ref=spot,
            send_sem=z_send.at[d, k, j],
            recv_sem=z_recv.at[d, k + 1, j],
            device_id={"sp": target * 2 + core},
            device_id_type=pl.DeviceIdType.MESH,
        )

    def along_x(d, k, j):
        block = jnp.where(d == 0, z - k + zn, z + k) % zn
        q = lax.rem(x + j, n_tp)
        spot = rows_buf.at[block * 2 + core, q]
        return pltpu.make_async_remote_copy(
            src_ref=spot,
            dst_ref=spot,
            send_sem=x_send.at[d, k, j],
            recv_sem=x_recv.at[d, k, j],
            device_id={"tp": jnp.where(j == 0, right, left)},
            device_id_type=pl.DeviceIdType.MESH,
        )

    def to_partner(d, k):
        block = jnp.where(d == 0, z - k + zn, z + k) % zn
        spot = rows_buf.at[block * 2 + core]
        return pltpu.make_async_remote_copy(
            src_ref=spot,
            dst_ref=spot,
            send_sem=d_send.at[d, k],
            recv_sem=d_recv.at[d, k],
            device_id={"sp": partner},
            device_id_type=pl.DeviceIdType.MESH,
        )

    def arrives(d, k):
        going_up = (k <= z) & (k <= steps_up)
        going_down = ((z + k) % zn < steps_down) & (k <= steps_down)
        return jnp.where(d == 0, going_up, going_down)

    def goes_on(d, k):
        going_up = (k <= z) & (k < steps_up) & (z + 1 < zn)
        going_down = ((z + k) % zn < steps_down) & (k < steps_down)
        return jnp.where(d == 0, going_up, going_down)

    def seen(d, k):
        going_up = (k <= z) & (k <= steps_up)
        going_down = (z + k >= zn) & (z + k - zn < steps_down) & (k <= steps_down)
        return (k >= 1) & jnp.where(d == 0, going_up, going_down)

    wide_factor = (WIDE_HEAD_SIZE + ROPE) ** (-0.5) * LOG2E
    narrow_factor = (NARROW_HEAD_SIZE + ROPE) ** (-0.5) * LOG2E

    def attend(plane, own):
        rows = rows_buf[pl.ds(plane * 2, 2)].reshape(2 * tokens, width + LANES)
        latents, turned_rows = rows[:, :width], rows[:, width:]
        keys = 2 * tokens
        ones = jnp.ones((keys, LANES), jnp.bfloat16)

        def up_from(weight):
            return jnp.dot(latents, weight[...], preferred_element_type=jnp.float32).astype(jnp.bfloat16)

        wide_k, wide_v, narrow = up_from(wide_key_ref), up_from(wide_value_ref), up_from(narrow_weight)
        narrow_k = jnp.concatenate([narrow[:, :LANES], turned_rows], axis=1)
        narrow_v = jnp.concatenate([narrow[:, LANES:], ones], axis=1)
        if own:
            gap = lax.broadcasted_iota(jnp.int32, (tokens, keys), 1) - lax.broadcasted_iota(
                jnp.int32, (tokens, keys), 0
            )
            visible = gap <= core * tokens
        for h in range(4):
            if h < 2:
                at = slice(h * LANES, (h + 1) * LANES)
                k_h = jnp.concatenate([wide_k[:, at], turned_rows], axis=1)
                v_h = jnp.concatenate([wide_v[:, at], ones], axis=1)
            else:
                k_h, v_h = narrow_k, narrow_v
            scores = lax.dot_general(
                queries[h], k_h, (((1,), (1,)), ((), ())), preferred_element_type=jnp.float32
            ) * (wide_factor if h < 2 else narrow_factor)
            if own:
                scores = jnp.where(visible, scores, NEG_FILL)
            old = top[h]
            new = jnp.maximum(old, jnp.max(scores, axis=1, keepdims=True))
            top[h] = new
            weights = jnp.exp2(scores - jnp.concatenate([new] * (keys // LANES), axis=1)).astype(jnp.bfloat16)
            fading = jnp.exp2(old - new)
            mixed[h] = mixed[h] * jnp.concatenate([fading, fading], axis=1) + jnp.dot(
                weights, v_h, preferred_element_type=jnp.float32
            )

    to_partner(0, 0).start()
    for d in range(2):

        @pl.when(goes_on(d, 0) & ((d == 0) | (z > 0)))
        def _():
            for j in range(2):
                along_z(d, 0, j).start()

    to_partner(0, 0).wait_recv()

    attend(z, True)

    @pl.when(z == 0)
    def _():
        pl.semaphore_wait(wrap_open, 1)
        for j in range(2):
            along_z(1, 0, j).start()

    def one_step(k, carry):
        def quarter_step(j, carry):
            def forward(d, c):
                @pl.when(arrives(d, k))
                def _():
                    along_z(d, k - 1, j).wait_recv()

                @pl.when(goes_on(d, k))
                def _():
                    along_z(d, k, j).start()

                @pl.when(seen(d, k))
                def _():
                    along_x(d, k, j).start()

                return c

            def share(d, c):
                @pl.when(seen(d, k - 1) & (j == 1))
                def _():
                    for side in range(2):
                        along_x(d, k - 1, side).wait_recv()
                    to_partner(d, k - 1).start()

                return c

            lax.fori_loop(0, 2, forward, 0)
            lax.fori_loop(0, 2, share, 0)

            @pl.when(seen(j, k - 3))
            def _():
                to_partner(j, k - 3).wait_recv()
                attend(jnp.where(j == 0, z - k + 3, z + k - 3 - zn), False)

            return carry

        return lax.fori_loop(0, 2, quarter_step, carry)

    lax.fori_loop(1, steps_up + 4, one_step, 0)

    to_partner(0, 0).wait_send()

    def settle(k, carry):
        def both(d, c):
            @pl.when(goes_on(d, k))
            def _():
                for j in range(2):
                    along_z(d, k, j).wait_send()

            @pl.when(seen(d, k))
            def _():
                for j in range(2):
                    along_x(d, k, j).wait_send()
                to_partner(d, k).wait_send()

            return c

        return lax.fori_loop(0, 2, both, carry)

    lax.fori_loop(0, steps_up + 1, settle, 0)

    for h in range(2):
        out_ref[:, h * LANES : (h + 1) * LANES] = (mixed[h, :, :LANES] / mixed[h, :, LANES:]).astype(
            out_ref.dtype
        )
    out_ref[:, 2 * LANES :] = jnp.where(
        low, mixed[2, :, :LANES] / mixed[2, :, LANES:], mixed[3, :, :LANES] / mixed[3, :, LANES:]
    ).astype(out_ref.dtype)


def attention(
    latent, rope_key, wide_query, narrow_query, wide_key, wide_value, narrow_key, narrow_value, gain
):
    tokens, width = latent.shape
    n_sp, n_tp = lax.axis_size("sp"), lax.axis_size("tp")
    zn = n_sp // 2
    assert n_sp % 4 == 0 and n_tp == 4 and wide_query.shape[1] == 3 * LANES
    assert narrow_query.shape[1] == 2 * LANES and zn >= 4
    local_cos, local_sin = angle_tables(np.arange(tokens, dtype=np.float64))
    base_cos, base_sin = angle_tables(np.arange(n_sp, dtype=np.float64) * tokens)
    hops = zn // 2 + 1
    dma = pltpu.SemaphoreType.DMA
    vmem = pl.BlockSpec(memory_space=pltpu.VMEM)
    return pl.pallas_call(
        functools.partial(attention_kernel, n_sp, n_tp),
        out_shape=jax.ShapeDtypeStruct((tokens, 3 * LANES), jnp.bfloat16),
        in_specs=[pl.BlockSpec(memory_space=pltpu.HBM)] * 13,
        out_specs=vmem,
        scratch_shapes=[
            pltpu.VMEM(latent.shape, jnp.bfloat16),
            pltpu.VMEM(rope_key.shape[::-1], jnp.bfloat16),
            pltpu.VMEM(wide_query.shape, jnp.bfloat16),
            pltpu.VMEM(narrow_query.shape, jnp.bfloat16),
            pltpu.VMEM(wide_key.shape, jnp.bfloat16),
            pltpu.VMEM(wide_value.shape, jnp.bfloat16),
            pltpu.VMEM((1, width), jnp.float32),
            pltpu.VMEM(local_cos.shape, jnp.float32),
            pltpu.VMEM(local_sin.shape, jnp.float32),
            pltpu.VMEM(base_cos.shape, jnp.float32),
            pltpu.VMEM(base_sin.shape, jnp.float32),
            pltpu.VMEM((n_sp, n_tp, tokens // n_tp, width + LANES), jnp.bfloat16),
            pltpu.VMEM((4, tokens, 2 * LANES), jnp.bfloat16),
            pltpu.VMEM((width, 2 * LANES), jnp.bfloat16),
            pltpu.VMEM((4, tokens, LANES), jnp.float32),
            pltpu.VMEM((4, tokens, 2 * LANES), jnp.float32),
            dma((13,)),
            dma((2, hops, 2)),
            dma((2, hops + 1, 2)),
            dma((2, hops, 2)),
            dma((2, hops, 2)),
            dma((2, hops)),
            dma((2, hops)),
            pltpu.SemaphoreType.REGULAR,
        ],
        compiler_params=pltpu.CompilerParams(
            collective_id=0, has_side_effects=True, vmem_limit_bytes=VMEM_BYTES
        ),
    )(
        latent,
        rope_key.T,
        wide_query,
        narrow_query,
        wide_key,
        wide_value,
        narrow_key,
        narrow_value,
        gain.reshape(1, width),
        local_cos,
        local_sin,
        base_cos,
        base_sin,
    )


DELTAS = ((0, 6, -6, 5, -5, 2, -2, 1), (8, 7, -7, 4, -4, 3, -3, -1))
COLUMNS = 1024
CAPACITY = 2


def silu(v):
    return v / (1.0 + jnp.exp(-v))


def experts_kernel(
    n_sp,
    n_tp,
    mix_ref,
    routes_hbm,
    weight_hbm,
    out_wide_hbm,
    out_narrow_hbm,
    residual_hbm,
    gain_hbm,
    shared_gate_hbm,
    shared_up_hbm,
    shared_down_hbm,
    expert_gate_hbm,
    expert_up_hbm,
    expert_down_hbm,
    out_ref,
    routes_ref,
    weight_ref,
    places,
    out_weight,
    residual_ref,
    gain_ref,
    shared_in,
    shared_down,
    expert_in,
    expert_down,
    part,
    opposite,
    summed,
    landed,
    stream,
    gathered,
    outgoing,
    first_recv,
    first_relay,
    second_send,
    second_recv,
    finished,
    back_recv,
    back_send,
    back_relay,
    returned,
    shared_send,
    shared_recv,
    fetch,
    send_sems,
    recv_sems,
):
    rows, depth = residual_hbm.shape
    half = depth // 2
    zn = n_sp // 2
    lanes = 2 * n_tp
    piece = outgoing.shape[1]
    wide_rows = out_wide_hbm.shape[0]
    ff = shared_gate_hbm.shape[1]
    hidden = expert_gate_hbm.shape[1]
    top_count = routes_hbm.shape[0]
    me = lax.axis_index("sp")
    x = lax.axis_index("tp")
    z = me // 2
    core = lax.rem(me, 2)
    lane = core * n_tp + x

    def at_plane(delta):
        return lax.rem(z + (delta + zn), zn)

    def on_plane(delta):
        return {"sp": at_plane(delta) * 2 + core}

    def along_x(dx):
        return {"tp": lax.rem(x + (dx + n_tp), n_tp)}

    def in_plane(dc, dx):
        other = 1 - core if dc else core
        return {"sp": z * 2 + other, "tp": lax.rem(x + (dx + n_tp), n_tp)}

    relative = [(dc, dx) for dc in range(2) for dx in range(n_tp)]

    taken = [0]

    def remote(source, target, place):
        i = taken[0]
        taken[0] += 1
        return pltpu.make_async_remote_copy(
            src_ref=source,
            dst_ref=target,
            send_sem=send_sems.at[i],
            recv_sem=recv_sems.at[i],
            device_id=place,
            device_id_type=pl.DeviceIdType.MESH,
        )

    barrier = pltpu.get_barrier_semaphore()
    greeted = [on_plane(d) for d in range(1, zn)] + [in_plane(dc, dx) for dc, dx in relative[1:]]
    for place in greeted:
        pl.semaphore_signal(barrier, inc=1, device_id=place, device_id_type=pl.DeviceIdType.MESH)

    fetches = [
        pltpu.make_async_copy(source, target, fetch.at[i])
        for i, (source, target) in enumerate(
            (
                (routes_hbm, routes_ref),
                (weight_hbm, weight_ref),
                (out_wide_hbm, out_weight.at[pl.ds(0, wide_rows)]),
                (out_narrow_hbm, out_weight.at[pl.ds(wide_rows, out_narrow_hbm.shape[0])]),
                (residual_hbm, residual_ref),
                (gain_hbm, gain_ref),
                (shared_gate_hbm, shared_in.at[:, pl.ds(0, ff)]),
                (shared_up_hbm, shared_in.at[:, pl.ds(ff, ff)]),
                (shared_down_hbm, shared_down),
                (expert_gate_hbm.at[0], expert_in.at[pl.ds(0, hidden)]),
                (expert_up_hbm.at[0], expert_in.at[pl.ds(hidden, hidden)]),
                (expert_down_hbm.at[0], expert_down),
            )
        )
    ]
    for copy in fetches[:6]:
        copy.start()

    def normed(values):
        return rms_scale(values.astype(jnp.float32), gain_ref[...]).astype(jnp.bfloat16)

    def chunks():
        return [pl.ds(n, COLUMNS) for n in range(0, depth, COLUMNS)]

    half_cols = (pl.ds(0, half), pl.ds(half, half))
    lower, upper = half_cols
    split = half // 2

    def sides(g):
        return pl.ds(g * half, split), pl.ds(g * half + split, split)

    def project(dx, g):
        q = pl.multiple_of(lax.rem(x + dx, n_tp) * rows, rows)
        mine = mix_ref[pl.ds(q, rows), :]
        for cols in sides(g):
            part[dx, :, cols] = jnp.dot(
                mine, out_weight[:, cols], preferred_element_type=jnp.float32
            ).astype(jnp.bfloat16)

    sent = []

    def begin(source, target, place):
        copy = remote(source, target, place)
        copy.start()
        sent.append(copy)
        return copy

    def to_opposite(g):
        left_side, right_side = sides(g)
        return (
            begin(part.at[2, :, left_side], opposite.at[g, 0], along_x(1)),
            begin(part.at[2, :, right_side], opposite.at[g, 1], along_x(-1)),
        )

    def straight(g):
        left_side, right_side = sides(g)
        return (
            begin(part.at[1, :, right_side], landed.at[g, 0, 1], along_x(1)),
            begin(part.at[3, :, left_side], landed.at[g, 1, 0], along_x(-1)),
        )

    def joined(g, waiting):
        copies = []
        for side, (dx, cols) in enumerate(zip((1, 3), sides(g))):
            waiting[side].wait_recv()
            summed[g, side] = (
                part[dx, :, cols].astype(jnp.float32) + opposite[g, side].astype(jnp.float32)
            ).astype(jnp.bfloat16)
            copies.append(
                begin(summed.at[g, side], landed.at[g, side, side], along_x(1 if side == 0 else -1))
            )
        return tuple(copies)

    def add_up(g, waiting):
        for copy in waiting:
            copy.wait_recv()
        for side, cols in enumerate(sides(g)):
            stream[:, cols] = (
                residual_ref[:, cols].astype(jnp.float32)
                + part[0, :, cols].astype(jnp.float32)
                + landed[g, 0, side].astype(jnp.float32)
                + landed[g, 1, side].astype(jnp.float32)
            ).astype(jnp.bfloat16)
        gathered[0, :, half_cols[g]] = stream[:, half_cols[g]]
        for cols in sides(g):
            outgoing[:, :, cols] = (
                jnp.dot(send_map, gathered[0, :, cols], preferred_element_type=jnp.float32)
                .astype(jnp.bfloat16)
                .reshape(zn, piece, split)
            )

    for copy in fetches[:4]:
        copy.wait()
    for copy in fetches[6:]:
        copy.start()
    project(2, 0)
    pl.semaphore_wait(barrier, len(greeted))
    opposite_copies = [to_opposite(0)]
    project(1, 0)
    project(3, 0)
    straight_copies = [straight(0)]
    project(0, 0)

    r0 = lax.broadcasted_iota(jnp.int32, (rows, rows), 0)
    r1 = lax.broadcasted_iota(jnp.int32, (rows, rows), 1)

    def upright(row):
        return jnp.sum(jnp.where(r0 == r1, row, 0.0), axis=1, keepdims=True)

    named = [routes_ref[c : c + 1, :].astype(jnp.float32) for c in range(top_count)]
    shares = [upright(weight_ref[c : c + 1, :]) for c in range(top_count)]
    slot = lax.broadcasted_iota(jnp.int32, (zn * piece, rows), 0).astype(jnp.float32)
    maps = []
    for c in range(top_count):
        earlier = jnp.zeros((1, rows), jnp.float32)
        for other in range(top_count):
            same = (upright(named[other]) == named[c]) & (r0 < r1)
            earlier = earlier + jnp.sum(jnp.where(same, 1.0, 0.0), axis=0, keepdims=True)
        maps.append(jnp.where(slot == named[c] * CAPACITY + earlier, 1.0, 0.0))
        places[c] = maps[c].T.astype(jnp.bfloat16)
    send_map = sum(maps[1:], maps[0]).astype(jnp.bfloat16)

    joined_copies = [joined(0, opposite_copies[0])]
    project(2, 1)
    opposite_copies.append(to_opposite(1))
    project(1, 1)
    project(3, 1)
    straight_copies.append(straight(1))
    project(0, 1)
    for copy in fetches[4:6]:
        copy.wait()

    far = at_plane(8)
    first = [[], []]
    relays_in = []
    for g, cols in enumerate(half_cols):
        add_up(g, straight_copies[g] + joined_copies[g])
        relays_in.append(begin(outgoing.at[far, :, cols], first_relay.at[g], on_plane(4 if g == 0 else -4)))
        for j, delta in enumerate(DELTAS[0]):
            if delta not in (0, 8):
                first[0].append(
                    begin(outgoing.at[at_plane(delta), :, cols], first_recv.at[0, j, :, cols], on_plane(delta))
                )
        if g == 0:
            joined_copies.append(joined(1, opposite_copies[1]))
    spread = [begin(gathered.at[0], gathered.at[dx], along_x(dx)) for dx in (1, 3, 2)]
    first_recv[0, 0] = outgoing[z]
    far_slot = DELTAS[1].index(8)
    for g, cols in enumerate(half_cols):
        relays_in[g].wait_recv()
        first[1].append(
            begin(first_relay.at[g], first_recv.at[1, far_slot, :, cols], on_plane(4 if g == 0 else -4))
        )
    for j, delta in enumerate(DELTAS[1]):
        if delta != 8:
            first[1].append(begin(outgoing.at[at_plane(delta)], first_recv.at[1, j], on_plane(delta)))

    count = lanes * piece
    o = lax.broadcasted_iota(jnp.int32, (count, count), 0)
    i = lax.broadcasted_iota(jnp.int32, (count, count), 1)
    swap = jnp.where(
        (o // piece == (i % piece) // 2) & ((o % piece) // 2 == i // piece) & (o % 2 == i % 2), 1.0, 0.0
    ).astype(jnp.bfloat16)

    def swapped(source, target, ch):
        for cols in chunks():
            target[ch, :, :, cols] = (
                jnp.dot(
                    swap, source[ch, :, :, cols].reshape(count, COLUMNS), preferred_element_type=jnp.float32
                )
                .astype(jnp.bfloat16)
                .reshape(lanes, piece, COLUMNS)
            )

    def to_lanes(ch):
        swapped(first_recv, second_send, ch)
        copies = []
        for r, (dc, dx) in enumerate(relative):
            if r == 0:
                continue
            other = (1 - core if dc else core) * n_tp + lax.rem(x + dx, n_tp)
            copies.append(remote(second_send.at[ch, other], second_recv.at[ch, r], in_plane(dc, dx)))
            copies[-1].start()
        second_recv[ch, 0] = second_send[ch, lane]
        return copies

    def run_expert(ch):
        taken_in = normed(second_recv[ch].reshape(count, depth))
        gate, lifted = (
            lax.dot_general(
                taken_in,
                expert_in[pl.ds(at, hidden), :],
                (((1,), (1,)), ((), ())),
                preferred_element_type=jnp.float32,
            )
            for at in (0, hidden)
        )
        active = (silu(gate) * lifted).astype(jnp.bfloat16)
        for cols in chunks():
            finished[ch, :, :, cols] = (
                jnp.dot(active, expert_down[:, cols], preferred_element_type=jnp.float32)
                .astype(jnp.bfloat16)
                .reshape(lanes, piece, COLUMNS)
            )
        copies = []
        for r, (dc, dx) in enumerate(relative):
            if r == 0:
                continue
            copies.append(remote(finished.at[ch, r], back_recv.at[ch, lane], in_plane(dc, -dx)))
            copies[-1].start()
        back_recv[ch, lane] = finished[ch, 0]
        return copies

    def home(ch):
        swapped(back_recv, back_send, ch)
        copies = []
        relays = []
        for j, delta in enumerate(DELTAS[ch]):
            if delta == 8:
                relays = [
                    remote(back_send.at[ch, j, :, lower], back_relay.at[0], on_plane(4)),
                    remote(back_send.at[ch, j, :, upper], back_relay.at[1], on_plane(-4)),
                ]
                for copy in relays:
                    copy.start()
        for j, delta in enumerate(DELTAS[ch]):
            if delta == 0:
                returned[z] = back_send[ch, j]
            elif delta != 8:
                copies.append(remote(back_send.at[ch, j], returned.at[z], on_plane(-delta)))
                copies[-1].start()
        return copies, relays

    for copy in first[0]:
        copy.wait_recv()
    lane_copies = to_lanes(0)

    for copy in fetches[6:]:
        copy.wait()
    for copy in spread:
        copy.wait_recv()
    every = normed(gathered[...].reshape(n_tp * rows, depth))
    both = jnp.dot(every, shared_in[...], preferred_element_type=jnp.float32)
    act = (silu(both[:, :ff]) * both[:, ff:]).astype(jnp.bfloat16)
    for cols in chunks():
        shared_send[:, :, cols] = (
            jnp.dot(act, shared_down[:, cols], preferred_element_type=jnp.float32)
            .astype(jnp.bfloat16)
            .reshape(n_tp, rows, COLUMNS)
        )

    for copy in lane_copies:
        copy.wait_recv()
    back_copies = run_expert(0)
    for copy in back_copies:
        copy.wait_recv()
    home_copies, _ = home(0)
    sent += lane_copies + back_copies + home_copies

    for copy in first[1]:
        copy.wait_recv()
    lane_copies = to_lanes(1)
    for copy in lane_copies:
        copy.wait_recv()
    back_copies = run_expert(1)
    shared_back = [remote(shared_send.at[dx], shared_recv.at[dx - 1], along_x(-dx)) for dx in range(1, n_tp)]
    for copy in shared_back:
        copy.start()
    sent += shared_back
    for copy in back_copies:
        copy.wait_recv()
    more_home, relays = home(1)
    relays[0].wait_recv()
    last_up = remote(back_relay.at[0], returned.at[at_plane(-4), :, lower], on_plane(4))
    last_up.start()
    relays[1].wait_recv()
    last_down = remote(back_relay.at[1], returned.at[at_plane(4), :, upper], on_plane(-4))
    last_down.start()
    sent += lane_copies + back_copies + more_home + relays + [last_up, last_down]

    for copy in shared_back:
        copy.wait_recv()
    for copy in home_copies + more_home + [last_up, last_down]:
        copy.wait_recv()
    for cols in chunks():
        total = stream[:, cols].astype(jnp.float32) + shared_send[0, :, cols].astype(jnp.float32)
        for dx in range(n_tp - 1):
            total = total + shared_recv[dx, :, cols].astype(jnp.float32)
        results = returned[:, :, cols].reshape(zn * piece, COLUMNS)
        for c in range(top_count):
            total = total + shares[c] * jnp.dot(places[c], results, preferred_element_type=jnp.float32)
        out_ref[:, cols] = total.astype(out_ref.dtype)
    for copy in sent:
        copy.wait_send()


def projected_experts(
    mix,
    routes,
    route_weights,
    out_wide,
    out_narrow,
    residual,
    gain,
    shared_gate,
    shared_up,
    shared_down,
    expert_gate,
    expert_up,
    expert_down,
):
    rows, depth = residual.shape
    n_sp, n_tp = lax.axis_size("sp"), lax.axis_size("tp")
    zn, lanes = n_sp // 2, 2 * n_tp
    piece = CAPACITY * lanes
    ff = shared_gate.shape[1]
    hidden = expert_gate.shape[2]
    assert zn == 16 and n_tp == 4 and expert_gate.shape[0] == 1
    vmem, hbm = pl.BlockSpec(memory_space=pltpu.VMEM), pl.BlockSpec(memory_space=pltpu.HBM)
    bf16 = jnp.bfloat16
    chunk = (2, lanes, piece, depth)
    dma = pltpu.SemaphoreType.DMA
    return pl.pallas_call(
        functools.partial(experts_kernel, n_sp, n_tp),
        out_shape=jax.ShapeDtypeStruct((rows, depth), bf16),
        in_specs=[vmem] + [hbm] * 12,
        out_specs=vmem,
        scratch_shapes=[
            pltpu.VMEM(routes.shape[::-1], jnp.int32),
            pltpu.VMEM(route_weights.shape[::-1], jnp.float32),
            pltpu.VMEM((routes.shape[1], rows, zn * piece), bf16),
            pltpu.VMEM((out_wide.shape[0] + out_narrow.shape[0], depth), bf16),
            pltpu.VMEM((rows, depth), bf16),
            pltpu.VMEM((1, depth), jnp.float32),
            pltpu.VMEM((depth, 2 * ff), bf16),
            pltpu.VMEM(shared_down.shape, bf16),
            pltpu.VMEM((2 * hidden, depth), bf16),
            pltpu.VMEM(expert_down.shape[1:], bf16),
            pltpu.VMEM((n_tp, rows, depth), bf16),
            pltpu.VMEM((2, 2, rows, depth // 4), bf16),
            pltpu.VMEM((2, 2, rows, depth // 4), bf16),
            pltpu.VMEM((2, 2, 2, rows, depth // 4), bf16),
            pltpu.VMEM((rows, depth), bf16),
            pltpu.VMEM((n_tp, rows, depth), bf16),
            pltpu.VMEM((zn, piece, depth), bf16),
            pltpu.VMEM(chunk, bf16),
            pltpu.VMEM((2, piece, depth // 2), bf16),
            pltpu.VMEM(chunk, bf16),
            pltpu.VMEM(chunk, bf16),
            pltpu.VMEM(chunk, bf16),
            pltpu.VMEM(chunk, bf16),
            pltpu.VMEM(chunk, bf16),
            pltpu.VMEM((2, piece, depth // 2), bf16),
            pltpu.VMEM((zn, piece, depth), bf16),
            pltpu.VMEM((n_tp, rows, depth), bf16),
            pltpu.VMEM((n_tp - 1, rows, depth), bf16),
            dma((12,)),
            dma((104,)),
            dma((104,)),
        ],
        compiler_params=pltpu.CompilerParams(
            collective_id=1, has_side_effects=True, vmem_limit_bytes=VMEM_BYTES
        ),
    )(
        mix,
        routes.T,
        route_weights.T,
        out_wide,
        out_narrow,
        residual,
        gain.reshape(1, depth),
        shared_gate,
        shared_up,
        shared_down,
        jnp.swapaxes(expert_gate, 1, 2),
        jnp.swapaxes(expert_up, 1, 2),
        expert_down,
    )


def body(
    latent,
    rope_key,
    wide_query,
    narrow_query,
    wide_key_weight,
    wide_value_weight,
    narrow_key_weight,
    narrow_value_weight,
    latent_norm_scale,
    out_wide,
    out_narrow,
    residual,
    ffn_gain,
    shared_gate,
    shared_up,
    shared_down,
    expert_gate,
    expert_up,
    expert_down,
    routes,
    route_weights,
):
    mix = attention(
        latent,
        rope_key,
        wide_query,
        narrow_query,
        wide_key_weight,
        wide_value_weight,
        narrow_key_weight,
        narrow_value_weight,
        latent_norm_scale,
    )
    return projected_experts(
        mix,
        routes,
        route_weights,
        out_wide,
        out_narrow,
        residual,
        ffn_gain,
        shared_gate,
        shared_up,
        shared_down,
        expert_gate,
        expert_up,
        expert_down,
    )


def solution(mesh):
    placed = (
        P(("grp", "sp"), None),
        P(("grp", "sp"), None),
        P(("grp", "sp"), "tp"),
        P(("grp", "sp"), "tp"),
        P(None, "tp"),
        P(None, "tp"),
        P(None, "tp"),
        P(None, "tp"),
        P(),
        P("tp", None),
        P("tp", None),
        P(("grp", "sp", "tp"), None),
        P(),
        P(None, "tp"),
        P(None, "tp"),
        P("tp", None),
        P(("sp", "tp"), None, None),
        P(("sp", "tp"), None, None),
        P(("sp", "tp"), None, None),
        P(("grp", "sp", "tp"), None),
        P(("grp", "sp", "tp"), None),
    )
    return jax.shard_map(
        body, mesh=mesh, in_specs=placed, out_specs=P(("grp", "sp", "tp"), None), check_vma=False
    )
```

```python
import functools

import jax
import jax.numpy as jnp
import numpy as np
from jax import lax
from jax.experimental import pallas as pl
from jax.experimental.pallas import tpu as pltpu
from jax.sharding import PartitionSpec as P

ROPE = 64
WIDE_HEAD_SIZE = 128
NARROW_HEAD_SIZE = 64
LANES = 128
VMEM_BYTES = 67_043_328


EPS = 1e-06
ROPE_BASE = 10000.0
NEG_FILL = -1e30
LOG2E = 1.4426950408889634


def rms_scale(values, gain):
    return values * lax.rsqrt(jnp.mean(values * values, axis=-1, keepdims=True) + EPS) * gain


def angle_tables(positions):
    half = ROPE // 2
    inverse = ROPE_BASE ** (-np.arange(half) * 2.0 / ROPE)
    angles = positions[:, None] * np.concatenate([inverse, inverse])[None, :]
    pad = ((0, 0), (0, LANES - ROPE))
    return (
        np.pad(np.cos(angles), pad).astype(np.float32),
        np.pad(np.sin(angles), pad).astype(np.float32),
    )


def attention_kernel(
    n_sp,
    n_tp,
    latent_hbm,
    rope_key_hbm,
    wide_query_hbm,
    narrow_query_hbm,
    wide_key_hbm,
    wide_value_hbm,
    narrow_key_hbm,
    narrow_value_hbm,
    gain_hbm,
    local_cos_hbm,
    local_sin_hbm,
    base_cos_hbm,
    base_sin_hbm,
    out_ref,
    latent_ref,
    rope_key_ref,
    wide_query_ref,
    narrow_query_ref,
    wide_key_ref,
    wide_value_ref,
    gain_ref,
    local_cos_ref,
    local_sin_ref,
    base_cos_ref,
    base_sin_ref,
    rows_buf,
    queries,
    narrow_weight,
    top,
    mixed,
    fetch,
    z_send,
    z_recv,
    x_send,
    x_recv,
    d_send,
    d_recv,
    wrap_open,
):
    tokens, width = latent_hbm.shape
    quarter = tokens // n_tp
    zn = n_sp // 2
    steps_up = zn // 2
    steps_down = zn - 1 - steps_up
    me = lax.axis_index("sp")
    x = lax.axis_index("tp")
    z = me // 2
    core = lax.rem(me, 2)
    right = lax.rem(x + 1, n_tp)
    left = lax.rem(x + n_tp - 1, n_tp)
    up = lax.rem(z + 1, zn)
    down = lax.rem(z + zn - 1, zn)
    partner = z * 2 + 1 - core

    fetches = [
        pltpu.make_async_copy(source, target, fetch.at[i])
        for i, (source, target) in enumerate(
            (
                (latent_hbm, latent_ref),
                (rope_key_hbm, rope_key_ref),
                (gain_hbm, gain_ref),
                (local_cos_hbm, local_cos_ref),
                (local_sin_hbm, local_sin_ref),
                (base_cos_hbm, base_cos_ref),
                (base_sin_hbm, base_sin_ref),
                (wide_query_hbm, wide_query_ref),
                (narrow_query_hbm, narrow_query_ref),
                (wide_key_hbm, wide_key_ref),
                (wide_value_hbm, wide_value_ref),
                (narrow_key_hbm, narrow_weight.at[:, pl.ds(0, LANES)]),
                (narrow_value_hbm, narrow_weight.at[:, pl.ds(LANES, LANES)]),
            )
        )
    ]
    for copy in fetches:
        copy.start()

    barrier = pltpu.get_barrier_semaphore()
    for place in ({"sp": down * 2 + core}, {"sp": partner}, {"tp": left}, {"tp": right}):
        pl.semaphore_signal(barrier, inc=1, device_id=place, device_id_type=pl.DeviceIdType.MESH)

    above = {"sp": up * 2 + core}

    @pl.when(z < zn - 1)
    def _():
        pl.semaphore_signal(barrier, inc=1, device_id=above, device_id_type=pl.DeviceIdType.MESH)


    for copy in fetches:
        copy.wait()
    lane = lax.broadcasted_iota(jnp.int32, (tokens, LANES), 1)
    low = lane < ROPE
    lc, ls = local_cos_ref[...], local_sin_ref[...]
    bc, bs = base_cos_ref[pl.ds(me, 1), :], base_sin_ref[pl.ds(me, 1), :]
    cosine = lc * bc - ls * bs
    sine = jnp.where(lane < ROPE // 2, -1.0, 1.0) * (ls * bc + lc * bs)

    def turn(v):
        other = jnp.where(
            lane < ROPE // 2, pltpu.roll(v, LANES - ROPE // 2, 1), pltpu.roll(v, ROPE // 2, 1)
        )
        return (v * cosine + other * sine).astype(jnp.bfloat16)

    lat = latent_ref[...].astype(jnp.float32)
    normed = rms_scale(lat, gain_ref[...]).astype(jnp.bfloat16)
    rope = rope_key_ref[...].astype(jnp.float32).T
    turned = turn(jnp.concatenate([rope, jnp.zeros_like(rope)], axis=1))
    for q in range(n_tp):
        rows_buf[me, q, :, :width] = normed[q * quarter : (q + 1) * quarter]
        rows_buf[me, q, :, width:] = turned[q * quarter : (q + 1) * quarter]

    t1 = wide_query_ref[:, LANES : 2 * LANES].astype(jnp.float32)
    t2 = wide_query_ref[:, 2 * LANES :].astype(jnp.float32)
    n0 = narrow_query_ref[:, :LANES].astype(jnp.float32)
    n1 = narrow_query_ref[:, LANES:].astype(jnp.float32)
    half = LANES // 2
    queries[0, :, :LANES] = wide_query_ref[:, :LANES]
    queries[0, :, LANES:] = turn(t1)
    queries[1, :, :LANES] = pltpu.roll(jnp.where(low, t2, t1), half, 1).astype(jnp.bfloat16)
    queries[1, :, LANES:] = turn(pltpu.roll(t2, half, 1))
    queries[2, :, :LANES] = jnp.where(low, n0, 0.0).astype(jnp.bfloat16)
    queries[2, :, LANES:] = turn(pltpu.roll(n0, half, 1))
    queries[3, :, :LANES] = pltpu.roll(jnp.where(low, n1, 0.0), half, 1).astype(jnp.bfloat16)
    queries[3, :, LANES:] = turn(pltpu.roll(n1, half, 1))
    top[...] = jnp.full(top.shape, NEG_FILL, jnp.float32)
    mixed[...] = jnp.zeros(mixed.shape, jnp.float32)

    @pl.when(z > 0)
    def _():
        pl.semaphore_wait(barrier, 5)

    @pl.when(z == 0)
    def _():
        pl.semaphore_wait(barrier, 4)

    @pl.when(z == zn - 1)
    def _():
        pl.semaphore_signal(wrap_open, inc=1, device_id=above, device_id_type=pl.DeviceIdType.MESH)

    def along_z(d, k, j):
        block = jnp.where(d == 0, z - k + zn, z + k) % zn
        target = jnp.where(d == 0, up, down)
        q = lax.rem(x + j, n_tp)
        spot = rows_buf.at[block * 2 + core, q]
        return pltpu.make_async_remote_copy(
            src_ref=spot,
            dst_ref=spot,
            send_sem=z_send.at[d, k, j],
            recv_sem=z_recv.at[d, k + 1, j],
            device_id={"sp": target * 2 + core},
            device_id_type=pl.DeviceIdType.MESH,
        )

    def along_x(d, k, j):
        block = jnp.where(d == 0, z - k + zn, z + k) % zn
        q = lax.rem(x + j, n_tp)
        spot = rows_buf.at[block * 2 + core, q]
        return pltpu.make_async_remote_copy(
            src_ref=spot,
            dst_ref=spot,
            send_sem=x_send.at[d, k, j],
            recv_sem=x_recv.at[d, k, j],
            device_id={"tp": jnp.where(j == 0, right, left)},
            device_id_type=pl.DeviceIdType.MESH,
        )

    def to_partner(d, k):
        block = jnp.where(d == 0, z - k + zn, z + k) % zn
        spot = rows_buf.at[block * 2 + core]
        return pltpu.make_async_remote_copy(
            src_ref=spot,
            dst_ref=spot,
            send_sem=d_send.at[d, k],
            recv_sem=d_recv.at[d, k],
            device_id={"sp": partner},
            device_id_type=pl.DeviceIdType.MESH,
        )

    def arrives(d, k):
        going_up = (k <= z) & (k <= steps_up)
        going_down = ((z + k) % zn < steps_down) & (k <= steps_down)
        return jnp.where(d == 0, going_up, going_down)

    def goes_on(d, k):
        going_up = (k <= z) & (k < steps_up) & (z + 1 < zn)
        going_down = ((z + k) % zn < steps_down) & (k < steps_down)
        return jnp.where(d == 0, going_up, going_down)

    def seen(d, k):
        going_up = (k <= z) & (k <= steps_up)
        going_down = (z + k >= zn) & (z + k - zn < steps_down) & (k <= steps_down)
        return (k >= 1) & jnp.where(d == 0, going_up, going_down)

    wide_factor = (WIDE_HEAD_SIZE + ROPE) ** (-0.5) * LOG2E
    narrow_factor = (NARROW_HEAD_SIZE + ROPE) ** (-0.5) * LOG2E

    def attend(plane, own):
        rows = rows_buf[pl.ds(plane * 2, 2)].reshape(2 * tokens, width + LANES)
        latents, turned_rows = rows[:, :width], rows[:, width:]
        keys = 2 * tokens
        ones = jnp.ones((keys, LANES), jnp.bfloat16)

        def up_from(weight):
            return jnp.dot(latents, weight[...], preferred_element_type=jnp.float32).astype(jnp.bfloat16)

        wide_k, wide_v, narrow = up_from(wide_key_ref), up_from(wide_value_ref), up_from(narrow_weight)
        narrow_k = jnp.concatenate([narrow[:, :LANES], turned_rows], axis=1)
        narrow_v = jnp.concatenate([narrow[:, LANES:], ones], axis=1)
        if own:
            gap = lax.broadcasted_iota(jnp.int32, (tokens, keys), 1) - lax.broadcasted_iota(
                jnp.int32, (tokens, keys), 0
            )
            visible = gap <= core * tokens
        for h in range(4):
            if h < 2:
                at = slice(h * LANES, (h + 1) * LANES)
                k_h = jnp.concatenate([wide_k[:, at], turned_rows], axis=1)
                v_h = jnp.concatenate([wide_v[:, at], ones], axis=1)
            else:
                k_h, v_h = narrow_k, narrow_v
            scores = lax.dot_general(
                queries[h], k_h, (((1,), (1,)), ((), ())), preferred_element_type=jnp.float32
            ) * (wide_factor if h < 2 else narrow_factor)
            if own:
                scores = jnp.where(visible, scores, NEG_FILL)
            old = top[h]
            new = jnp.maximum(old, jnp.max(scores, axis=1, keepdims=True))
            top[h] = new
            weights = jnp.exp2(scores - jnp.concatenate([new] * (keys // LANES), axis=1)).astype(jnp.bfloat16)
            fading = jnp.exp2(old - new)
            mixed[h] = mixed[h] * jnp.concatenate([fading, fading], axis=1) + jnp.dot(
                weights, v_h, preferred_element_type=jnp.float32
            )

    to_partner(0, 0).start()
    for d in range(2):

        @pl.when(goes_on(d, 0) & ((d == 0) | (z > 0)))
        def _():
            for j in range(2):
                along_z(d, 0, j).start()

    to_partner(0, 0).wait_recv()

    attend(z, True)

    @pl.when(z == 0)
    def _():
        pl.semaphore_wait(wrap_open, 1)
        for j in range(2):
            along_z(1, 0, j).start()

    def one_step(k, carry):
        def quarter_step(j, carry):
            def forward(d, c):
                @pl.when(arrives(d, k))
                def _():
                    along_z(d, k - 1, j).wait_recv()

                @pl.when(goes_on(d, k))
                def _():
                    along_z(d, k, j).start()

                @pl.when(seen(d, k))
                def _():
                    along_x(d, k, j).start()

                return c

            def share(d, c):
                @pl.when(seen(d, k - 1) & (j == 1))
                def _():
                    for side in range(2):
                        along_x(d, k - 1, side).wait_recv()
                    to_partner(d, k - 1).start()

                return c

            lax.fori_loop(0, 2, forward, 0)
            lax.fori_loop(0, 2, share, 0)

            @pl.when(seen(j, k - 3))
            def _():
                to_partner(j, k - 3).wait_recv()
                attend(jnp.where(j == 0, z - k + 3, z + k - 3 - zn), False)

            return carry

        return lax.fori_loop(0, 2, quarter_step, carry)

    lax.fori_loop(1, steps_up + 4, one_step, 0)

    to_partner(0, 0).wait_send()

    def settle(k, carry):
        def both(d, c):
            @pl.when(goes_on(d, k))
            def _():
                for j in range(2):
                    along_z(d, k, j).wait_send()

            @pl.when(seen(d, k))
            def _():
                for j in range(2):
                    along_x(d, k, j).wait_send()
                to_partner(d, k).wait_send()

            return c

        return lax.fori_loop(0, 2, both, carry)

    lax.fori_loop(0, steps_up + 1, settle, 0)

    for h in range(2):
        out_ref[:, h * LANES : (h + 1) * LANES] = (mixed[h, :, :LANES] / mixed[h, :, LANES:]).astype(
            out_ref.dtype
        )
    out_ref[:, 2 * LANES :] = jnp.where(
        low, mixed[2, :, :LANES] / mixed[2, :, LANES:], mixed[3, :, :LANES] / mixed[3, :, LANES:]
    ).astype(out_ref.dtype)


def attention(
    latent, rope_key, wide_query, narrow_query, wide_key, wide_value, narrow_key, narrow_value, gain
):
    tokens, width = latent.shape
    n_sp, n_tp = lax.axis_size("sp"), lax.axis_size("tp")
    zn = n_sp // 2
    assert n_sp % 4 == 0 and n_tp == 4 and wide_query.shape[1] == 3 * LANES
    assert narrow_query.shape[1] == 2 * LANES and zn >= 4
    local_cos, local_sin = angle_tables(np.arange(tokens, dtype=np.float64))
    base_cos, base_sin = angle_tables(np.arange(n_sp, dtype=np.float64) * tokens)
    hops = zn // 2 + 1
    dma = pltpu.SemaphoreType.DMA
    vmem = pl.BlockSpec(memory_space=pltpu.VMEM)
    return pl.pallas_call(
        functools.partial(attention_kernel, n_sp, n_tp),
        out_shape=jax.ShapeDtypeStruct((tokens, 3 * LANES), jnp.bfloat16),
        in_specs=[pl.BlockSpec(memory_space=pltpu.HBM)] * 13,
        out_specs=vmem,
        scratch_shapes=[
            pltpu.VMEM(latent.shape, jnp.bfloat16),
            pltpu.VMEM(rope_key.shape[::-1], jnp.bfloat16),
            pltpu.VMEM(wide_query.shape, jnp.bfloat16),
            pltpu.VMEM(narrow_query.shape, jnp.bfloat16),
            pltpu.VMEM(wide_key.shape, jnp.bfloat16),
            pltpu.VMEM(wide_value.shape, jnp.bfloat16),
            pltpu.VMEM((1, width), jnp.float32),
            pltpu.VMEM(local_cos.shape, jnp.float32),
            pltpu.VMEM(local_sin.shape, jnp.float32),
            pltpu.VMEM(base_cos.shape, jnp.float32),
            pltpu.VMEM(base_sin.shape, jnp.float32),
            pltpu.VMEM((n_sp, n_tp, tokens // n_tp, width + LANES), jnp.bfloat16),
            pltpu.VMEM((4, tokens, 2 * LANES), jnp.bfloat16),
            pltpu.VMEM((width, 2 * LANES), jnp.bfloat16),
            pltpu.VMEM((4, tokens, LANES), jnp.float32),
            pltpu.VMEM((4, tokens, 2 * LANES), jnp.float32),
            dma((13,)),
            dma((2, hops, 2)),
            dma((2, hops + 1, 2)),
            dma((2, hops, 2)),
            dma((2, hops, 2)),
            dma((2, hops)),
            dma((2, hops)),
            pltpu.SemaphoreType.REGULAR,
        ],
        compiler_params=pltpu.CompilerParams(
            collective_id=0, has_side_effects=True, vmem_limit_bytes=VMEM_BYTES
        ),
    )(
        latent,
        rope_key.T,
        wide_query,
        narrow_query,
        wide_key,
        wide_value,
        narrow_key,
        narrow_value,
        gain.reshape(1, width),
        local_cos,
        local_sin,
        base_cos,
        base_sin,
    )


DELTAS = ((0, 6, -6, 5, -5, 3, -3, 1), (8, 7, -7, 4, -4, 2, -2, -1))
COLUMNS = 1024
CAPACITY = 2


def silu(v):
    return v / (1.0 + jnp.exp(-v))


def experts_kernel(
    n_sp,
    n_tp,
    mix_ref,
    routes_hbm,
    weight_hbm,
    out_wide_hbm,
    out_narrow_hbm,
    residual_hbm,
    gain_hbm,
    shared_gate_hbm,
    shared_up_hbm,
    shared_down_hbm,
    expert_gate_hbm,
    expert_up_hbm,
    expert_down_hbm,
    out_ref,
    routes_ref,
    weight_ref,
    places,
    out_weight,
    residual_ref,
    gain_ref,
    shared_in,
    shared_down,
    expert_in,
    expert_down,
    part,
    opposite,
    summed,
    landed,
    stream,
    gathered,
    outgoing,
    first_recv,
    first_relay,
    second_send,
    second_recv,
    finished,
    back_recv,
    back_send,
    back_relay,
    returned,
    shared_send,
    shared_recv,
    fetch,
    send_sems,
    recv_sems,
):
    rows, depth = residual_hbm.shape
    half = depth // 2
    zn = n_sp // 2
    lanes = 2 * n_tp
    piece = outgoing.shape[1]
    wide_rows = out_wide_hbm.shape[0]
    ff = shared_gate_hbm.shape[1]
    hidden = expert_gate_hbm.shape[1]
    top_count = routes_hbm.shape[0]
    me = lax.axis_index("sp")
    x = lax.axis_index("tp")
    z = me // 2
    core = lax.rem(me, 2)
    lane = core * n_tp + x

    def at_plane(delta):
        return lax.rem(z + (delta + zn), zn)

    def on_plane(delta):
        return {"sp": at_plane(delta) * 2 + core}

    def along_x(dx):
        return {"tp": lax.rem(x + (dx + n_tp), n_tp)}

    def in_plane(dc, dx):
        other = 1 - core if dc else core
        return {"sp": z * 2 + other, "tp": lax.rem(x + (dx + n_tp), n_tp)}

    relative = [(dc, dx) for dc in range(2) for dx in range(n_tp)]

    taken = [0]

    def remote(source, target, place):
        i = taken[0]
        taken[0] += 1
        return pltpu.make_async_remote_copy(
            src_ref=source,
            dst_ref=target,
            send_sem=send_sems.at[i],
            recv_sem=recv_sems.at[i],
            device_id=place,
            device_id_type=pl.DeviceIdType.MESH,
        )

    barrier = pltpu.get_barrier_semaphore()
    greeted = [on_plane(d) for d in range(1, zn)] + [in_plane(dc, dx) for dc, dx in relative[1:]]
    for place in greeted:
        pl.semaphore_signal(barrier, inc=1, device_id=place, device_id_type=pl.DeviceIdType.MESH)

    fetches = [
        pltpu.make_async_copy(source, target, fetch.at[i])
        for i, (source, target) in enumerate(
            (
                (routes_hbm, routes_ref),
                (weight_hbm, weight_ref),
                (out_wide_hbm, out_weight.at[pl.ds(0, wide_rows)]),
                (out_narrow_hbm, out_weight.at[pl.ds(wide_rows, out_narrow_hbm.shape[0])]),
                (residual_hbm, residual_ref),
                (gain_hbm, gain_ref),
                (shared_gate_hbm, shared_in.at[:, pl.ds(0, ff)]),
                (shared_up_hbm, shared_in.at[:, pl.ds(ff, ff)]),
                (shared_down_hbm, shared_down),
                (expert_gate_hbm.at[0], expert_in.at[pl.ds(0, hidden)]),
                (expert_up_hbm.at[0], expert_in.at[pl.ds(hidden, hidden)]),
                (expert_down_hbm.at[0], expert_down),
            )
        )
    ]
    for copy in fetches[:6]:
        copy.start()

    def normed(values):
        return rms_scale(values.astype(jnp.float32), gain_ref[...]).astype(jnp.bfloat16)

    def chunks():
        return [pl.ds(n, COLUMNS) for n in range(0, depth, COLUMNS)]

    half_cols = (pl.ds(0, half), pl.ds(half, half))
    lower, upper = half_cols
    split = half // 2

    def sides(g):
        return pl.ds(g * half, split), pl.ds(g * half + split, split)

    def project(dx, g):
        q = pl.multiple_of(lax.rem(x + dx, n_tp) * rows, rows)
        mine = mix_ref[pl.ds(q, rows), :]
        for cols in sides(g):
            part[dx, :, cols] = jnp.dot(
                mine, out_weight[:, cols], preferred_element_type=jnp.float32
            ).astype(jnp.bfloat16)

    sent = []

    def begin(source, target, place):
        copy = remote(source, target, place)
        copy.start()
        sent.append(copy)
        return copy

    def to_opposite(g):
        left_side, right_side = sides(g)
        return (
            begin(part.at[2, :, left_side], opposite.at[g, 0], along_x(1)),
            begin(part.at[2, :, right_side], opposite.at[g, 1], along_x(-1)),
        )

    def straight(g):
        left_side, right_side = sides(g)
        return (
            begin(part.at[1, :, right_side], landed.at[g, 0, 1], along_x(1)),
            begin(part.at[3, :, left_side], landed.at[g, 1, 0], along_x(-1)),
        )

    def joined(g, waiting):
        copies = []
        for side, (dx, cols) in enumerate(zip((1, 3), sides(g))):
            waiting[side].wait_recv()
            summed[g, side] = (
                part[dx, :, cols].astype(jnp.float32) + opposite[g, side].astype(jnp.float32)
            ).astype(jnp.bfloat16)
            copies.append(
                begin(summed.at[g, side], landed.at[g, side, side], along_x(1 if side == 0 else -1))
            )
        return tuple(copies)

    def add_up(g, waiting):
        for copy in waiting:
            copy.wait_recv()
        for side, cols in enumerate(sides(g)):
            stream[:, cols] = (
                residual_ref[:, cols].astype(jnp.float32)
                + part[0, :, cols].astype(jnp.float32)
                + landed[g, 0, side].astype(jnp.float32)
                + landed[g, 1, side].astype(jnp.float32)
            ).astype(jnp.bfloat16)
        gathered[0, :, half_cols[g]] = stream[:, half_cols[g]]
        for cols in sides(g):
            outgoing[:, :, cols] = (
                jnp.dot(send_map, gathered[0, :, cols], preferred_element_type=jnp.float32)
                .astype(jnp.bfloat16)
                .reshape(zn, piece, split)
            )

    for copy in fetches[:4]:
        copy.wait()
    for copy in fetches[6:]:
        copy.start()
    project(2, 0)
    pl.semaphore_wait(barrier, len(greeted))
    opposite_copies = [to_opposite(0)]
    project(1, 0)
    project(3, 0)
    straight_copies = [straight(0)]
    project(0, 0)

    r0 = lax.broadcasted_iota(jnp.int32, (rows, rows), 0)
    r1 = lax.broadcasted_iota(jnp.int32, (rows, rows), 1)

    def upright(row):
        return jnp.sum(jnp.where(r0 == r1, row, 0.0), axis=1, keepdims=True)

    named = [routes_ref[c : c + 1, :].astype(jnp.float32) for c in range(top_count)]
    shares = [upright(weight_ref[c : c + 1, :]) for c in range(top_count)]
    slot = lax.broadcasted_iota(jnp.int32, (zn * piece, rows), 0).astype(jnp.float32)
    maps = []
    for c in range(top_count):
        earlier = jnp.zeros((1, rows), jnp.float32)
        for other in range(top_count):
            same = (upright(named[other]) == named[c]) & (r0 < r1)
            earlier = earlier + jnp.sum(jnp.where(same, 1.0, 0.0), axis=0, keepdims=True)
        maps.append(jnp.where(slot == named[c] * CAPACITY + earlier, 1.0, 0.0))
        places[c] = maps[c].T.astype(jnp.bfloat16)
    send_map = sum(maps[1:], maps[0]).astype(jnp.bfloat16)

    joined_copies = [joined(0, opposite_copies[0])]
    project(2, 1)
    opposite_copies.append(to_opposite(1))
    project(1, 1)
    project(3, 1)
    straight_copies.append(straight(1))
    project(0, 1)
    for copy in fetches[4:6]:
        copy.wait()

    far = at_plane(8)
    first = [[], []]
    relays_in = []
    for g, cols in enumerate(half_cols):
        add_up(g, straight_copies[g] + joined_copies[g])
        relays_in.append(begin(outgoing.at[far, :, cols], first_relay.at[g], on_plane(4 if g == 0 else -4)))
        for j, delta in enumerate(DELTAS[0]):
            if delta not in (0, 8):
                first[0].append(
                    begin(outgoing.at[at_plane(delta), :, cols], first_recv.at[0, j, :, cols], on_plane(delta))
                )
        if g == 0:
            joined_copies.append(joined(1, opposite_copies[1]))
    spread = [begin(gathered.at[0], gathered.at[dx], along_x(dx)) for dx in (1, 3, 2)]
    first_recv[0, 0] = outgoing[z]
    far_slot = DELTAS[1].index(8)
    for g, cols in enumerate(half_cols):
        relays_in[g].wait_recv()
        first[1].append(
            begin(first_relay.at[g], first_recv.at[1, far_slot, :, cols], on_plane(4 if g == 0 else -4))
        )
    for j, delta in enumerate(DELTAS[1]):
        if delta != 8:
            first[1].append(begin(outgoing.at[at_plane(delta)], first_recv.at[1, j], on_plane(delta)))

    count = lanes * piece
    o = lax.broadcasted_iota(jnp.int32, (count, count), 0)
    i = lax.broadcasted_iota(jnp.int32, (count, count), 1)
    swap = jnp.where(
        (o // piece == (i % piece) // 2) & ((o % piece) // 2 == i // piece) & (o % 2 == i % 2), 1.0, 0.0
    ).astype(jnp.bfloat16)

    def swapped(source, target, ch):
        for cols in chunks():
            target[ch, :, :, cols] = (
                jnp.dot(
                    swap, source[ch, :, :, cols].reshape(count, COLUMNS), preferred_element_type=jnp.float32
                )
                .astype(jnp.bfloat16)
                .reshape(lanes, piece, COLUMNS)
            )

    def to_lanes(ch):
        swapped(first_recv, second_send, ch)
        copies = []
        for r, (dc, dx) in enumerate(relative):
            if r == 0:
                continue
            other = (1 - core if dc else core) * n_tp + lax.rem(x + dx, n_tp)
            copies.append(remote(second_send.at[ch, other], second_recv.at[ch, r], in_plane(dc, dx)))
            copies[-1].start()
        second_recv[ch, 0] = second_send[ch, lane]
        return copies

    def run_expert(ch):
        taken_in = normed(second_recv[ch].reshape(count, depth))
        gate, lifted = (
            lax.dot_general(
                taken_in,
                expert_in[pl.ds(at, hidden), :],
                (((1,), (1,)), ((), ())),
                preferred_element_type=jnp.float32,
            )
            for at in (0, hidden)
        )
        active = (silu(gate) * lifted).astype(jnp.bfloat16)
        for cols in chunks():
            finished[ch, :, :, cols] = (
                jnp.dot(active, expert_down[:, cols], preferred_element_type=jnp.float32)
                .astype(jnp.bfloat16)
                .reshape(lanes, piece, COLUMNS)
            )
        copies = []
        for r, (dc, dx) in enumerate(relative):
            if r == 0:
                continue
            copies.append(remote(finished.at[ch, r], back_recv.at[ch, lane], in_plane(dc, -dx)))
            copies[-1].start()
        back_recv[ch, lane] = finished[ch, 0]
        return copies

    def home(ch):
        swapped(back_recv, back_send, ch)
        copies = []
        relays = []
        for j, delta in enumerate(DELTAS[ch]):
            if delta == 8:
                relays = [
                    remote(back_send.at[ch, j, :, lower], back_relay.at[0], on_plane(4)),
                    remote(back_send.at[ch, j, :, upper], back_relay.at[1], on_plane(-4)),
                ]
                for copy in relays:
                    copy.start()
        for j, delta in enumerate(DELTAS[ch]):
            if delta == 0:
                returned[z] = back_send[ch, j]
            elif delta != 8:
                copies.append(remote(back_send.at[ch, j], returned.at[z], on_plane(-delta)))
                copies[-1].start()
        return copies, relays

    for copy in first[0]:
        copy.wait_recv()
    lane_copies = to_lanes(0)

    for copy in fetches[6:]:
        copy.wait()
    for copy in spread:
        copy.wait_recv()
    every = normed(gathered[...].reshape(n_tp * rows, depth))
    both = jnp.dot(every, shared_in[...], preferred_element_type=jnp.float32)
    act = (silu(both[:, :ff]) * both[:, ff:]).astype(jnp.bfloat16)
    for cols in chunks():
        shared_send[:, :, cols] = (
            jnp.dot(act, shared_down[:, cols], preferred_element_type=jnp.float32)
            .astype(jnp.bfloat16)
            .reshape(n_tp, rows, COLUMNS)
        )

    for copy in lane_copies:
        copy.wait_recv()
    back_copies = run_expert(0)
    for copy in back_copies:
        copy.wait_recv()
    home_copies, _ = home(0)
    sent += lane_copies + back_copies + home_copies

    for copy in first[1]:
        copy.wait_recv()
    lane_copies = to_lanes(1)
    for copy in lane_copies:
        copy.wait_recv()
    back_copies = run_expert(1)
    shared_back = [remote(shared_send.at[dx], shared_recv.at[dx - 1], along_x(-dx)) for dx in range(1, n_tp)]
    for copy in shared_back:
        copy.start()
    sent += shared_back
    for copy in back_copies:
        copy.wait_recv()
    more_home, relays = home(1)
    relays[0].wait_recv()
    last_up = remote(back_relay.at[0], returned.at[at_plane(-4), :, lower], on_plane(4))
    last_up.start()
    relays[1].wait_recv()
    last_down = remote(back_relay.at[1], returned.at[at_plane(4), :, upper], on_plane(-4))
    last_down.start()
    sent += lane_copies + back_copies + more_home + relays + [last_up, last_down]

    for copy in shared_back:
        copy.wait_recv()
    for copy in home_copies + more_home + [last_up, last_down]:
        copy.wait_recv()
    for cols in chunks():
        total = stream[:, cols].astype(jnp.float32) + shared_send[0, :, cols].astype(jnp.float32)
        for dx in range(n_tp - 1):
            total = total + shared_recv[dx, :, cols].astype(jnp.float32)
        results = returned[:, :, cols].reshape(zn * piece, COLUMNS)
        for c in range(top_count):
            total = total + shares[c] * jnp.dot(places[c], results, preferred_element_type=jnp.float32)
        out_ref[:, cols] = total.astype(out_ref.dtype)
    for copy in sent:
        copy.wait_send()


def projected_experts(
    mix,
    routes,
    route_weights,
    out_wide,
    out_narrow,
    residual,
    gain,
    shared_gate,
    shared_up,
    shared_down,
    expert_gate,
    expert_up,
    expert_down,
):
    rows, depth = residual.shape
    n_sp, n_tp = lax.axis_size("sp"), lax.axis_size("tp")
    zn, lanes = n_sp // 2, 2 * n_tp
    piece = CAPACITY * lanes
    ff = shared_gate.shape[1]
    hidden = expert_gate.shape[2]
    assert zn == 16 and n_tp == 4 and expert_gate.shape[0] == 1
    vmem, hbm = pl.BlockSpec(memory_space=pltpu.VMEM), pl.BlockSpec(memory_space=pltpu.HBM)
    bf16 = jnp.bfloat16
    chunk = (2, lanes, piece, depth)
    dma = pltpu.SemaphoreType.DMA
    return pl.pallas_call(
        functools.partial(experts_kernel, n_sp, n_tp),
        out_shape=jax.ShapeDtypeStruct((rows, depth), bf16),
        in_specs=[vmem] + [hbm] * 12,
        out_specs=vmem,
        scratch_shapes=[
            pltpu.VMEM(routes.shape[::-1], jnp.int32),
            pltpu.VMEM(route_weights.shape[::-1], jnp.float32),
            pltpu.VMEM((routes.shape[1], rows, zn * piece), bf16),
            pltpu.VMEM((out_wide.shape[0] + out_narrow.shape[0], depth), bf16),
            pltpu.VMEM((rows, depth), bf16),
            pltpu.VMEM((1, depth), jnp.float32),
            pltpu.VMEM((depth, 2 * ff), bf16),
            pltpu.VMEM(shared_down.shape, bf16),
            pltpu.VMEM((2 * hidden, depth), bf16),
            pltpu.VMEM(expert_down.shape[1:], bf16),
            pltpu.VMEM((n_tp, rows, depth), bf16),
            pltpu.VMEM((2, 2, rows, depth // 4), bf16),
            pltpu.VMEM((2, 2, rows, depth // 4), bf16),
            pltpu.VMEM((2, 2, 2, rows, depth // 4), bf16),
            pltpu.VMEM((rows, depth), bf16),
            pltpu.VMEM((n_tp, rows, depth), bf16),
            pltpu.VMEM((zn, piece, depth), bf16),
            pltpu.VMEM(chunk, bf16),
            pltpu.VMEM((2, piece, depth // 2), bf16),
            pltpu.VMEM(chunk, bf16),
            pltpu.VMEM(chunk, bf16),
            pltpu.VMEM(chunk, bf16),
            pltpu.VMEM(chunk, bf16),
            pltpu.VMEM(chunk, bf16),
            pltpu.VMEM((2, piece, depth // 2), bf16),
            pltpu.VMEM((zn, piece, depth), bf16),
            pltpu.VMEM((n_tp, rows, depth), bf16),
            pltpu.VMEM((n_tp - 1, rows, depth), bf16),
            dma((12,)),
            dma((104,)),
            dma((104,)),
        ],
        compiler_params=pltpu.CompilerParams(
            collective_id=1, has_side_effects=True, vmem_limit_bytes=VMEM_BYTES
        ),
    )(
        mix,
        routes.T,
        route_weights.T,
        out_wide,
        out_narrow,
        residual,
        gain.reshape(1, depth),
        shared_gate,
        shared_up,
        shared_down,
        jnp.swapaxes(expert_gate, 1, 2),
        jnp.swapaxes(expert_up, 1, 2),
        expert_down,
    )


def body(
    latent,
    rope_key,
    wide_query,
    narrow_query,
    wide_key_weight,
    wide_value_weight,
    narrow_key_weight,
    narrow_value_weight,
    latent_norm_scale,
    out_wide,
    out_narrow,
    residual,
    ffn_gain,
    shared_gate,
    shared_up,
    shared_down,
    expert_gate,
    expert_up,
    expert_down,
    routes,
    route_weights,
):
    mix = attention(
        latent,
        rope_key,
        wide_query,
        narrow_query,
        wide_key_weight,
        wide_value_weight,
        narrow_key_weight,
        narrow_value_weight,
        latent_norm_scale,
    )
    return projected_experts(
        mix,
        routes,
        route_weights,
        out_wide,
        out_narrow,
        residual,
        ffn_gain,
        shared_gate,
        shared_up,
        shared_down,
        expert_gate,
        expert_up,
        expert_down,
    )


def solution(mesh):
    placed = (
        P(("grp", "sp"), None),
        P(("grp", "sp"), None),
        P(("grp", "sp"), "tp"),
        P(("grp", "sp"), "tp"),
        P(None, "tp"),
        P(None, "tp"),
        P(None, "tp"),
        P(None, "tp"),
        P(),
        P("tp", None),
        P("tp", None),
        P(("grp", "sp", "tp"), None),
        P(),
        P(None, "tp"),
        P(None, "tp"),
        P("tp", None),
        P(("sp", "tp"), None, None),
        P(("sp", "tp"), None, None),
        P(("sp", "tp"), None, None),
        P(("grp", "sp", "tp"), None),
        P(("grp", "sp", "tp"), None),
    )
    return jax.shard_map(
        body, mesh=mesh, in_specs=placed, out_specs=P(("grp", "sp", "tp"), None), check_vma=False
    )
```
